32 devices in a mesh: grp: 2 (over y), sp: 4 (over z), tp: 4 (over x, core).
Axes of the slice: x: 2, y: 2, z: 4, core: 2. Of those that a mesh axis runs over, the one named last changes fastest.
Arguments:
- tokens_in: bfloat16 [3072, 4096], P(('grp', 'sp')), parts along dimension 0, may hold values from -6 to 6
- norm_gain: float32 [4096], replicated, may hold values from 0.1 to 1.9
- window_query: bfloat16 [4096, 1024], P('sp', 'tp'), may hold values from -0.09375 to 0.09375
- window_key: bfloat16 [4096, 512], P('sp', 'tp'), may hold values from -0.09375 to 0.09375
- window_value: bfloat16 [4096, 512], P('sp', 'tp'), may hold values from -0.09375 to 0.09375
- window_query_gain: float32 [64], replicated, may hold values from 0.6 to 16
- window_key_gain: float32 [64], replicated, may hold values from 0.6 to 16
- sink_logit: float32 [16], P('tp'), may hold values from 1 to 6
- dense_query: bfloat16 [4096, 1024], P('sp', 'tp'), may hold values from -0.09375 to 0.09375
- dense_key: bfloat16 [4096, 512], P('sp', 'tp'), may hold values from -0.09375 to 0.09375
- dense_value: bfloat16 [4096, 512], P('sp', 'tp'), may hold values from -0.09375 to 0.09375
- dense_query_gain: float32 [64], replicated, may hold values from 1 to 14
- dense_key_gain: float32 [64], replicated, may hold values from 1 to 14
- window_out: bfloat16 [1024, 4096], P('tp', 'sp'), may hold values from -1.5 to 1.5
- dense_out: bfloat16 [1024, 4096], P('tp', 'sp'), may hold values from -3 to 3
Outputs:
- mixed_out: bfloat16 [3072, 4096], P(('grp', 'sp', 'tp')), parts along dimension 0
The draws below stay inside these ranges and needn't reach their ends.
There are 2 independent parts, one for each index of `grp`. The reference program is written for one: setup_inputs(seed, part) draws one part's arguments, and reference() takes and returns one part's arrays. A program takes and returns all parts, laid end to end along the dimension named above; an argument that names none is the same for every part. Nothing has to cross between parts.
All inputs are finite; a program needn't handle non-finite values.
Results may differ from the reference program's by a relative error of at most 0.03.
The reference program's roundings to bfloat16 on the way count: a program that leaves them out, or rounds other values in their place, can miss the bound.
Values may be sent and summed in bfloat16 or wider, within the bound.
A program may use at most 64 MiB of HBM per device.

```python
import jax
import jax.numpy as jnp
from jax import lax

D = 4096
B_HEADS = 16
B_KV = 8
C_HEADS = 16
C_KV = 8
HD = 64
WINDOW = 128
GRID_W = 64
TOKENS = 1536
N_TP = 4


def gain_values(key, salt, low, high, hidden_low, hidden_high):
    subkey = jax.random.fold_in(key, salt)
    return jax.random.uniform(subkey, (HD,), jnp.float32, low, high)


def draw_window_query_gain(key, part):
    return gain_values(key, 101, 0.6, 1.6, 12.0, 16.0)


def draw_window_key_gain(key, part):
    return gain_values(key, 102, 0.6, 1.6, 12.0, 16.0)


def draw_dense_query_gain(key, part):
    return gain_values(key, 103, 1.0, 1.8, 10.0, 14.0)


def draw_dense_key_gain(key, part):
    return gain_values(key, 104, 1.0, 1.8, 10.0, 14.0)


def steps_of(key, shape, pieces, least, top_value):
    loudness = 1.0
    for axis_at, blocks in pieces:
        draws = jax.random.uniform(jax.random.fold_in(jax.random.fold_in(key, 6), axis_at), (blocks,), jnp.float32, least / len(pieces), top_value / len(pieces))
        loudness = loudness * jnp.repeat(jnp.exp(draws), shape[axis_at] // blocks).reshape((-1,) + (1,) * (len(shape) - 1 - axis_at))
    return loudness


def noise(key, extent, deviation, reach, cuts=(), held_as=jnp.bfloat16):
    loudness = steps_of(key, extent, cuts, -0.22, 0.18) if cuts else 1.0
    entries = jax.random.normal(key, extent, jnp.float32) * deviation * loudness
    return jnp.minimum(jnp.maximum(entries, -reach), reach).astype(held_as)


def setup_inputs(seed: int = 0, part: int = 0) -> dict:
    seeds = jax.random.split(jax.random.key(seed), 16)
    part_splits = jax.random.split(jax.random.fold_in(seeds[15], part), 16)
    tokens_in = noise(part_splits[0], (TOKENS, D), 1.0, 6.0, ((0, 4),))
    norm_gain = jnp.clip(1.0 + 0.18 * jax.random.normal(seeds[1], (D,), jnp.float32), 0.1, 1.9)
    window_query = noise(seeds[2], (D, B_HEADS * HD), D ** -0.5, 0.09375, ((0, 4), (1, 4)))
    window_key = noise(seeds[3], (D, B_KV * HD), D ** -0.5, 0.09375, ((0, 4), (1, 4)))
    window_value = noise(seeds[4], (D, B_KV * HD), D ** -0.5, 0.09375, ((0, 4), (1, 4)))
    window_query_gain = draw_window_query_gain(jax.random.fold_in(seeds[15], 71), part)
    window_key_gain = draw_window_key_gain(jax.random.fold_in(seeds[15], 71), part)
    sink_logit = jnp.clip(1.0 + 5.0 * jax.random.uniform(seeds[7], (B_HEADS,), jnp.float32) ** steps_of(seeds[7], (B_HEADS,), ((0, 4),), -0.2, 0.2), 1.0, 6.0)
    dense_query = noise(seeds[8], (D, C_HEADS * HD), D ** -0.5, 0.09375, ((0, 4), (1, 4)))
    dense_key = noise(seeds[9], (D, C_KV * HD), D ** -0.5, 0.09375, ((0, 4), (1, 4)))
    dense_value = noise(seeds[10], (D, C_KV * HD), D ** -0.5, 0.09375, ((0, 4), (1, 4)))
    dense_query_gain = draw_dense_query_gain(jax.random.fold_in(seeds[15], 71), part)
    dense_key_gain = draw_dense_key_gain(jax.random.fold_in(seeds[15], 71), part)
    window_out = noise(seeds[13], (B_HEADS * HD, D), 0.25, 1.5, ((0, 4), (1, 4)))
    dense_out = noise(seeds[14], (C_HEADS * HD, D), 0.5, 3.0, ((0, 4), (1, 4)))
    return {"tokens_in": tokens_in, "norm_gain": norm_gain, "window_query": window_query, "window_key": window_key, "window_value": window_value, "window_query_gain": window_query_gain, "window_key_gain": window_key_gain, "sink_logit": sink_logit, "dense_query": dense_query, "dense_key": dense_key, "dense_value": dense_value, "dense_query_gain": dense_query_gain, "dense_key_gain": dense_key_gain, "window_out": window_out, "dense_out": dense_out}


EPS = 1e-06
THETA = 10000.0

def store(values):
    return lax.optimization_barrier(values.astype(jnp.bfloat16))

def rope_table(places, width):
    inverse = THETA ** (-jnp.arange(0, width, 2, dtype=jnp.float32) / width)
    angles = places.astype(jnp.float32)[:, None] * inverse[None, :]
    angles = jnp.concatenate([angles, angles], axis=-1)
    return (jnp.cos(angles), jnp.sin(angles))

def turn(values, tables):
    cosine, sine = tables
    middle = values.shape[-1] // 2
    rotated = jnp.concatenate([-values[..., middle:], values[..., :middle]], axis=-1)
    return values * cosine[:, None, :] + rotated * sine[:, None, :]

def head_norm(projected, gain):
    width = gain.shape[0]
    heads = projected.reshape(projected.shape[0], -1, width)
    return heads * lax.rsqrt(lax.optimization_barrier(jnp.mean(heads * heads, axis=-1, keepdims=True)) + EPS) * gain

def line_heads(projected, gain, places):
    normed = head_norm(projected, gain)
    return turn(normed, rope_table(places, gain.shape[0])).reshape(projected.shape)

def grid_heads(projected, gain, places):
    normed = head_norm(projected, gain)
    middle = gain.shape[0] // 2
    by_row = turn(normed[..., :middle], rope_table(places // GRID_W, middle))
    by_col = turn(normed[..., middle:], rope_table(places % GRID_W, middle))
    return jnp.concatenate([by_row, by_col], axis=-1).reshape(projected.shape)

def banded(query, keys_ext, values_ext, offset, total_len, sink_logit):
    length = query.shape[0]
    kv_heads = keys_ext.shape[1] // HD
    group_size = query.shape[1] // (HD * kv_heads)
    block_count = length // WINDOW
    query_blocks = query.astype(jnp.float32).reshape(block_count, WINDOW, kv_heads, group_size, HD)
    key_blocks = keys_ext.astype(jnp.float32).reshape(block_count + 2, WINDOW, kv_heads, HD)
    value_blocks = values_ext.astype(jnp.float32).reshape(block_count + 2, WINDOW, kv_heads, HD)
    key_near = jnp.concatenate([key_blocks[:-2], key_blocks[1:-1], key_blocks[2:]], axis=1)
    value_near = jnp.concatenate([value_blocks[:-2], value_blocks[1:-1], value_blocks[2:]], axis=1)
    scores = jnp.einsum('nqhgd,nkhd->nhgqk', query_blocks, key_near) * HD ** (-0.5)
    query_pos = offset + jnp.arange(length, dtype=jnp.int32).reshape(block_count, WINDOW)
    key_pos = offset - WINDOW + (jnp.arange(block_count, dtype=jnp.int32)[:, None] * WINDOW + jnp.arange(3 * WINDOW, dtype=jnp.int32)[None, :])
    valid = (jnp.abs(query_pos[:, :, None] - key_pos[:, None, :]) <= WINDOW) & (key_pos >= 0)[:, None, :] & (key_pos < total_len)[:, None, :]
    scores = jnp.where(valid[:, None, None], scores, -jnp.inf)
    floor = sink_logit.reshape(kv_heads, group_size)[None, :, :, None, None]
    top = jnp.maximum(lax.optimization_barrier(jnp.max(scores, axis=-1, keepdims=True)), floor)
    expon = jnp.exp(scores - top)
    weights = store(expon / (lax.optimization_barrier(jnp.sum(expon, axis=-1, keepdims=True)) + jnp.exp(floor - top)))
    result = jnp.einsum('nhgqk,nkhd->nqhgd', weights.astype(jnp.float32), value_near)
    return result.reshape(length, -1)

def dense_attention(query, keys, values):
    length = query.shape[0]
    kv_heads = keys.shape[1] // HD
    group_size = query.shape[1] // (HD * kv_heads)
    if length % 256 == 0:
        block = 256
    elif length % 128 == 0:
        block = 128
    else:
        block = length
    query_blocks = query.astype(jnp.float32).reshape(length // block, block, kv_heads, group_size, HD)
    key_heads = keys.astype(jnp.float32).reshape(length, kv_heads, HD)
    value_heads = values.astype(jnp.float32).reshape(length, kv_heads, HD)

    def one_block(query_block):
        scores = jnp.einsum('qhgd,khd->hgqk', query_block, key_heads) * HD ** (-0.5)
        top = lax.optimization_barrier(jnp.max(scores, axis=-1, keepdims=True))
        expon = jnp.exp(scores - top)
        total = lax.optimization_barrier(jnp.sum(expon, axis=-1))
        rounded = store(expon).astype(jnp.float32)
        summed = jnp.einsum('hgqk,khd->qhgd', rounded, value_heads)
        return summed / jnp.transpose(total, (2, 0, 1))[..., None]
    result = lax.map(one_block, query_blocks)
    return result.reshape(length, -1)

def reference(tokens_in, norm_gain, window_query, window_key, window_value, window_query_gain, window_key_gain, sink_logit, dense_query, dense_key, dense_value, dense_query_gain, dense_key_gain, window_out, dense_out):
    inputs = tokens_in.astype(jnp.float32)
    normed = (inputs * lax.rsqrt(lax.optimization_barrier(jnp.mean(inputs * inputs, axis=-1, keepdims=True)) + EPS) * norm_gain).astype(jnp.bfloat16)

    def project(weight):
        return jnp.dot(normed, weight, preferred_element_type=jnp.float32)
    places = jnp.arange(TOKENS, dtype=jnp.int32)
    query_win = store(line_heads(project(window_query), window_query_gain, places))
    key_win = store(line_heads(project(window_key), window_key_gain, places))
    value_win = store(project(window_value))
    query_den = store(grid_heads(project(dense_query), dense_query_gain, places))
    key_den = store(grid_heads(project(dense_key), dense_key_gain, places))
    value_den = store(project(dense_value))
    margin = ((WINDOW, WINDOW), (0, 0))
    att_win = store(banded(query_win, jnp.pad(key_win, margin), jnp.pad(value_win, margin), 0, TOKENS, sink_logit))
    att_den = store(dense_attention(query_den, key_den, value_den))
    win_parts = att_win.reshape(TOKENS, N_TP, -1).transpose(1, 0, 2)
    den_parts = att_den.reshape(TOKENS, N_TP, -1).transpose(1, 0, 2)
    win_rows = window_out.reshape(N_TP, -1, D)
    den_rows = dense_out.reshape(N_TP, -1, D)

    def add_group(running, members):
        win_part, win_weight, den_part, den_weight = members
        partial_value = jnp.dot(win_part, win_weight, preferred_element_type=jnp.float32) + jnp.dot(den_part, den_weight, preferred_element_type=jnp.float32)
        return (running + store(partial_value).astype(jnp.float32), None)
    running, unused = lax.scan(add_group, jnp.zeros((TOKENS, D), jnp.float32), (win_parts, win_rows, den_parts, den_rows))
    return running.astype(jnp.bfloat16)
```

```python
import functools

import jax
import jax.numpy as jnp
import numpy as np
from jax import lax
from jax.experimental import pallas as pl
from jax.experimental.pallas import tpu as pltpu
from jax.sharding import PartitionSpec as P

HD = 64
WINDOW = 128
GRID_W = 64


EPS = 1e-06
THETA = 10000.0


MESH = pl.DeviceIdType.MESH
HALVES = 2


class LineGather:
    def __init__(self, own, buf, z_recv, r_send, l_send, y_recv=None, y_send=None, axis=0):
        self.own, self.buf = own, buf
        self.z_recv, self.y_recv = z_recv, y_recv
        self.r_send, self.l_send, self.y_send = r_send, l_send, y_send
        self.n = lax.axis_size("sp")
        self.s = lax.axis_index("sp")
        self.shared = y_recv is not None
        self.g = lax.axis_index("grp") if self.shared else 0
        self.chunks = z_recv.shape[1]
        self.axis = axis
        extent = buf.shape[1 + axis]
        self.half = extent // HALVES if self.shared else extent
        self.size = self.half // self.chunks

    def rows(self, half, c):
        piece = pl.ds(pl.multiple_of(half * self.half + c * self.size, self.size), self.size)
        return (piece,) if self.axis == 0 else (slice(None), piece)

    def block(self, o, half, c):
        return self.buf.at[(o,) + self.rows(half, c)]

    def copy(self, src, o, c, sem, recv, target, half):
        return pltpu.make_async_remote_copy(
            src_ref=src,
            dst_ref=self.block(o, half, c),
            send_sem=sem.at[o, c],
            recv_sem=recv.at[o, c],
            device_id=target,
            device_id_type=MESH,
        )

    def right(self, src, o, c):
        return self.copy(src, o, c, self.r_send, self.z_recv, {"sp": lax.rem(self.s + 1, self.n)}, self.g)

    def left(self, src, o, c):
        return self.copy(
            src, o, c, self.l_send, self.z_recv, {"sp": lax.rem(self.s + self.n - 1, self.n)}, self.g
        )

    def twin(self, o, c, half):
        return self.copy(
            self.block(o, half, c), o, c, self.y_send, self.y_recv, {"grp": 1 - self.g}, half
        )

    def mine(self, c):
        if self.own is None:
            return self.block(self.s, self.g, c)
        return self.own.at[self.rows(self.g, c)]

    def start(self, first=0, last=None):
        for c in range(first, self.chunks if last is None else last):
            mine = self.mine(c)

            @pl.when(self.s + 1 < self.n)
            def _():
                self.right(mine, self.s, c).start()

            @pl.when(self.s > 0)
            def _():
                self.left(mine, self.s, c).start()

    def forward(self, d):
        for c in range(self.chunks):

            @pl.when(self.s - d >= 0)
            def _():
                o = self.s - d
                there = self.block(o, self.g, c)
                self.right(there, o, c).wait_recv()

                @pl.when(self.s + 1 < self.n)
                def _():
                    self.right(there, o, c).start()

                if self.shared:
                    self.twin(o, c, self.g).start()

            @pl.when(self.s + d < self.n)
            def _():
                o = self.s + d
                there = self.block(o, self.g, c)
                self.left(there, o, c).wait_recv()

                @pl.when(self.s > 0)
                def _():
                    self.left(there, o, c).start()

                if self.shared:
                    self.twin(o, c, self.g).start()

    def use(self, d, fn, near=None):
        for there, o in ((self.s - d >= 0, self.s - d), (self.s + d < self.n, self.s + d)):
            if near is not None:

                @pl.when(there)
                def _():
                    near(o)

        for there, o in ((self.s - d >= 0, self.s - d), (self.s + d < self.n, self.s + d)):

            @pl.when(there)
            def _():
                for c in range(self.chunks):
                    self.twin(o, c, 1 - self.g).wait_recv()
                fn(o)

    def run(self, fn, near=None, last=None):
        self.forward(1)
        self.rest(fn, near, last)

    def rest(self, fn, near=None, last=None):
        @pl.loop(2, self.n)
        def _(d):
            self.forward(d)
            self.use(d - 1, fn, near)

        if last is not None:
            last()
        self.use(self.n - 1, fn, near)

    def finish(self):
        @pl.loop(0, self.n)
        def _(o):
            for c in range(self.chunks):
                there = self.block(o, self.g, c)

                @pl.when((o <= self.s) & (self.s + 1 < self.n))
                def _():
                    self.right(there, o, c).wait_send()

                @pl.when((o >= self.s) & (self.s > 0))
                def _():
                    self.left(there, o, c).wait_send()

                if self.shared:

                    @pl.when(o != self.s)
                    def _():
                        self.twin(o, c, self.g).wait_send()


def greet():
    n, s, g = lax.axis_size("sp"), lax.axis_index("sp"), lax.axis_index("grp")
    n_tp, t = lax.axis_size("tp"), lax.axis_index("tp")
    barrier = pltpu.get_barrier_semaphore()
    pl.semaphore_signal(barrier, inc=1, device_id={"grp": 1 - g}, device_id_type=MESH)
    for j in range(1, n_tp):
        pl.semaphore_signal(barrier, inc=1, device_id={"tp": lax.rem(t + j, n_tp)}, device_id_type=MESH)

    @pl.when(s + 1 < n)
    def _():
        pl.semaphore_signal(barrier, inc=1, device_id={"sp": lax.rem(s + 1, n)}, device_id_type=MESH)

    @pl.when(s > 0)
    def _():
        pl.semaphore_signal(barrier, inc=1, device_id={"sp": lax.rem(s + n - 1, n)}, device_id_type=MESH)

    pl.semaphore_wait(barrier, n_tp + (s + 1 < n).astype(jnp.int32) + (s > 0).astype(jnp.int32))


LANES = 128


def by_half(low, high):
    lane = lax.broadcasted_iota(jnp.int32, low.shape, 1)
    return jnp.where(lane < HD, low, high)


def swap_pairs(values, reach):
    lane = lax.broadcasted_iota(jnp.int32, values.shape, 1)
    ahead = pltpu.roll(values, LANES - reach, 1)
    behind = pltpu.roll(values, reach, 1)
    return jnp.where(lax.rem(lane, 2 * reach) < reach, ahead, behind)


def head_tile(tile, kinds, gains_ref, tables_ref):
    square = tile * tile
    zero = jnp.zeros_like(square)
    low = jnp.sum(by_half(square, zero), axis=-1, keepdims=True)
    high = jnp.sum(by_half(zero, square), axis=-1, keepdims=True)
    mean = by_half(jnp.broadcast_to(low, tile.shape), jnp.broadcast_to(high, tile.shape)) * (1.0 / HD)
    scaled = tile * lax.rsqrt(mean + EPS)

    def one(kind):
        if kind is None:
            return tile
        gain, table, reach = kind
        normed = scaled * gains_ref[gain : gain + 1, :]
        return normed * tables_ref[2 * table] + swap_pairs(normed, reach) * tables_ref[2 * table + 1]

    if kinds[0] == kinds[1]:
        return one(kinds[0])
    return by_half(one(kinds[0]), one(kinds[1]))


def layer_kernel(
    sizes, x_ref, gain_ref, fixed_ref, g0, g1, g2, g3, sink_ref, *refs
):
    n_in = sizes[2]
    in_refs, out_refs = refs[:n_in], refs[n_in : n_in + 2]
    run_layer(sizes[:2], x_ref, gain_ref, fixed_ref, (g0, g1, g2, g3), sink_ref, in_refs, out_refs, *refs[n_in + 2 :])


def run_layer(
    sizes, x_ref, gain_ref, fixed_ref, head_gains, sink_ref, in_refs, out_refs, out_ref,
    small_ref, w_ref, wo_ref, tables_ref, load_sem, xn, proj, wbuf, wo_all, kvd, ext, qs, att, part, rs, halo_recv, halo_send, rs_recv, rs_send, *sems
):
    q_heads, kv_heads = sizes
    n, s = lax.axis_size("sp"), lax.axis_index("sp")
    n_tp, t = lax.axis_size("tp"), lax.axis_index("tp")
    depth = w_ref.shape[0]
    length = x_ref.shape[0]
    into = LineGather(w_ref, wbuf, *sems[:5])
    out = LineGather(wo_ref, wo_all, *sems[5:10], axis=1)
    keys = LineGather(None, kvd, *sems[10:])
    loads, at = [], 0
    for ref in in_refs:
        wide = ref.shape[1]
        loads.append(
            pltpu.make_async_copy(ref, w_ref.at[:, at : at + wide], load_sem.at[len(loads)])
        )
        at += wide
    at = 0
    for ref in out_refs:
        tall = ref.shape[0]
        loads.append(pltpu.make_async_copy(ref, wo_ref.at[at : at + tall], load_sem.at[len(loads)]))
        at += tall
    for load in loads:
        load.start()
    greet()
    for load in loads:
        load.wait()
    into.start()

    for k, ref in enumerate(head_gains):
        small_ref[k : k + 1, :] = jnp.concatenate([ref[...], ref[...]], axis=1)
    small_ref[4:8, :] = fixed_ref[...]
    step = 16

    @pl.loop(0, length // step)
    def _(i):
        rows = pl.ds(pl.multiple_of(i * step, step), step)
        values = x_ref[rows, :].astype(jnp.float32)
        mean = jnp.mean(values * values, axis=-1, keepdims=True)
        xn[rows, :] = (values * lax.rsqrt(mean + EPS) * gain_ref[...]).astype(jnp.bfloat16)

    def columns(o):
        return pl.ds(pl.multiple_of(o * depth, depth), depth)

    proj[...] = jnp.dot(xn[:, columns(s)], w_ref[...], preferred_element_type=jnp.float32)

    band = 64 if length % 64 == 0 else length

    @pl.loop(0, length // band)
    def _(i):
        rows = pl.ds(pl.multiple_of(i * band, band), band)
        shape = (band, LANES)
        place = lax.broadcasted_iota(jnp.int32, shape, 0) + (s * length + i * band)
        lane = lax.broadcasted_iota(jnp.int32, shape, 1)
        spot = jnp.where(lax.rem(lane, HD) < HD // 2, place // GRID_W, lax.rem(place, GRID_W))
        for k, where in enumerate((place, spot)):
            angles = where.astype(jnp.float32) * small_ref[4 + k : 5 + k, :]
            tables_ref[2 * k, rows, :] = jnp.cos(angles)
            tables_ref[2 * k + 1, rows, :] = jnp.sin(angles) * small_ref[6 + k : 7 + k, :]

    def add(o):
        proj[...] += jnp.dot(xn[:, columns(o)], wbuf[o], preferred_element_type=jnp.float32)

    into.run(add, last=lambda: out.start(0, 1))

    win_q, win_k, den_q, den_k = (0, 0, 32), (1, 0, 32), (2, 1, 16), (3, 1, 16)
    kinds = (
        [win_q] * q_heads + [den_q] * q_heads + [den_k] * kv_heads + [None] * kv_heads
        + [win_k] * kv_heads + [None] * kv_heads
    )
    q_tiles = 2 * q_heads * HD // LANES
    kv_tiles = 2 * kv_heads * HD // LANES

    def finished(i):
        return head_tile(
            proj[:, i * LANES : (i + 1) * LANES], kinds[2 * i : 2 * i + 2], small_ref, tables_ref
        )

    for i in range(kv_tiles):
        ext[WINDOW : WINDOW + length, i * LANES : (i + 1) * LANES] = finished(
            q_tiles + kv_tiles + i
        ).astype(jnp.bfloat16)
    for i in range(kv_tiles):
        kvd[s, :, i * LANES : (i + 1) * LANES] = finished(q_tiles + i).astype(jnp.bfloat16)

    def halo(side):
        source = pl.ds(length, WINDOW) if side == 0 else pl.ds(WINDOW, WINDOW)
        target = pl.ds(0, WINDOW) if side == 0 else pl.ds(WINDOW + length, WINDOW)
        peer = lax.rem(s + 1, n) if side == 0 else lax.rem(s + n - 1, n)
        return pltpu.make_async_remote_copy(
            src_ref=ext.at[source], dst_ref=ext.at[target], send_sem=halo_send.at[side],
            recv_sem=halo_recv.at[side], device_id={"sp": peer}, device_id_type=MESH,
        )

    has_right, has_left = s + 1 < n, s > 0

    @pl.when(has_right)
    def _():
        halo(0).start()

    @pl.when(has_left)
    def _():
        halo(1).start()

    keys.start()
    none = jnp.zeros((WINDOW, ext.shape[1]), jnp.bfloat16)

    @pl.when(jnp.logical_not(has_left))
    def _():
        ext[0:WINDOW, :] = none

    @pl.when(jnp.logical_not(has_right))
    def _():
        ext[WINDOW + length : WINDOW + length + WINDOW, :] = none

    group = q_heads // kv_heads

    def place(head):
        return head // 2, head % 2

    for i in range(q_tiles):
        tile = finished(i) * HD ** (-0.5)
        for b in range(2):
            head = 2 * i + b
            half = place((head % q_heads) // group)[1]
            moved = tile if half == b else pltpu.roll(tile, HD, 1)
            zero = jnp.zeros_like(moved)
            kept = by_half(moved, zero) if half == 0 else by_half(zero, moved)
            qs[head] = kept.astype(jnp.bfloat16)

    @pl.when(has_left)
    def _():
        halo(0).wait_recv()

    @pl.when(has_right)
    def _():
        halo(1).wait_recv()

    total_len = length * n

    def joined(results, heads):
        placed = []
        for b in range(2):
            half = place(kv_heads + heads[b] // group)[1]
            placed.append(results[b] if half == b else pltpu.roll(results[b], HD, 1))
        return by_half(placed[0], placed[1]).astype(jnp.bfloat16)

    def tile_of(head):
        return pl.ds(place(head)[0] * LANES, LANES)

    nt = (((1,), (1,)), ((), ()))

    def windowed(pair):
        @pl.loop(0, length // WINDOW)
        def _(b):
            base = pl.multiple_of(b * WINDOW, WINDOW)
            rows = pl.ds(base, WINDOW)
            near = pl.ds(base, 3 * WINDOW)
            shape = (WINDOW, 3 * WINDOW)
            at = lax.broadcasted_iota(jnp.int32, shape, 1) - WINDOW
            away = at - lax.broadcasted_iota(jnp.int32, shape, 0)
            pos = at + (s * length + base)
            valid = (away <= WINDOW) & (away >= -WINDOW) & (pos >= 0) & (pos < total_len)
            results = []
            for head in (2 * pair, 2 * pair + 1):
                key = ext[near, tile_of(head // group)]
                value = ext[near, tile_of(kv_heads + head // group)]
                scores = lax.dot_general(qs[head, rows, :], key, nt, preferred_element_type=jnp.float32)
                scores = jnp.where(valid, scores, -jnp.inf)
                floor = sink_ref[0, head]
                top = jnp.maximum(jnp.max(scores, axis=-1, keepdims=True), floor)
                expon = jnp.exp(scores - top)
                total = jnp.sum(expon, axis=-1, keepdims=True) + jnp.exp(floor - top)
                weights = (expon / total).astype(jnp.bfloat16)
                results.append(jnp.dot(weights, value, preferred_element_type=jnp.float32))
            att[rows, pair * LANES : (pair + 1) * LANES] = joined(results, (2 * pair, 2 * pair + 1))

    pairs = q_heads // 2
    keys.forward(1)
    windowed(0)

    @pl.loop(2, n)
    def _(d):
        keys.forward(d)

    out.start(1)
    for pair in range(1, pairs):
        windowed(pair)

    def dense(pair):
        @pl.loop(0, length // LANES)
        def _(b):
            rows = pl.ds(pl.multiple_of(b * LANES, LANES), LANES)
            results = []
            for head in (2 * pair, 2 * pair + 1):
                key = kvd[:, :, tile_of(head // group)].reshape(total_len, LANES)
                value = kvd[:, :, tile_of(kv_heads + head // group)].reshape(total_len, LANES)
                scores = lax.dot_general(
                    qs[q_heads + head, rows, :], key, nt, preferred_element_type=jnp.float32
                )
                top = jnp.max(scores, axis=-1, keepdims=True)
                expon = jnp.exp(scores - top)
                total = jnp.sum(expon, axis=-1, keepdims=True)
                summed = jnp.dot(
                    expon.astype(jnp.bfloat16), value, preferred_element_type=jnp.float32
                )
                results.append(summed / total)
            at = (pairs + pair) * LANES
            att[rows, at : at + LANES] = joined(results, (2 * pair, 2 * pair + 1))

    dense(0)
    out.forward(1)
    for pair in range(1, pairs):
        dense(pair)

    share = length // n_tp

    wide = wo_ref.shape[1]
    part_cols = wide // HALVES
    mine = lax.axis_index("grp")

    def span(h):
        return pl.ds(pl.multiple_of(h * part_cols, part_cols), part_cols)

    def exchange(o, h, j):
        peer = lax.rem(t + j, n_tp)
        return pltpu.make_async_remote_copy(
            src_ref=part.at[o, pl.ds(pl.multiple_of(peer * share, share), share), span(h)],
            dst_ref=rs.at[t, o, :, span(h)], send_sem=rs_send.at[j - 1, o, h],
            recv_sem=rs_recv.at[t, o, h], device_id={"tp": peer}, device_id_type=MESH,
        )

    def arrived(o, h, j):
        source = lax.rem(t + n_tp - j, n_tp)
        there = rs.at[source, o, :, span(h)]
        return pltpu.make_async_remote_copy(
            src_ref=there, dst_ref=there, send_sem=rs_send.at[j - 1, o, h],
            recv_sem=rs_recv.at[source, o, h], device_id={"tp": source}, device_id_type=MESH,
        )

    def emit(o, h, weight):
        part[o, :, span(h)] = jnp.dot(
            att[...], weight, preferred_element_type=jnp.float32
        ).astype(jnp.bfloat16)
        for j in range(1, n_tp):
            exchange(o, h, j).start()
        rs[t, o, :, span(h)] = part[o, pl.ds(pl.multiple_of(t * share, share), share), span(h)]

    def collect(o, h):
        for j in range(1, n_tp):
            arrived(o, h, j).wait_recv()
        total = rs[0, o, :, span(h)].astype(jnp.float32)
        for g in range(1, n_tp):
            total += rs[g, o, :, span(h)].astype(jnp.float32)
        columns_out = pl.ds(pl.multiple_of(o * wide + h * part_cols, part_cols), part_cols)
        out_ref[:, columns_out] = total.astype(jnp.bfloat16)

    for h in range(HALVES):
        emit(s, h, wo_ref[:, span(h)])
    out.rest(
        lambda o: emit(o, 1 - mine, wo_all[o, :, span(1 - mine)]),
        near=lambda o: emit(o, mine, wo_all[o, :, span(mine)]),
    )

    @pl.loop(0, n)
    def _(d):
        o = lax.rem(s + d, n)
        for h in range(HALVES):
            collect(o, h)

    @pl.loop(0, n)
    def _(o):
        for h in range(HALVES):
            for j in range(1, n_tp):
                exchange(o, h, j).wait_send()

    @pl.when(has_right)
    def _():
        halo(0).wait_send()

    @pl.when(has_left)
    def _():
        halo(1).wait_send()

    into.finish()
    out.finish()
    keys.finish()


def local_ring(
    tokens_in,
    norm_gain,
    window_query,
    window_key,
    window_value,
    window_query_gain,
    window_key_gain,
    sink_logit,
    dense_query,
    dense_key,
    dense_value,
    dense_query_gain,
    dense_key_gain,
    window_out,
    dense_out,
):
    length, width = tokens_in.shape
    n, n_tp = lax.axis_size("sp"), lax.axis_size("tp")
    q_heads, kv_heads = window_query.shape[1] // HD, window_key.shape[1] // HD
    weights, held = [], []
    for weight in (window_query, dense_query, dense_key, dense_value, window_key, window_value):
        held.append(weight)
        if sum(w.shape[1] for w in held) % LANES == 0:
            weights.append(held[0] if len(held) == 1 else jnp.concatenate(held, axis=1))
            held = []
    depth, in_cols = window_query.shape[0], sum(w.shape[1] for w in weights)
    out_rows, out_cols = window_out.shape[0] + dense_out.shape[0], window_out.shape[1]

    lane = np.arange(LANES)
    fixed = np.stack(
        [THETA ** (-2.0 * (lane % (wide // 2)) / wide) for wide in (HD, HD // 2)]
        + [np.where(lane % wide < wide // 2, -1.0, 1.0) for wide in (HD, HD // 2)]
    ).astype(np.float32)
    gains = [g[None, :] for g in (window_query_gain, window_key_gain, dense_query_gain, dense_key_gain)]

    def gather(chunks):
        return [pltpu.SemaphoreType.DMA((n, chunks)) for _ in range(5)]

    in_chunks = 8 if n <= 4 else 1
    out_chunks = out_cols // HALVES // LANES if n <= 4 else 1
    kv_cols = 2 * kv_heads * HD
    vmem = pl.BlockSpec(memory_space=pltpu.VMEM)
    share = length // n_tp
    return pl.pallas_call(
        functools.partial(layer_kernel, (q_heads, kv_heads, len(weights))),
        out_shape=jax.ShapeDtypeStruct((share, width), jnp.bfloat16),
        in_specs=[vmem] * 7
        + [pl.BlockSpec(memory_space=pltpu.SMEM)]
        + [pl.BlockSpec(memory_space=pl.ANY)] * (len(weights) + 2),
        out_specs=vmem,
        scratch_shapes=[
            pltpu.VMEM((8, LANES), jnp.float32),
            pltpu.VMEM((depth, in_cols), jnp.bfloat16),
            pltpu.VMEM((out_rows, out_cols), jnp.bfloat16),
            pltpu.VMEM((4, length, LANES), jnp.float32),
            pltpu.SemaphoreType.DMA((len(weights) + 2,)),
            pltpu.VMEM((length, width), jnp.bfloat16),
            pltpu.VMEM((length, in_cols), jnp.float32),
            pltpu.VMEM((n, depth, in_cols), jnp.bfloat16),
            pltpu.VMEM((n, out_rows, out_cols), jnp.bfloat16),
            pltpu.VMEM((n, length, kv_cols), jnp.bfloat16),
            pltpu.VMEM((length + 2 * WINDOW, kv_cols), jnp.bfloat16),
            pltpu.VMEM((2 * q_heads, length, LANES), jnp.bfloat16),
            pltpu.VMEM((length, out_rows), jnp.bfloat16),
            pltpu.VMEM((n, length, out_cols), jnp.bfloat16),
            pltpu.VMEM((n_tp, n, share, out_cols), jnp.bfloat16),
            pltpu.SemaphoreType.DMA((2,)),
            pltpu.SemaphoreType.DMA((2,)),
            pltpu.SemaphoreType.DMA((n_tp, n, HALVES)),
            pltpu.SemaphoreType.DMA((n_tp - 1, n, HALVES)),
        ]
        + gather(in_chunks)
        + gather(out_chunks)
        + [pltpu.SemaphoreType.DMA((n, 2 if n <= 4 else 1)) for _ in range(3)],
        compiler_params=pltpu.CompilerParams(
            collective_id=0, has_side_effects=True, vmem_limit_bytes=62 * 1024 * 1024
        ),
    )(tokens_in, norm_gain[None, :], fixed, *gains, sink_logit[None, :], *weights, window_out, dense_out)


KINDS = 4
SHARED = (True, True, False, False)
ROWS = 128


def pair_kernel(sizes, *refs):
    gain_ref, fixed_ref, g0, g1, g2, g3, sink_ref, x_hbm = refs[:8]
    weights, outs, out_hbm = refs[8:14], refs[14:16], refs[16]
    run_pairs(sizes, gain_ref, fixed_ref, (g0, g1, g2, g3), sink_ref, x_hbm, weights, outs, out_hbm, *refs[17:])


def run_pairs(
    sizes, gain_ref, fixed_ref, head_gains, sink_ref, x_hbm, weights, outs, out_hbm,
    small_ref, tables_ref, xv, xn, wbuf, wo, proj, kvd, ext, extm, qc, qm, qs, att, part, dbuf, xsend, xrecv, ostage,
    load_sem, store_sem, zs, zr, ys, yr, wis, wzr, wos, wys, wyr,
    xzs, xzr, xxs, xxr, xds, xdr, xes, xer, kis, kos, kr, es, er, qsn, qr, ds, dr, rxs, rxr,
):
    q_heads, kv_heads = sizes
    n, s = lax.axis_size("sp"), lax.axis_index("sp")
    n_tp, t = lax.axis_size("tp"), lax.axis_index("tp")
    g = lax.axis_index("grp")
    length, width = xv.shape
    depth, cols = wbuf.shape[2], wbuf.shape[3]
    out_rows, out_cols = wo.shape[1], wo.shape[2]
    share = length // n_tp
    chunks, out_chunks = zs.shape[3], wis.shape[2]
    low = 2 * s < n
    high = jnp.logical_not(low)
    inner = (s > 0) & (s < n - 1)
    outer = jnp.logical_not(inner)
    step = jnp.where(low, 1, -1)
    inward = s + step
    outward = lax.rem(s - step + n, n)
    core, chip = lax.rem(t, 2), t // 2
    twin = t + 1 - 2 * core
    across = lax.rem(t + 2, n_tp)
    diagonal = lax.rem(twin + 2, n_tp)

    def place_of(j):
        if j == 0:
            return s
        return jnp.where(inner, (s - step, s - step, s + step, s + 2 * step)[j], s + j * step)

    sent = []

    def remote(when, ends):
        def build():
            src, dst, send, recv, peer = ends()
            return pltpu.make_async_remote_copy(
                src_ref=src, dst_ref=dst, send_sem=send, recv_sem=recv, device_id=peer, device_id_type=MESH
            )

        sent.append((when, build))
        build().start()

    def landed(ref, sem, peer):
        pltpu.make_async_remote_copy(
            src_ref=ref, dst_ref=ref, send_sem=sem, recv_sem=sem, device_id=peer, device_id_type=MESH
        ).wait_recv()

    z_in, z_out, y_peer = {"sp": inward}, {"sp": outward}, {"grp": 1 - g}

    half = depth // HALVES
    size = half // chunks

    def w_at(k, slot, rel, c):
        h = g if rel == 0 else 1 - g
        return wbuf.at[k, slot, pl.ds(pl.multiple_of(h * half + c * size, size), size)]

    def w_inward(role, k, slot, rel, c):
        to = 1 if role == "outer" else slot + 2
        remote(role, lambda: (
            w_at(k, slot, rel, c), w_at(k, to, rel, c), zs.at[k, slot, rel, c], zr.at[k, to, rel, c], z_in
        ))

    def w_landed(k, slot, rel, c):
        landed(w_at(k, slot, rel, c), zr.at[k, slot, rel, c], z_out if slot == 1 else z_in)

    def w_twin(k, slot, c):
        remote("inner", lambda: (
            w_at(k, slot, 0, c), w_at(k, slot, 0, c), ys.at[k, slot, c], yr.at[k, slot, c], y_peer
        ))

    def w_twin_landed(k, slot, c):
        landed(w_at(k, slot, 1, c), yr.at[k, slot, c], y_peer)

    out_half = out_cols // HALVES
    out_size = out_half // out_chunks

    def o_at(slot, rel, c):
        h = g if rel == 0 else 1 - g
        return wo.at[slot, :, pl.ds(pl.multiple_of(h * out_half + c * out_size, out_size), out_size)]

    def o_inward(role, slot, rel, c):
        to = 1 if role == "outer" else slot + 2
        remote(role, lambda: (
            o_at(slot, rel, c), o_at(to, rel, c), wis.at[slot, rel, c], wzr.at[to, rel, c], z_in
        ))

    def o_outward(slot, c):
        to = 1 if slot == 0 else slot
        remote("inner", lambda: (
            o_at(slot, 0, c), o_at(to, 0, c), wos.at[slot, c], wzr.at[to, 0, c], z_out
        ))

    def o_landed(slot, rel, c, peer):
        landed(o_at(slot, rel, c), wzr.at[slot, rel, c], peer)

    def o_twin(role, slot, c):
        remote(role, lambda: (o_at(slot, 0, c), o_at(slot, 0, c), wys.at[slot, c], wyr.at[slot, c], y_peer))

    def o_twin_landed(slot, c):
        landed(o_at(slot, 1, c), wyr.at[slot, c], y_peer)

    def x_rows(quarter):
        return pl.ds(pl.multiple_of(length + quarter * share, share), share)

    def x_cols(p):
        return pl.ds(p * depth, depth)

    def x_relay(p):
        def piece():
            return xn.at[x_rows(t), x_cols(p)]

        landed(piece(), xzr.at[p], z_out)
        remote("inner", lambda: (piece(), piece(), xxs.at[p], xxr.at[p], {"tp": across}))
        remote("inner", lambda: (piece(), piece(), xds.at[p], xdr.at[p], {"tp": twin}))

    def x_pass(p):
        def piece():
            return xn.at[x_rows(across), x_cols(p)]

        landed(piece(), xxr.at[p], {"tp": across})
        remote("inner", lambda: (piece(), piece(), xes.at[p], xer.at[p], {"tp": twin}))

    def x_all(p):
        landed(xn.at[x_rows(twin), x_cols(p)], xdr.at[p], {"tp": twin})
        landed(xn.at[x_rows(diagonal), x_cols(p)], xer.at[p], {"tp": twin})

    kv_cols = cols // 2
    loads = []

    def load(src, dst):
        copy = pltpu.make_async_copy(src, dst, load_sem.at[len(loads)])
        loads.append(copy)
        copy.start()

    wq, dq, dk, dv, wk, wv = weights
    load(dk, wbuf.at[0, 0, :, 0:kv_cols])
    load(dv, wbuf.at[0, 0, :, kv_cols:cols])
    load(x_hbm, xv)
    load(dq, wbuf.at[1, 0])
    load(wk, wbuf.at[2, 0, :, 0:kv_cols])
    load(wv, wbuf.at[2, 0, :, kv_cols:cols])
    load(wq, wbuf.at[3, 0])
    rows_of = outs[0].shape[0]
    load(outs[0], wo.at[0, 0:rows_of])
    load(outs[1], wo.at[0, rows_of:out_rows])
    greet()

    all_chunks, all_out = range(chunks), range(out_chunks)
    loads[0].wait()
    loads[1].wait()

    for role, test in (("inner", inner), ("outer", outer)):

        @pl.when(test)
        def _():
            for c in all_chunks:
                w_inward(role, 0, 0, 0, c)

    for k, ref in enumerate(head_gains):
        small_ref[k : k + 1, :] = jnp.concatenate([ref[...], ref[...]], axis=1)
    small_ref[4:8, :] = fixed_ref[...]
    loads[2].wait()

    def normalize(first, count):
        stripe = 16

        @pl.loop(0, count // stripe)
        def _(i):
            at = pl.multiple_of(i * stripe, stripe)
            values = xv[pl.ds(first + at, stripe), :].astype(jnp.float32)
            mean = jnp.mean(values * values, axis=-1, keepdims=True)
            xn[pl.ds(at, stripe), :] = (values * lax.rsqrt(mean + EPS) * gain_ref[...]).astype(jnp.bfloat16)

    band = 64

    def tables(first, count):
        @pl.loop(0, count // band)
        def _(i):
            at = pl.multiple_of(i * band, band) + first
            rows = pl.ds(at, band)
            shape = (band, LANES)
            base = jnp.where(at < length, s * length + at, (s - step) * length + at - length)
            place = lax.broadcasted_iota(jnp.int32, shape, 0) + base
            lane = lax.broadcasted_iota(jnp.int32, shape, 1)
            spot = jnp.where(lax.rem(lane, HD) < HD // 2, place // GRID_W, lax.rem(place, GRID_W))
            for k, where in enumerate((place, spot)):
                angles = where.astype(jnp.float32) * small_ref[4 + k : 5 + k, :]
                tables_ref[2 * k, rows, :] = jnp.cos(angles)
                tables_ref[2 * k + 1, rows, :] = jnp.sin(angles) * small_ref[6 + k : 7 + k, :]

    def project(k, j):
        at = pl.multiple_of(place_of(j) * depth, depth)

        @pl.loop(0, 2)
        def _(i):
            rows = pl.ds(pl.multiple_of(i * length, length), length)
            found = jnp.dot(xn[rows, pl.ds(at, depth)], wbuf[k, j], preferred_element_type=jnp.float32)
            proj[rows, :] = found if j == 0 else proj[rows, :] + found

    den_q, den_k, win_q, win_k = (2, 1, 16), (3, 1, 16), (0, 0, 32), (1, 0, 32)
    plans = ((den_k, None), (den_q, den_q), (win_k, None), (win_q, win_q))
    targets = ((kvd.at[0], kvd.at[1]), (qc.at[0], qm.at[0]), (ext.at[pl.ds(WINDOW, length)], extm), (qc.at[1], qm.at[1]))

    def finished(k):
        for side, target in enumerate(targets[k]):

            @pl.loop(0, length // ROWS)
            def _(i):
                at = pl.multiple_of(i * ROWS, ROWS)
                rows = pl.ds(side * length + at, ROWS)
                for tile in range(cols // LANES):
                    lanes = pl.ds(tile * LANES, LANES)
                    kind = plans[k][tile * 2 * LANES // cols]
                    value = proj[rows, lanes]
                    if kind is not None:
                        value = head_tile(
                            value, (kind, kind), small_ref,
                            [tables_ref.at[m][rows, :] for m in range(4)],
                        )
                        if k % 2:
                            value = value * HD ** (-0.5)
                    target[pl.ds(at, ROWS), lanes] = value.astype(jnp.bfloat16)

    def mates(k, c):
        w_landed(k, 1, 0, c)
        w_inward("inner", k, 1, 0, c)
        if SHARED[k]:
            w_twin(k, 1, c)

    def crossing(k, slot, c):
        w_landed(k, slot, 0, c)
        w_twin(k, slot, c)

    def mate_ready(k):
        for c in all_chunks:
            if SHARED[k]:
                w_twin_landed(k, 1, c)
            else:
                w_landed(k, 1, 1, c)

    def twin_ready(k, slot):
        for c in all_chunks:
            w_twin_landed(k, slot, c)

    def o_mates(c):
        o_landed(1, 0, c, z_out)
        o_inward("inner", 1, 0, c)

    def o_crossing(slot, c):
        o_landed(slot, 0, c, z_in)
        o_outward(slot, c)
        o_twin("inner", slot, c)

    def o_outer(slot, c):
        o_landed(slot, 0, c, z_in)
        o_twin("outer", slot, c)

    def edge(first):
        return pl.ds(jnp.where(first, WINDOW, length), WINDOW)

    def halo_at(leading):
        return pl.ds(jnp.where(leading, 0, WINDOW + length), WINDOW)

    def kv_landed(j, peer):
        landed(kvd.at[j], kr.at[j], peer)

    def kv_outward(j):
        remote("inner", lambda: (kvd.at[j], kvd.at[j], kos.at[j], kr.at[j], z_out))

    def kv_inward(j):
        remote("inner", lambda: (kvd.at[j], kvd.at[j + 2], kis.at[j], kr.at[j + 2], z_in))

    def x_inward(p):
        remote("outer", lambda: (
            xn.at[0:share, x_cols(p)], xn.at[x_rows(t), x_cols(p)], xzs.at[p], xzr.at[p], z_in
        ))

    def q_outward(a):
        remote("inner", lambda: (qm.at[a], qc.at[a], qsn.at[a], qr.at[a], z_out))

    @pl.when(outer)
    def _():
        normalize(t * share, share)
        for p in range(width // depth):
            x_inward(p)
        for one in loads[3:]:
            one.wait()
        for k in range(1, KINDS):
            for rel in range(1 if SHARED[k] else 2):
                for c in all_chunks:
                    w_inward("outer", k, 0, rel, c)
        for rel in range(2):
            for c in all_out:
                o_inward("outer", 0, rel, c)
        for c in all_out:
            o_outer(1, c)
        none = jnp.zeros((WINDOW, cols), jnp.bfloat16)
        ext[halo_at(low), :] = none
        for j in range(2):
            kv_landed(j, z_in)
        landed(qc.at[0], qr.at[0], z_in)
        for j in range(2, 4):
            kv_landed(j, z_in)

    @pl.when(inner)
    def _():
        for one in loads[3:]:
            one.wait()
        for c in all_out:
            o_outward(0, c)
        normalize(0, length)
        for c in all_chunks:
            mates(0, c)
            crossing(0, 2, c)
        for k in range(1, KINDS):
            for c in all_chunks:
                w_inward("inner", k, 0, 0, c)
        tables(0, length)
        for c in all_chunks:
            crossing(0, 3, c)
        x_relay(0)
        tables(length, length)
        crossing(1, 2, 0)
        x_relay(1)
        crossing(1, 2, 1)
        x_pass(0)
        x_relay(2)
        crossing(2, 2, 0)
        x_pass(1)
        x_relay(3)
        crossing(2, 2, 1)
        x_pass(2)
        crossing(3, 2, 0)
        mates(1, 0)
        x_pass(3)
        crossing(3, 2, 1)
        mates(1, 1)
        for p in range(width // depth):
            x_all(p)
        project(0, 0)
        mate_ready(0)
        project(0, 1)
        twin_ready(0, 2)
        project(0, 2)
        twin_ready(0, 3)
        project(0, 3)
        finished(0)
        for j in range(2):
            kv_inward(j)
            kv_outward(j)
        for c in all_chunks:
            mates(2, c)
            crossing(1, 3, c)
        project(1, 0)
        mate_ready(1)
        project(1, 1)
        twin_ready(1, 2)
        project(1, 2)
        twin_ready(1, 3)
        project(1, 3)
        finished(1)
        q_outward(0)
        for j in range(2, 4):
            kv_landed(j, z_in)
            kv_outward(j)
        for c in all_chunks:
            mates(3, c)
        for c in all_out:
            o_inward("inner", 0, 0, c)
        project(2, 0)
        for c in all_chunks:
            crossing(2, 3, c)

    group = q_heads // kv_heads

    def spot_of(head):
        return head // 2, head % 2

    q_tiles = q_heads * HD // LANES

    def expand(a):
        for i in range(q_tiles):
            tile = qc[a, :, i * LANES : (i + 1) * LANES].astype(jnp.float32)
            for b in range(2):
                head = 2 * i + b
                side = spot_of(head // group)[1]
                moved = tile if side == b else pltpu.roll(tile, HD, 1)
                zero = jnp.zeros_like(moved)
                kept = by_half(moved, zero) if side == 0 else by_half(zero, moved)
                qs[head] = kept.astype(jnp.bfloat16)

    total_len = length * n

    def joined(results, heads):
        placed = []
        for b in range(2):
            side = spot_of(kv_heads + heads[b] // group)[1]
            placed.append(results[b] if side == b else pltpu.roll(results[b], HD, 1))
        return by_half(placed[0], placed[1]).astype(jnp.bfloat16)

    def tile_of(head):
        return pl.ds(spot_of(head)[0] * LANES, LANES)

    nt = (((1,), (1,)), ((), ()))
    pairs = q_heads // 2

    def windowed(pair):
        @pl.loop(0, length // WINDOW)
        def _(b):
            base = pl.multiple_of(b * WINDOW, WINDOW)
            rows = pl.ds(base, WINDOW)
            near = pl.ds(base, 3 * WINDOW)
            shape = (WINDOW, 3 * WINDOW)
            at = lax.broadcasted_iota(jnp.int32, shape, 1) - WINDOW
            away = at - lax.broadcasted_iota(jnp.int32, shape, 0)
            pos = at + (s * length + base)
            valid = (away <= WINDOW) & (away >= -WINDOW) & (pos >= 0) & (pos < total_len)
            results = []
            for head in (2 * pair, 2 * pair + 1):
                key = ext[near, tile_of(head // group)]
                value = ext[near, tile_of(kv_heads + head // group)]
                scores = lax.dot_general(qs[head, rows, :], key, nt, preferred_element_type=jnp.float32)
                scores = jnp.where(valid, scores, -jnp.inf)
                floor = sink_ref[0, head]
                top = jnp.maximum(jnp.max(scores, axis=-1, keepdims=True), floor)
                expon = jnp.exp(scores - top)
                total = jnp.sum(expon, axis=-1, keepdims=True) + jnp.exp(floor - top)
                weight = (expon / total).astype(jnp.bfloat16)
                results.append(jnp.dot(weight, value, preferred_element_type=jnp.float32))
            att[rows, pair * LANES : (pair + 1) * LANES] = joined(results, (2 * pair, 2 * pair + 1))

    def dense(pair):
        @pl.loop(0, length // LANES)
        def _(b):
            rows = pl.ds(pl.multiple_of(b * LANES, LANES), LANES)
            results = []
            for head in (2 * pair, 2 * pair + 1):
                key = kvd[:, :, tile_of(head // group)].reshape(total_len, LANES)
                value = kvd[:, :, tile_of(kv_heads + head // group)].reshape(total_len, LANES)
                scores = lax.dot_general(qs[head, rows, :], key, nt, preferred_element_type=jnp.float32)
                top = jnp.max(scores, axis=-1, keepdims=True)
                expon = jnp.exp(scores - top)
                total = jnp.sum(expon, axis=-1, keepdims=True)
                summed = jnp.dot(expon.astype(jnp.bfloat16), value, preferred_element_type=jnp.float32)
                results.append(summed / total)
            at = (pairs + pair) * LANES
            att[rows, at : at + LANES] = joined(results, (2 * pair, 2 * pair + 1))

    expand(0)
    dense(0)

    @pl.when(inner)
    def _():
        mate_ready(2)
        project(2, 1)
        twin_ready(2, 2)
        project(2, 2)
        twin_ready(2, 3)
        project(2, 3)
        finished(2)
        ext[halo_at(low), :] = extm[pl.ds(jnp.where(low, length - WINDOW, 0), WINDOW), :]
        remote("inner", lambda: (ext.at[edge(high)], ext.at[halo_at(low)], es.at[2], er.at[2], z_in))
        remote("inner", lambda: (extm, ext.at[pl.ds(WINDOW, length)], es.at[0], er.at[0], z_out))
        remote("inner", lambda: (ext.at[edge(low)], ext.at[halo_at(high)], es.at[1], er.at[1], z_out))
        for c in all_out:
            o_mates(c)
        for c in all_chunks:
            crossing(3, 3, c)
        project(3, 0)
        mate_ready(3)
        project(3, 1)
        twin_ready(3, 2)
        project(3, 2)

    dense(1)

    @pl.when(outer)
    def _():
        landed(ext.at[pl.ds(WINDOW, length)], er.at[0], z_in)
        landed(ext.at[halo_at(high)], er.at[1], z_in)
        for c in all_out:
            o_outer(2, c)
        landed(qc.at[1], qr.at[1], z_in)

    @pl.when(inner)
    def _():
        for c in all_out:
            o_crossing(2, c)
        twin_ready(3, 3)
        project(3, 3)
        finished(3)
        q_outward(1)
        landed(ext.at[halo_at(high)], er.at[2], z_in)

    expand(1)
    for pair in range(pairs):
        windowed(pair)

    def span(rel):
        h = g if rel == 0 else 1 - g
        return pl.ds(pl.multiple_of(h * out_half, out_half), out_half)

    def part_rows(dest):
        return pl.ds(pl.multiple_of(dest * share, share), share)

    def emit(j, rel):
        part[j, :, span(rel)] = jnp.dot(
            att[...], wo[j, :, span(rel)], preferred_element_type=jnp.float32
        ).astype(jnp.bfloat16)
        for i in range(2):
            exchange(j, rel, i)

    def exchange(j, rel, i):
        remote("both", lambda: (
            part.at[j, part_rows(2 * i + 1 - core), span(rel)], dbuf.at[j, i, :, span(rel)],
            ds.at[j, rel, i], dr.at[j, rel, i], {"tp": twin},
        ))

    def combine(j, rel):
        for i in range(2):
            landed(dbuf.at[j, i, :, span(rel)], dr.at[j, rel, i], {"tp": twin})
        other = 1 - chip
        both = (
            part[j, part_rows(2 * other + core), span(rel)].astype(jnp.float32)
            + dbuf[j, other, :, span(rel)].astype(jnp.float32)
        )
        xsend[j, :, span(rel)] = both.astype(jnp.bfloat16)
        remote("both", lambda: (
            xsend.at[j, :, span(rel)], xrecv.at[j, :, span(rel)], rxs.at[j, rel], rxr.at[j, rel], {"tp": across}
        ))

    def store(j, rel):
        h = g if rel == 0 else 1 - g
        at = pl.ds(pl.multiple_of(place_of(j) * out_cols + h * out_half, out_half), out_half)
        return pltpu.make_async_copy(ostage.at[j, :, span(rel)], out_hbm.at[:, at], store_sem.at[j, rel])

    def settle(j, rel):
        landed(xrecv.at[j, :, span(rel)], rxr.at[j, rel], {"tp": across})
        total = (
            part[j, part_rows(t), span(rel)].astype(jnp.float32)
            + dbuf[j, chip, :, span(rel)].astype(jnp.float32)
            + xrecv[j, :, span(rel)].astype(jnp.float32)
        )
        ostage[j, :, span(rel)] = total.astype(jnp.bfloat16)
        store(j, rel).start()

    def arrive(j, rel):
        if (j, rel) == (1, 1):

            @pl.when(inner)
            def _():
                for c in all_out:
                    o_landed(1, 1, c, z_out)

            @pl.when(outer)
            def _():
                for c in all_out:
                    o_twin_landed(1, c)

        elif rel == 1 and j > 1:
            for c in all_out:
                o_twin_landed(j, c)
        elif (j, rel) == (3, 0):

            @pl.when(inner)
            def _():
                for c in all_out:
                    o_crossing(3, c)

            @pl.when(outer)
            def _():
                for c in all_out:
                    o_outer(3, c)

    order = ((0, 0), (0, 1), (1, 0), (2, 0), (2, 1), (3, 0), (1, 1), (3, 1))
    for i, piece in enumerate(order):
        arrive(*piece)
        emit(*piece)
        if i >= 1:
            combine(*order[i - 1])
        if i >= 2:
            settle(*order[i - 2])
    combine(*order[-1])
    settle(*order[-2])
    settle(*order[-1])

    for role, test in (("inner", inner), ("outer", outer)):

        @pl.when(test)
        def _():
            for when, build in sent:
                if when == role:
                    build().wait_send()

    for when, build in sent:
        if when == "both":
            build().wait_send()
    for piece in order:
        store(*piece).wait()


def local(*args):
    tokens_in, norm_gain, wq, wk, wv, wq_gain, wk_gain, sink, dq, dk, dv, dq_gain, dk_gain, w_out, d_out = args
    length, width = tokens_in.shape
    n, n_tp = lax.axis_size("sp"), lax.axis_size("tp")
    depth, cols = wq.shape
    paired = (
        n == 4 and n_tp == 4 and wk.shape[1] == LANES and cols == 2 * LANES and depth * n == width
        and length % (n_tp * 32) == 0 and length % WINDOW == 0
    )
    if not paired:
        return local_ring(*args)
    q_heads, kv_heads = cols // HD, wk.shape[1] // HD
    out_rows, out_cols = w_out.shape[0] + d_out.shape[0], w_out.shape[1]
    share = length // n_tp
    lane = np.arange(LANES)
    fixed = np.stack(
        [THETA ** (-2.0 * (lane % (wide // 2)) / wide) for wide in (HD, HD // 2)]
        + [np.where(lane % wide < wide // 2, -1.0, 1.0) for wide in (HD, HD // 2)]
    ).astype(np.float32)
    gains = [gain[None, :] for gain in (wq_gain, wk_gain, dq_gain, dk_gain)]
    chunks, out_chunks, pieces = 2, 4, width // depth
    vmem = pl.BlockSpec(memory_space=pltpu.VMEM)
    bf16 = jnp.bfloat16

    def sem(*shape):
        return pltpu.SemaphoreType.DMA(shape)

    return pl.pallas_call(
        functools.partial(pair_kernel, (q_heads, kv_heads)),
        out_shape=jax.ShapeDtypeStruct((share, width), bf16),
        in_specs=[vmem] * 6
        + [pl.BlockSpec(memory_space=pltpu.SMEM)]
        + [pl.BlockSpec(memory_space=pl.ANY)] * 9,
        out_specs=pl.BlockSpec(memory_space=pl.ANY),
        scratch_shapes=[
            pltpu.VMEM((8, LANES), jnp.float32),
            pltpu.VMEM((4, 2 * length, LANES), jnp.float32),
            pltpu.VMEM((length, width), bf16),
            pltpu.VMEM((2 * length, width), bf16),
            pltpu.VMEM((KINDS, n, depth, cols), bf16),
            pltpu.VMEM((n, out_rows, out_cols), bf16),
            pltpu.VMEM((2 * length, cols), jnp.float32),
            pltpu.VMEM((n, length, cols), bf16),
            pltpu.VMEM((length + 2 * WINDOW, cols), bf16),
            pltpu.VMEM((length, cols), bf16),
            pltpu.VMEM((2, length, cols), bf16),
            pltpu.VMEM((2, length, cols), bf16),
            pltpu.VMEM((q_heads, length, LANES), bf16),
            pltpu.VMEM((length, out_rows), bf16),
            pltpu.VMEM((n, length, out_cols), bf16),
            pltpu.VMEM((n, 2, share, out_cols), bf16),
            pltpu.VMEM((n, share, out_cols), bf16),
            pltpu.VMEM((n, share, out_cols), bf16),
            pltpu.VMEM((n, share, out_cols), bf16),
            sem(9),
            sem(n, HALVES),
            sem(KINDS, 2, HALVES, chunks),
            sem(KINDS, n, HALVES, chunks),
            sem(KINDS, n, chunks),
            sem(KINDS, n, chunks),
            sem(2, HALVES, out_chunks),
            sem(n, HALVES, out_chunks),
            sem(n, out_chunks),
            sem(n, out_chunks),
            sem(n, out_chunks),
        ]
        + [sem(pieces)] * 8
        + [sem(2), sem(n), sem(n), sem(3), sem(3), sem(2), sem(2)]
        + [sem(n, HALVES, 2), sem(n, HALVES, 2), sem(n, HALVES), sem(n, HALVES)],
        compiler_params=pltpu.CompilerParams(
            collective_id=0, has_side_effects=True, vmem_limit_bytes=62 * 1024 * 1024
        ),
    )(norm_gain[None, :], fixed, *gains, sink[None, :], tokens_in, wq, dq, dk, dv, wk, wv, w_out, d_out)


def solution(mesh):
    return jax.shard_map(
        local,
        mesh=mesh,
        in_specs=(
            P(("grp", "sp"), None),
            P(),
            P("sp", "tp"),
            P("sp", "tp"),
            P("sp", "tp"),
            P(),
            P(),
            P("tp"),
            P("sp", "tp"),
            P("sp", "tp"),
            P("sp", "tp"),
            P(),
            P(),
            P("tp", "sp"),
            P("tp", "sp"),
        ),
        out_specs=P(("grp", "sp", "tp"), None),
        check_vma=False,
    )
```

```python
import functools

import jax
import jax.numpy as jnp
import numpy as np
from jax import lax
from jax.experimental import pallas as pl
from jax.experimental.pallas import tpu as pltpu
from jax.sharding import PartitionSpec as P

HD = 64
WINDOW = 128
GRID_W = 64


EPS = 1e-06
THETA = 10000.0


MESH = pl.DeviceIdType.MESH
HALVES = 2


class LineGather:
    def __init__(self, own, buf, z_recv, r_send, l_send, y_recv=None, y_send=None, axis=0):
        self.own, self.buf = own, buf
        self.z_recv, self.y_recv = z_recv, y_recv
        self.r_send, self.l_send, self.y_send = r_send, l_send, y_send
        self.n = lax.axis_size("sp")
        self.s = lax.axis_index("sp")
        self.shared = y_recv is not None
        self.g = lax.axis_index("grp") if self.shared else 0
        self.chunks = z_recv.shape[1]
        self.axis = axis
        extent = buf.shape[1 + axis]
        self.half = extent // HALVES if self.shared else extent
        self.size = self.half // self.chunks

    def rows(self, half, c):
        piece = pl.ds(pl.multiple_of(half * self.half + c * self.size, self.size), self.size)
        return (piece,) if self.axis == 0 else (slice(None), piece)

    def block(self, o, half, c):
        return self.buf.at[(o,) + self.rows(half, c)]

    def copy(self, src, o, c, sem, recv, target, half):
        return pltpu.make_async_remote_copy(
            src_ref=src,
            dst_ref=self.block(o, half, c),
            send_sem=sem.at[o, c],
            recv_sem=recv.at[o, c],
            device_id=target,
            device_id_type=MESH,
        )

    def right(self, src, o, c):
        return self.copy(src, o, c, self.r_send, self.z_recv, {"sp": lax.rem(self.s + 1, self.n)}, self.g)

    def left(self, src, o, c):
        return self.copy(
            src, o, c, self.l_send, self.z_recv, {"sp": lax.rem(self.s + self.n - 1, self.n)}, self.g
        )

    def twin(self, o, c, half):
        return self.copy(
            self.block(o, half, c), o, c, self.y_send, self.y_recv, {"grp": 1 - self.g}, half
        )

    def mine(self, c):
        if self.own is None:
            return self.block(self.s, self.g, c)
        return self.own.at[self.rows(self.g, c)]

    def start(self, first=0, last=None):
        for c in range(first, self.chunks if last is None else last):
            mine = self.mine(c)

            @pl.when(self.s + 1 < self.n)
            def _():
                self.right(mine, self.s, c).start()

            @pl.when(self.s > 0)
            def _():
                self.left(mine, self.s, c).start()

    def forward(self, d):
        for c in range(self.chunks):

            @pl.when(self.s - d >= 0)
            def _():
                o = self.s - d
                there = self.block(o, self.g, c)
                self.right(there, o, c).wait_recv()

                @pl.when(self.s + 1 < self.n)
                def _():
                    self.right(there, o, c).start()

                if self.shared:
                    self.twin(o, c, self.g).start()

            @pl.when(self.s + d < self.n)
            def _():
                o = self.s + d
                there = self.block(o, self.g, c)
                self.left(there, o, c).wait_recv()

                @pl.when(self.s > 0)
                def _():
                    self.left(there, o, c).start()

                if self.shared:
                    self.twin(o, c, self.g).start()

    def use(self, d, fn, near=None):
        for there, o in ((self.s - d >= 0, self.s - d), (self.s + d < self.n, self.s + d)):
            if near is not None:

                @pl.when(there)
                def _():
                    near(o)

        for there, o in ((self.s - d >= 0, self.s - d), (self.s + d < self.n, self.s + d)):

            @pl.when(there)
            def _():
                for c in range(self.chunks):
                    self.twin(o, c, 1 - self.g).wait_recv()
                fn(o)

    def run(self, fn, near=None, last=None):
        self.forward(1)
        self.rest(fn, near, last)

    def rest(self, fn, near=None, last=None):
        @pl.loop(2, self.n)
        def _(d):
            self.forward(d)
            self.use(d - 1, fn, near)

        if last is not None:
            last()
        self.use(self.n - 1, fn, near)

    def finish(self):
        @pl.loop(0, self.n)
        def _(o):
            for c in range(self.chunks):
                there = self.block(o, self.g, c)

                @pl.when((o <= self.s) & (self.s + 1 < self.n))
                def _():
                    self.right(there, o, c).wait_send()

                @pl.when((o >= self.s) & (self.s > 0))
                def _():
                    self.left(there, o, c).wait_send()

                if self.shared:

                    @pl.when(o != self.s)
                    def _():
                        self.twin(o, c, self.g).wait_send()


def greet():
    n, s, g = lax.axis_size("sp"), lax.axis_index("sp"), lax.axis_index("grp")
    n_tp, t = lax.axis_size("tp"), lax.axis_index("tp")
    barrier = pltpu.get_barrier_semaphore()
    pl.semaphore_signal(barrier, inc=1, device_id={"grp": 1 - g}, device_id_type=MESH)
    for j in range(1, n_tp):
        pl.semaphore_signal(barrier, inc=1, device_id={"tp": lax.rem(t + j, n_tp)}, device_id_type=MESH)

    @pl.when(s + 1 < n)
    def _():
        pl.semaphore_signal(barrier, inc=1, device_id={"sp": lax.rem(s + 1, n)}, device_id_type=MESH)

    @pl.when(s > 0)
    def _():
        pl.semaphore_signal(barrier, inc=1, device_id={"sp": lax.rem(s + n - 1, n)}, device_id_type=MESH)

    pl.semaphore_wait(barrier, n_tp + (s + 1 < n).astype(jnp.int32) + (s > 0).astype(jnp.int32))


LANES = 128


def by_half(low, high):
    lane = lax.broadcasted_iota(jnp.int32, low.shape, 1)
    return jnp.where(lane < HD, low, high)


def swap_pairs(values, reach):
    lane = lax.broadcasted_iota(jnp.int32, values.shape, 1)
    ahead = pltpu.roll(values, LANES - reach, 1)
    behind = pltpu.roll(values, reach, 1)
    return jnp.where(lax.rem(lane, 2 * reach) < reach, ahead, behind)


def head_tile(tile, kinds, gains_ref, tables_ref):
    square = tile * tile
    zero = jnp.zeros_like(square)
    low = jnp.sum(by_half(square, zero), axis=-1, keepdims=True)
    high = jnp.sum(by_half(zero, square), axis=-1, keepdims=True)
    mean = by_half(jnp.broadcast_to(low, tile.shape), jnp.broadcast_to(high, tile.shape)) * (1.0 / HD)
    scaled = tile * lax.rsqrt(mean + EPS)

    def one(kind):
        if kind is None:
            return tile
        gain, table, reach = kind
        normed = scaled * gains_ref[gain : gain + 1, :]
        return normed * tables_ref[2 * table] + swap_pairs(normed, reach) * tables_ref[2 * table + 1]

    if kinds[0] == kinds[1]:
        return one(kinds[0])
    return by_half(one(kinds[0]), one(kinds[1]))


def layer_kernel(
    sizes, x_ref, gain_ref, fixed_ref, g0, g1, g2, g3, sink_ref, *refs
):
    n_in = sizes[2]
    in_refs, out_refs = refs[:n_in], refs[n_in : n_in + 2]
    run_layer(sizes[:2], x_ref, gain_ref, fixed_ref, (g0, g1, g2, g3), sink_ref, in_refs, out_refs, *refs[n_in + 2 :])


def run_layer(
    sizes, x_ref, gain_ref, fixed_ref, head_gains, sink_ref, in_refs, out_refs, out_ref,
    small_ref, w_ref, wo_ref, tables_ref, load_sem, xn, proj, wbuf, wo_all, kvd, ext, qs, att, part, rs, halo_recv, halo_send, rs_recv, rs_send, *sems
):
    q_heads, kv_heads = sizes
    n, s = lax.axis_size("sp"), lax.axis_index("sp")
    n_tp, t = lax.axis_size("tp"), lax.axis_index("tp")
    depth = w_ref.shape[0]
    length = x_ref.shape[0]
    into = LineGather(w_ref, wbuf, *sems[:5])
    out = LineGather(wo_ref, wo_all, *sems[5:10], axis=1)
    keys = LineGather(None, kvd, *sems[10:])
    loads, at = [], 0
    for ref in in_refs:
        wide = ref.shape[1]
        loads.append(
            pltpu.make_async_copy(ref, w_ref.at[:, at : at + wide], load_sem.at[len(loads)])
        )
        at += wide
    at = 0
    for ref in out_refs:
        tall = ref.shape[0]
        loads.append(pltpu.make_async_copy(ref, wo_ref.at[at : at + tall], load_sem.at[len(loads)]))
        at += tall
    for load in loads:
        load.start()
    greet()
    for load in loads:
        load.wait()
    into.start()

    for k, ref in enumerate(head_gains):
        small_ref[k : k + 1, :] = jnp.concatenate([ref[...], ref[...]], axis=1)
    small_ref[4:8, :] = fixed_ref[...]
    step = 16

    @pl.loop(0, length // step)
    def _(i):
        rows = pl.ds(pl.multiple_of(i * step, step), step)
        values = x_ref[rows, :].astype(jnp.float32)
        mean = jnp.mean(values * values, axis=-1, keepdims=True)
        xn[rows, :] = (values * lax.rsqrt(mean + EPS) * gain_ref[...]).astype(jnp.bfloat16)

    def columns(o):
        return pl.ds(pl.multiple_of(o * depth, depth), depth)

    proj[...] = jnp.dot(xn[:, columns(s)], w_ref[...], preferred_element_type=jnp.float32)

    band = 64 if length % 64 == 0 else length

    @pl.loop(0, length // band)
    def _(i):
        rows = pl.ds(pl.multiple_of(i * band, band), band)
        shape = (band, LANES)
        place = lax.broadcasted_iota(jnp.int32, shape, 0) + (s * length + i * band)
        lane = lax.broadcasted_iota(jnp.int32, shape, 1)
        spot = jnp.where(lax.rem(lane, HD) < HD // 2, place // GRID_W, lax.rem(place, GRID_W))
        for k, where in enumerate((place, spot)):
            angles = where.astype(jnp.float32) * small_ref[4 + k : 5 + k, :]
            tables_ref[2 * k, rows, :] = jnp.cos(angles)
            tables_ref[2 * k + 1, rows, :] = jnp.sin(angles) * small_ref[6 + k : 7 + k, :]

    def add(o):
        proj[...] += jnp.dot(xn[:, columns(o)], wbuf[o], preferred_element_type=jnp.float32)

    into.run(add, last=lambda: out.start(0, 1))

    win_q, win_k, den_q, den_k = (0, 0, 32), (1, 0, 32), (2, 1, 16), (3, 1, 16)
    kinds = (
        [win_q] * q_heads + [den_q] * q_heads + [den_k] * kv_heads + [None] * kv_heads
        + [win_k] * kv_heads + [None] * kv_heads
    )
    q_tiles = 2 * q_heads * HD // LANES
    kv_tiles = 2 * kv_heads * HD // LANES

    def finished(i):
        return head_tile(
            proj[:, i * LANES : (i + 1) * LANES], kinds[2 * i : 2 * i + 2], small_ref, tables_ref
        )

    for i in range(kv_tiles):
        ext[WINDOW : WINDOW + length, i * LANES : (i + 1) * LANES] = finished(
            q_tiles + kv_tiles + i
        ).astype(jnp.bfloat16)
    for i in range(kv_tiles):
        kvd[s, :, i * LANES : (i + 1) * LANES] = finished(q_tiles + i).astype(jnp.bfloat16)

    def halo(side):
        source = pl.ds(length, WINDOW) if side == 0 else pl.ds(WINDOW, WINDOW)
        target = pl.ds(0, WINDOW) if side == 0 else pl.ds(WINDOW + length, WINDOW)
        peer = lax.rem(s + 1, n) if side == 0 else lax.rem(s + n - 1, n)
        return pltpu.make_async_remote_copy(
            src_ref=ext.at[source], dst_ref=ext.at[target], send_sem=halo_send.at[side],
            recv_sem=halo_recv.at[side], device_id={"sp": peer}, device_id_type=MESH,
        )

    has_right, has_left = s + 1 < n, s > 0

    @pl.when(has_right)
    def _():
        halo(0).start()

    @pl.when(has_left)
    def _():
        halo(1).start()

    keys.start()
    none = jnp.zeros((WINDOW, ext.shape[1]), jnp.bfloat16)

    @pl.when(jnp.logical_not(has_left))
    def _():
        ext[0:WINDOW, :] = none

    @pl.when(jnp.logical_not(has_right))
    def _():
        ext[WINDOW + length : WINDOW + length + WINDOW, :] = none

    group = q_heads // kv_heads

    def place(head):
        return head // 2, head % 2

    for i in range(q_tiles):
        tile = finished(i) * HD ** (-0.5)
        for b in range(2):
            head = 2 * i + b
            half = place((head % q_heads) // group)[1]
            moved = tile if half == b else pltpu.roll(tile, HD, 1)
            zero = jnp.zeros_like(moved)
            kept = by_half(moved, zero) if half == 0 else by_half(zero, moved)
            qs[head] = kept.astype(jnp.bfloat16)

    @pl.when(has_left)
    def _():
        halo(0).wait_recv()

    @pl.when(has_right)
    def _():
        halo(1).wait_recv()

    total_len = length * n

    def joined(results, heads):
        placed = []
        for b in range(2):
            half = place(kv_heads + heads[b] // group)[1]
            placed.append(results[b] if half == b else pltpu.roll(results[b], HD, 1))
        return by_half(placed[0], placed[1]).astype(jnp.bfloat16)

    def tile_of(head):
        return pl.ds(place(head)[0] * LANES, LANES)

    nt = (((1,), (1,)), ((), ()))

    def windowed(pair):
        @pl.loop(0, length // WINDOW)
        def _(b):
            base = pl.multiple_of(b * WINDOW, WINDOW)
            rows = pl.ds(base, WINDOW)
            near = pl.ds(base, 3 * WINDOW)
            shape = (WINDOW, 3 * WINDOW)
            at = lax.broadcasted_iota(jnp.int32, shape, 1) - WINDOW
            away = at - lax.broadcasted_iota(jnp.int32, shape, 0)
            pos = at + (s * length + base)
            valid = (away <= WINDOW) & (away >= -WINDOW) & (pos >= 0) & (pos < total_len)
            results = []
            for head in (2 * pair, 2 * pair + 1):
                key = ext[near, tile_of(head // group)]
                value = ext[near, tile_of(kv_heads + head // group)]
                scores = lax.dot_general(qs[head, rows, :], key, nt, preferred_element_type=jnp.float32)
                scores = jnp.where(valid, scores, -jnp.inf)
                floor = sink_ref[0, head]
                top = jnp.maximum(jnp.max(scores, axis=-1, keepdims=True), floor)
                expon = jnp.exp(scores - top)
                total = jnp.sum(expon, axis=-1, keepdims=True) + jnp.exp(floor - top)
                weights = (expon / total).astype(jnp.bfloat16)
                results.append(jnp.dot(weights, value, preferred_element_type=jnp.float32))
            att[rows, pair * LANES : (pair + 1) * LANES] = joined(results, (2 * pair, 2 * pair + 1))

    pairs = q_heads // 2
    keys.forward(1)
    windowed(0)

    @pl.loop(2, n)
    def _(d):
        keys.forward(d)

    out.start(1)
    for pair in range(1, pairs):
        windowed(pair)

    def dense(pair):
        @pl.loop(0, length // LANES)
        def _(b):
            rows = pl.ds(pl.multiple_of(b * LANES, LANES), LANES)
            results = []
            for head in (2 * pair, 2 * pair + 1):
                key = kvd[:, :, tile_of(head // group)].reshape(total_len, LANES)
                value = kvd[:, :, tile_of(kv_heads + head // group)].reshape(total_len, LANES)
                scores = lax.dot_general(
                    qs[q_heads + head, rows, :], key, nt, preferred_element_type=jnp.float32
                )
                top = jnp.max(scores, axis=-1, keepdims=True)
                expon = jnp.exp(scores - top)
                total = jnp.sum(expon, axis=-1, keepdims=True)
                summed = jnp.dot(
                    expon.astype(jnp.bfloat16), value, preferred_element_type=jnp.float32
                )
                results.append(summed / total)
            at = (pairs + pair) * LANES
            att[rows, at : at + LANES] = joined(results, (2 * pair, 2 * pair + 1))

    dense(0)
    out.forward(1)
    for pair in range(1, pairs):
        dense(pair)

    share = length // n_tp

    wide = wo_ref.shape[1]
    part_cols = wide // HALVES
    mine = lax.axis_index("grp")

    def span(h):
        return pl.ds(pl.multiple_of(h * part_cols, part_cols), part_cols)

    def exchange(o, h, j):
        peer = lax.rem(t + j, n_tp)
        return pltpu.make_async_remote_copy(
            src_ref=part.at[o, pl.ds(pl.multiple_of(peer * share, share), share), span(h)],
            dst_ref=rs.at[t, o, :, span(h)], send_sem=rs_send.at[j - 1, o, h],
            recv_sem=rs_recv.at[t, o, h], device_id={"tp": peer}, device_id_type=MESH,
        )

    def arrived(o, h, j):
        source = lax.rem(t + n_tp - j, n_tp)
        there = rs.at[source, o, :, span(h)]
        return pltpu.make_async_remote_copy(
            src_ref=there, dst_ref=there, send_sem=rs_send.at[j - 1, o, h],
            recv_sem=rs_recv.at[source, o, h], device_id={"tp": source}, device_id_type=MESH,
        )

    def emit(o, h, weight):
        part[o, :, span(h)] = jnp.dot(
            att[...], weight, preferred_element_type=jnp.float32
        ).astype(jnp.bfloat16)
        for j in range(1, n_tp):
            exchange(o, h, j).start()
        rs[t, o, :, span(h)] = part[o, pl.ds(pl.multiple_of(t * share, share), share), span(h)]

    def collect(o, h):
        for j in range(1, n_tp):
            arrived(o, h, j).wait_recv()
        total = rs[0, o, :, span(h)].astype(jnp.float32)
        for g in range(1, n_tp):
            total += rs[g, o, :, span(h)].astype(jnp.float32)
        columns_out = pl.ds(pl.multiple_of(o * wide + h * part_cols, part_cols), part_cols)
        out_ref[:, columns_out] = total.astype(jnp.bfloat16)

    for h in range(HALVES):
        emit(s, h, wo_ref[:, span(h)])
    out.rest(
        lambda o: emit(o, 1 - mine, wo_all[o, :, span(1 - mine)]),
        near=lambda o: emit(o, mine, wo_all[o, :, span(mine)]),
    )

    @pl.loop(0, n)
    def _(d):
        o = lax.rem(s + d, n)
        for h in range(HALVES):
            collect(o, h)

    @pl.loop(0, n)
    def _(o):
        for h in range(HALVES):
            for j in range(1, n_tp):
                exchange(o, h, j).wait_send()

    @pl.when(has_right)
    def _():
        halo(0).wait_send()

    @pl.when(has_left)
    def _():
        halo(1).wait_send()

    into.finish()
    out.finish()
    keys.finish()


def local_ring(
    tokens_in,
    norm_gain,
    window_query,
    window_key,
    window_value,
    window_query_gain,
    window_key_gain,
    sink_logit,
    dense_query,
    dense_key,
    dense_value,
    dense_query_gain,
    dense_key_gain,
    window_out,
    dense_out,
):
    length, width = tokens_in.shape
    n, n_tp = lax.axis_size("sp"), lax.axis_size("tp")
    q_heads, kv_heads = window_query.shape[1] // HD, window_key.shape[1] // HD
    weights, held = [], []
    for weight in (window_query, dense_query, dense_key, dense_value, window_key, window_value):
        held.append(weight)
        if sum(w.shape[1] for w in held) % LANES == 0:
            weights.append(held[0] if len(held) == 1 else jnp.concatenate(held, axis=1))
            held = []
    depth, in_cols = window_query.shape[0], sum(w.shape[1] for w in weights)
    out_rows, out_cols = window_out.shape[0] + dense_out.shape[0], window_out.shape[1]

    lane = np.arange(LANES)
    fixed = np.stack(
        [THETA ** (-2.0 * (lane % (wide // 2)) / wide) for wide in (HD, HD // 2)]
        + [np.where(lane % wide < wide // 2, -1.0, 1.0) for wide in (HD, HD // 2)]
    ).astype(np.float32)
    gains = [g[None, :] for g in (window_query_gain, window_key_gain, dense_query_gain, dense_key_gain)]

    def gather(chunks):
        return [pltpu.SemaphoreType.DMA((n, chunks)) for _ in range(5)]

    in_chunks = 8 if n <= 4 else 1
    out_chunks = out_cols // HALVES // LANES if n <= 4 else 1
    kv_cols = 2 * kv_heads * HD
    vmem = pl.BlockSpec(memory_space=pltpu.VMEM)
    share = length // n_tp
    return pl.pallas_call(
        functools.partial(layer_kernel, (q_heads, kv_heads, len(weights))),
        out_shape=jax.ShapeDtypeStruct((share, width), jnp.bfloat16),
        in_specs=[vmem] * 7
        + [pl.BlockSpec(memory_space=pltpu.SMEM)]
        + [pl.BlockSpec(memory_space=pl.ANY)] * (len(weights) + 2),
        out_specs=vmem,
        scratch_shapes=[
            pltpu.VMEM((8, LANES), jnp.float32),
            pltpu.VMEM((depth, in_cols), jnp.bfloat16),
            pltpu.VMEM((out_rows, out_cols), jnp.bfloat16),
            pltpu.VMEM((4, length, LANES), jnp.float32),
            pltpu.SemaphoreType.DMA((len(weights) + 2,)),
            pltpu.VMEM((length, width), jnp.bfloat16),
            pltpu.VMEM((length, in_cols), jnp.float32),
            pltpu.VMEM((n, depth, in_cols), jnp.bfloat16),
            pltpu.VMEM((n, out_rows, out_cols), jnp.bfloat16),
            pltpu.VMEM((n, length, kv_cols), jnp.bfloat16),
            pltpu.VMEM((length + 2 * WINDOW, kv_cols), jnp.bfloat16),
            pltpu.VMEM((2 * q_heads, length, LANES), jnp.bfloat16),
            pltpu.VMEM((length, out_rows), jnp.bfloat16),
            pltpu.VMEM((n, length, out_cols), jnp.bfloat16),
            pltpu.VMEM((n_tp, n, share, out_cols), jnp.bfloat16),
            pltpu.SemaphoreType.DMA((2,)),
            pltpu.SemaphoreType.DMA((2,)),
            pltpu.SemaphoreType.DMA((n_tp, n, HALVES)),
            pltpu.SemaphoreType.DMA((n_tp - 1, n, HALVES)),
        ]
        + gather(in_chunks)
        + gather(out_chunks)
        + [pltpu.SemaphoreType.DMA((n, 2 if n <= 4 else 1)) for _ in range(3)],
        compiler_params=pltpu.CompilerParams(
            collective_id=0, has_side_effects=True, vmem_limit_bytes=62 * 1024 * 1024
        ),
    )(tokens_in, norm_gain[None, :], fixed, *gains, sink_logit[None, :], *weights, window_out, dense_out)


KINDS = 4
SHARED = (True, False, False, False)

def pair_kernel(sizes, *refs):
    gain_ref, fixed_ref, g0, g1, g2, g3, sink_ref, x_hbm = refs[:8]
    weights, outs, out_hbm = refs[8:14], refs[14:16], refs[16]
    run_pairs(sizes, gain_ref, fixed_ref, (g0, g1, g2, g3), sink_ref, x_hbm, weights, outs, out_hbm, *refs[17:])


def run_pairs(
    sizes, gain_ref, fixed_ref, head_gains, sink_ref, x_hbm, weights, outs, out_hbm,
    small_ref, tables_ref, xv, xn, wbuf, wo, proj, kvd, ext, qs, att, part, dbuf, xsend, xrecv, ostage,
    load_sem, store_sem, zs, zr, ys, yr, wis, wzr, wos, wys, wyr,
    xzs, xzr, xxs, xxr, xds, xdr, xes, xer, kis, kr, hs, hr, ats, atr, ds, dr, rxs, rxr,
):
    q_heads, kv_heads = sizes
    n, s = lax.axis_size("sp"), lax.axis_index("sp")
    n_tp, t = lax.axis_size("tp"), lax.axis_index("tp")
    g = lax.axis_index("grp")
    length, width = xv.shape
    depth, cols = wbuf.shape[2], wbuf.shape[3]
    out_rows, out_cols = wo.shape[1], wo.shape[2]
    share = length // n_tp
    chunks, out_chunks = zs.shape[3], wis.shape[2]
    low = 2 * s < n
    high = jnp.logical_not(low)
    inner = (s > 0) & (s < n - 1)
    outer = jnp.logical_not(inner)
    step = jnp.where(low, 1, -1)
    inward = s + step
    outward = lax.rem(s - step + n, n)
    core, chip = lax.rem(t, 2), t // 2
    twin = t + 1 - 2 * core
    across = lax.rem(t + 2, n_tp)
    diagonal = lax.rem(twin + 2, n_tp)

    def place_of(j):
        if j == 0:
            return s
        return jnp.where(inner, (s - step, s - step, s + step, s + 2 * step)[j], s + j * step)

    sent = []

    def remote(when, ends):
        def build():
            src, dst, send, recv, peer = ends()
            return pltpu.make_async_remote_copy(
                src_ref=src, dst_ref=dst, send_sem=send, recv_sem=recv, device_id=peer, device_id_type=MESH
            )

        sent.append((when, build))
        build().start()

    def landed(ref, sem, peer):
        pltpu.make_async_remote_copy(
            src_ref=ref, dst_ref=ref, send_sem=sem, recv_sem=sem, device_id=peer, device_id_type=MESH
        ).wait_recv()

    z_in, z_out, y_peer = {"sp": inward}, {"sp": outward}, {"grp": 1 - g}

    half = depth // HALVES
    size = half // chunks

    def w_at(k, slot, rel, c):
        h = g if rel == 0 else 1 - g
        return wbuf.at[k, slot, pl.ds(pl.multiple_of(h * half + c * size, size), size)]

    def w_inward(role, k, slot, rel, c):
        to = 1 if role == "outer" else slot + 2
        remote(role, lambda: (
            w_at(k, slot, rel, c), w_at(k, to, rel, c), zs.at[k, slot, rel, c], zr.at[k, to, rel, c], z_in
        ))

    def w_landed(k, slot, rel, c):
        landed(w_at(k, slot, rel, c), zr.at[k, slot, rel, c], z_out if slot == 1 else z_in)

    def w_twin(k, slot, c):
        remote("inner", lambda: (
            w_at(k, slot, 0, c), w_at(k, slot, 0, c), ys.at[k, slot, c], yr.at[k, slot, c], y_peer
        ))

    def w_twin_landed(k, slot, c):
        landed(w_at(k, slot, 1, c), yr.at[k, slot, c], y_peer)

    out_half = out_cols // HALVES
    out_size = out_half // out_chunks

    def o_at(slot, rel, c):
        h = g if rel == 0 else 1 - g
        return wo.at[slot, :, pl.ds(pl.multiple_of(h * out_half + c * out_size, out_size), out_size)]

    def o_inward(role, slot, rel, c):
        to = 1 if role == "outer" else slot + 2
        remote(role, lambda: (
            o_at(slot, rel, c), o_at(to, rel, c), wis.at[slot, rel, c], wzr.at[to, rel, c], z_in
        ))

    def o_outward(slot, c):
        to = 1 if slot == 0 else slot
        remote("inner", lambda: (
            o_at(slot, 0, c), o_at(to, 0, c), wos.at[slot, c], wzr.at[to, 0, c], z_out
        ))

    def o_landed(slot, rel, c, peer):
        landed(o_at(slot, rel, c), wzr.at[slot, rel, c], peer)

    def o_twin(role, slot, c):
        remote(role, lambda: (o_at(slot, 0, c), o_at(slot, 0, c), wys.at[slot, c], wyr.at[slot, c], y_peer))

    def o_twin_landed(slot, c):
        landed(o_at(slot, 1, c), wyr.at[slot, c], y_peer)

    def x_rows(quarter):
        return pl.ds(pl.multiple_of(length + quarter * share, share), share)

    def x_cols(p):
        return pl.ds(p * depth, depth)

    def x_relay(p):
        def piece():
            return xn.at[x_rows(t), x_cols(p)]

        landed(piece(), xzr.at[p], z_out)
        remote("inner", lambda: (piece(), piece(), xxs.at[p], xxr.at[p], {"tp": across}))
        remote("inner", lambda: (piece(), piece(), xds.at[p], xdr.at[p], {"tp": twin}))

    def x_pass(p):
        def piece():
            return xn.at[x_rows(across), x_cols(p)]

        landed(piece(), xxr.at[p], {"tp": across})
        remote("inner", lambda: (piece(), piece(), xes.at[p], xer.at[p], {"tp": twin}))

    def x_all(p):
        landed(xn.at[x_rows(twin), x_cols(p)], xdr.at[p], {"tp": twin})
        landed(xn.at[x_rows(diagonal), x_cols(p)], xer.at[p], {"tp": twin})

    kv_cols = cols // 2
    loads = []

    def load(src, dst):
        copy = pltpu.make_async_copy(src, dst, load_sem.at[len(loads)])
        loads.append(copy)
        copy.start()

    wq, dq, dk, dv, wk, wv = weights
    load(dk, wbuf.at[0, 0, :, 0:kv_cols])
    load(dv, wbuf.at[0, 0, :, kv_cols:cols])
    load(x_hbm, xv)
    load(dq, wbuf.at[1, 0])
    load(wk, wbuf.at[2, 0, :, 0:kv_cols])
    load(wv, wbuf.at[2, 0, :, kv_cols:cols])
    load(wq, wbuf.at[3, 0])
    rows_of = outs[0].shape[0]
    load(outs[0], wo.at[0, 0:rows_of])
    load(outs[1], wo.at[0, rows_of:out_rows])
    greet()

    all_chunks, all_out = range(chunks), range(out_chunks)
    loads[0].wait()
    loads[1].wait()

    for role, test in (("inner", inner), ("outer", outer)):

        @pl.when(test)
        def _():
            for c in all_chunks:
                w_inward(role, 0, 0, 0, c)

    for k, ref in enumerate(head_gains):
        small_ref[k : k + 1, :] = jnp.concatenate([ref[...], ref[...]], axis=1)
    small_ref[4:8, :] = fixed_ref[...]
    loads[2].wait()

    def normalize(first, count):
        stripe = 16

        @pl.loop(0, count // stripe)
        def _(i):
            at = pl.multiple_of(i * stripe, stripe)
            values = xv[pl.ds(first + at, stripe), :].astype(jnp.float32)
            mean = jnp.mean(values * values, axis=-1, keepdims=True)
            xn[pl.ds(at, stripe), :] = (values * lax.rsqrt(mean + EPS) * gain_ref[...]).astype(jnp.bfloat16)

    band = 64

    def tables(first, count):
        @pl.loop(0, count // band)
        def _(i):
            at = pl.multiple_of(i * band, band) + first
            rows = pl.ds(at, band)
            shape = (band, LANES)
            base = jnp.where(at < length, s * length + at, (s - step) * length + at - length)
            place = lax.broadcasted_iota(jnp.int32, shape, 0) + base
            lane = lax.broadcasted_iota(jnp.int32, shape, 1)
            spot = jnp.where(lax.rem(lane, HD) < HD // 2, place // GRID_W, lax.rem(place, GRID_W))
            for k, where in enumerate((place, spot)):
                angles = where.astype(jnp.float32) * small_ref[4 + k : 5 + k, :]
                tables_ref[2 * k, rows, :] = jnp.cos(angles)
                tables_ref[2 * k + 1, rows, :] = jnp.sin(angles) * small_ref[6 + k : 7 + k, :]

    def project(k, j, sides=(0, 1)):
        at = pl.multiple_of(place_of(j) * depth, depth)

        @pl.loop(sides[0], sides[-1] + 1)
        def _(i):
            rows = pl.ds(pl.multiple_of(i * length, length), length)
            found = jnp.dot(xn[rows, pl.ds(at, depth)], wbuf[k, j], preferred_element_type=jnp.float32)
            proj[k % 2, rows, :] = found if j == 0 else proj[k % 2, rows, :] + found

    den_q, den_k, win_q, win_k = (2, 1, 16), (3, 1, 16), (0, 0, 32), (1, 0, 32)
    plans = ((den_k, None), (den_q, den_q), (win_k, None), (win_q, win_q))
    group = q_heads // kv_heads
    pairs = q_heads // 2

    def finished(k, side):
        rows = pl.ds(side * length, length)
        for tile in range(cols // LANES):
            lanes = pl.ds(tile * LANES, LANES)
            kind = plans[k][tile * 2 * LANES // cols]
            value = proj[k % 2, rows, lanes]
            if kind is not None:
                value = head_tile(
                    value, (kind, kind), small_ref, [tables_ref.at[m][rows, :] for m in range(4)]
                )
            if k % 2:
                value = value * HD ** (-0.5)
                zero = jnp.zeros_like(value)
                for b in range(2):
                    head = 2 * tile + b
                    half_of = head // group % 2
                    moved = value if half_of == b else pltpu.roll(value, HD, 1)
                    kept = by_half(moved, zero) if half_of == 0 else by_half(zero, moved)
                    qs[k // 2, side, head] = kept.astype(jnp.bfloat16)
            elif k == 0:
                kvd[side, :, lanes] = value.astype(jnp.bfloat16)
            else:
                ext[side, pl.ds(WINDOW, length), lanes] = value.astype(jnp.bfloat16)

    def mates(k, c):
        w_landed(k, 1, 0, c)
        w_inward("inner", k, 1, 0, c)
        if SHARED[k]:
            w_twin(k, 1, c)

    def crossing(k, slot, c):
        w_landed(k, slot, 0, c)
        w_twin(k, slot, c)

    def mate_ready(k):
        for c in all_chunks:
            if SHARED[k]:
                w_twin_landed(k, 1, c)
            else:
                w_landed(k, 1, 1, c)

    def twin_ready(k, slot):
        for c in all_chunks:
            w_twin_landed(k, slot, c)

    def o_mates(c):
        o_landed(1, 0, c, z_out)
        o_inward("inner", 1, 0, c)

    def o_crossing(slot, c):
        o_landed(slot, 0, c, z_in)
        o_outward(slot, c)
        o_twin("inner", slot, c)

    def o_outer(slot, c):
        o_landed(slot, 0, c, z_in)
        o_twin("outer", slot, c)

    def edge(first):
        return pl.ds(jnp.where(first, WINDOW, length), WINDOW)

    def halo_at(leading):
        return pl.ds(jnp.where(leading, 0, WINDOW + length), WINDOW)

    def halo_inward():
        remote("inner", lambda: (ext.at[0, edge(high)], ext.at[0, halo_at(low)], hs.at[0], hr.at[0], z_in))

    def halo_landed():
        landed(ext.at[0, halo_at(high)], hr.at[0], z_in)

    def halo_local():
        ext[0, halo_at(low), :] = ext[1, edge(high), :]
        ext[1, halo_at(high), :] = ext[0, edge(low), :]
        ext[1, halo_at(low), :] = jnp.zeros((WINDOW, cols), jnp.bfloat16)

    def kv_landed(j):
        landed(kvd.at[j], kr.at[j], z_in)

    def kv_inward(j):
        remote("inner", lambda: (kvd.at[j], kvd.at[j + 2], kis.at[j], kr.at[j + 2], z_in))

    def x_inward(p):
        remote("outer", lambda: (
            xn.at[0:share, x_cols(p)], xn.at[x_rows(t), x_cols(p)], xzs.at[p], xzr.at[p], z_in
        ))

    def att_at(side, i):
        return att.at[side, :, i * LANES : (i + 1) * LANES]

    def att_outward(i):
        remote("inner", lambda: (att_at(1, i), att_at(0, i), ats.at[i], atr.at[i], z_out))

    def att_landed(i):
        landed(att_at(0, i), atr.at[i], z_in)

    def joined(results, pair):
        side = (kv_heads + pair * 2 // group) % 2
        placed = [results[b] if side == b else pltpu.roll(results[b], HD, 1) for b in range(2)]
        return by_half(placed[0], placed[1]).astype(jnp.bfloat16)

    def tile_of(head):
        return pl.ds(head // 2 * LANES, LANES)

    nt = (((1,), (1,)), ((), ()))
    total_len = length * n

    def windowed(side, pair):
        start = (s if side == 0 else s - step) * length
        shape = (2 * WINDOW, 3 * WINDOW)
        row = lax.rem(lax.broadcasted_iota(jnp.int32, shape, 0), WINDOW)
        at = lax.broadcasted_iota(jnp.int32, shape, 1) - WINDOW
        near_by = (at - row <= WINDOW) & (at - row >= -WINDOW)
        first = lax.broadcasted_iota(jnp.int32, (2 * WINDOW, 1), 0) < WINDOW
        floor = jnp.where(first, sink_ref[0, 2 * pair], sink_ref[0, 2 * pair + 1])
        blocks = range(length // WINDOW)
        near = [pl.ds(b * WINDOW, 3 * WINDOW) for b in blocks]
        rows = [pl.ds(b * WINDOW, WINDOW) for b in blocks]
        scores, expon, total = [], [], []
        for b in blocks:
            key = ext[side, near[b], tile_of(2 * pair // group)]
            query = qs[1, side, 2 * pair : 2 * pair + 2, rows[b], :].reshape(2 * WINDOW, LANES)
            pos = at + (start + b * WINDOW)
            valid = near_by & (pos >= 0) & (pos < total_len)
            found = lax.dot_general(query, key, nt, preferred_element_type=jnp.float32)
            scores.append(jnp.where(valid, found, -jnp.inf))
        tops = [jnp.maximum(jnp.max(score, axis=-1, keepdims=True), floor) for score in scores]
        for score, top in zip(scores, tops):
            expon.append(jnp.exp(score - top))
            total.append(jnp.sum(expon[-1], axis=-1, keepdims=True) + jnp.exp(floor - top))
        for b in blocks:
            value = ext[side, near[b], tile_of(kv_heads + 2 * pair // group)]
            weight = (expon[b] / total[b]).astype(jnp.bfloat16)
            found = jnp.dot(weight, value, preferred_element_type=jnp.float32)
            att[side, rows[b], pair * LANES : (pair + 1) * LANES] = joined((found[:WINDOW], found[WINDOW:]), pair)

    def dense(side, pair):
        @pl.loop(0, length // LANES)
        def _(b):
            rows = pl.ds(pl.multiple_of(b * LANES, LANES), LANES)
            key = kvd[:, :, tile_of(2 * pair // group)].reshape(total_len, LANES)
            value = kvd[:, :, tile_of(kv_heads + 2 * pair // group)].reshape(total_len, LANES)
            query = qs[0, side, 2 * pair : 2 * pair + 2, rows, :].reshape(2 * LANES, LANES)
            scores = lax.dot_general(query, key, nt, preferred_element_type=jnp.float32)
            top = jnp.max(scores, axis=-1, keepdims=True)
            expon = jnp.exp(scores - top)
            total = jnp.sum(expon, axis=-1, keepdims=True)
            summed = jnp.dot(expon.astype(jnp.bfloat16), value, preferred_element_type=jnp.float32) / total
            at = (pairs + pair) * LANES
            att[side, rows, at : at + LANES] = joined((summed[:LANES], summed[LANES:]), pair)

    @pl.when(outer)
    def _():
        normalize(t * share, share)
        for p in range(width // depth):
            x_inward(p)
        for one in loads[3:]:
            one.wait()
        for k, rel in ((1, 0), (2, 0), (1, 1), (3, 0), (2, 1), (3, 1)):
            for c in all_chunks:
                w_inward("outer", k, 0, rel, c)
        for rel in range(2):
            for c in all_out:
                o_inward("outer", 0, rel, c)
        for c in all_out:
            o_outer(1, c)
        for i in range(pairs, 2 * pairs):
            att_landed(i)

    @pl.when(inner)
    def _():
        for one in loads[3:]:
            one.wait()
        for c in all_out:
            o_outward(0, c)
        normalize(0, length)
        for c in all_chunks:
            mates(0, c)
            crossing(0, 2, c)
        for k in range(1, KINDS):
            for c in all_chunks:
                w_inward("inner", k, 0, 0, c)
        tables(0, length)
        for c in all_chunks:
            crossing(0, 3, c)
        x_relay(0)
        tables(length, length)
        crossing(1, 2, 0)
        x_relay(1)
        crossing(1, 2, 1)
        x_pass(0)
        x_relay(2)
        crossing(2, 2, 0)
        x_pass(1)
        x_relay(3)
        crossing(2, 2, 1)
        mate_ready(0)
        for j in range(2, 4):
            twin_ready(0, j)
        for j in range(4):
            project(0, j, (0,))
        finished(0, 0)
        kv_inward(0)
        x_pass(2)
        crossing(3, 2, 0)
        mates(1, 0)
        x_pass(3)
        crossing(3, 2, 1)
        mates(1, 1)
        for p in range(width // depth):
            x_all(p)
        for j in range(4):
            project(0, j, (1,))
        finished(0, 1)
        kv_inward(1)
        project(1, 0)
        twin_ready(1, 2)
        project(1, 2)
        mates(2, 0)
        crossing(1, 3, 0)
        project(2, 0)
        mates(2, 1)
        crossing(1, 3, 1)
        twin_ready(2, 2)
        project(2, 2)
        mate_ready(1)
        project(1, 1)
        twin_ready(1, 3)
        project(1, 3)
        finished(1, 1)
        finished(1, 0)
        kv_landed(2)
        kv_landed(3)
        crossing(2, 3, 0)
        mates(3, 0)
        dense(1, 0)
        att_outward(pairs)
        crossing(2, 3, 1)
        mates(3, 1)
        for c in all_out:
            o_inward("inner", 0, 0, c)
        dense(1, 1)
        att_outward(pairs + 1)
        mate_ready(2)
        crossing(3, 3, 0)
        project(2, 1)
        twin_ready(2, 3)
        project(2, 3)
        project(3, 0)
        crossing(3, 3, 1)
        finished(2, 1)
        finished(2, 0)
        halo_inward()
        halo_local()
        twin_ready(3, 2)
        project(3, 2)
        mate_ready(3)
        project(3, 1)
        o_crossing(2, 0)
        twin_ready(3, 3)
        project(3, 3, (1,))
        finished(3, 1)
        o_mates(0)
        windowed(1, 0)
        att_outward(0)
        windowed(1, 1)
        att_outward(1)
        o_crossing(2, 1)
        o_mates(1)
        project(3, 3, (0,))
        finished(3, 0)
        halo_landed()
        o_crossing(2, 2)
        o_mates(2)
        windowed(0, 0)
        windowed(0, 1)
        o_crossing(2, 3)
        o_mates(3)
        dense(0, 0)
        o_crossing(3, 0)
        dense(0, 1)
        o_crossing(3, 1)

    @pl.when(outer)
    def _():
        o_outer(2, 0)
        for i in range(pairs):
            att_landed(i)

    def span(rel, first=0, count=out_chunks):
        h = g if rel == 0 else 1 - g
        return pl.ds(pl.multiple_of(h * out_half + first * out_size, out_size), count * out_size)

    def part_rows(dest):
        return pl.ds(pl.multiple_of(dest * share, share), share)

    def tail(role, script):
        def emit(j, rel, *cut):
            lanes = span(rel, *cut)
            part[j, :, lanes] = jnp.dot(
                att[0], wo[j, :, lanes], preferred_element_type=jnp.float32
            ).astype(jnp.bfloat16)
            for i in range(2):
                exchange(i, j, rel, *cut)

        def exchange(i, j, rel, *cut):
            at = cut[0] if cut else 0
            remote(role, lambda: (
                part.at[j, part_rows(2 * i + 1 - core), span(rel, *cut)], dbuf.at[j, i, :, span(rel, *cut)],
                ds.at[j, rel, at, i], dr.at[j, rel, at, i], {"tp": twin},
            ))

        def combine(j, rel, *cut):
            at = cut[0] if cut else 0
            lanes = span(rel, *cut)
            for i in range(2):
                landed(dbuf.at[j, i, :, lanes], dr.at[j, rel, at, i], {"tp": twin})
            other = 1 - chip
            both = (
                part[j, part_rows(2 * other + core), lanes].astype(jnp.float32)
                + dbuf[j, other, :, lanes].astype(jnp.float32)
            )
            xsend[j, :, lanes] = both.astype(jnp.bfloat16)
            remote(role, lambda: (
                xsend.at[j, :, span(rel, *cut)], xrecv.at[j, :, span(rel, *cut)],
                rxs.at[j, rel, at], rxr.at[j, rel, at], {"tp": across},
            ))

        stores = []

        def settle(j, rel, *cut):
            at = cut[0] if cut else 0
            lanes = span(rel, *cut)
            landed(xrecv.at[j, :, lanes], rxr.at[j, rel, at], {"tp": across})
            total = (
                part[j, part_rows(t), lanes].astype(jnp.float32)
                + dbuf[j, chip, :, lanes].astype(jnp.float32)
                + xrecv[j, :, lanes].astype(jnp.float32)
            )
            ostage[j, :, lanes] = total.astype(jnp.bfloat16)
            first, count = cut if cut else (0, out_chunks)
            h = g if rel == 0 else 1 - g
            base = place_of(j) * out_cols + h * out_half + first * out_size
            to = pl.ds(pl.multiple_of(base, out_size), count * out_size)
            copy = pltpu.make_async_copy(ostage.at[j, :, lanes], out_hbm.at[:, to], store_sem.at[j, rel, at])
            stores.append(copy)
            copy.start()

        def ready(j, first=0, count=out_chunks):
            for c in range(first, first + count):
                if role == "inner" and j == 1:
                    o_landed(1, 1, c, z_out)
                else:
                    o_twin_landed(j, c)

        def pump(j, c):
            if role == "inner":
                o_crossing(j, c)
            else:
                o_outer(j, c)

        words = {"emit": emit, "combine": combine, "settle": settle, "ready": ready, "pump": pump}
        for word, *piece in script:
            words[word](*piece)
        for copy in stores:
            copy.wait()

    closing = [
        ("settle", 0, 0), ("settle", 0, 1), ("settle", 1, 0), ("settle", 2, 0), ("settle", 2, 1),
        ("settle", 3, 0, 0, 2), ("settle", 3, 0, 2, 2), ("settle", 3, 1, 0, 2),
    ]
    opening = [("emit", 0, 0), ("emit", 0, 1), ("combine", 0, 0), ("emit", 1, 0), ("combine", 0, 1)]
    inner_script = (
        opening
        + [("pump", 3, 2), ("emit", 2, 0), ("combine", 1, 0), ("ready", 2), ("emit", 2, 1), ("combine", 2, 0)]
        + [("pump", 3, 3), ("emit", 3, 0, 0, 2), ("combine", 2, 1), ("emit", 3, 0, 2, 2), ("combine", 3, 0, 0, 2)]
        + [("ready", 1), ("emit", 1, 1), ("combine", 3, 0, 2, 2), ("ready", 3, 0, 2), ("emit", 3, 1, 0, 2)]
        + [("combine", 1, 1), ("ready", 3, 2, 2), ("emit", 3, 1, 2, 2), ("combine", 3, 1, 0, 2)]
        + [("combine", 3, 1, 2, 2)]
        + closing + [("settle", 1, 1), ("settle", 3, 1, 2, 2)]
    )
    outer_script = (
        opening
        + [("pump", 2, 1), ("ready", 1), ("emit", 1, 1), ("combine", 1, 0), ("pump", 2, 2), ("combine", 1, 1)]
        + [("pump", 2, 3), ("emit", 2, 0), ("pump", 3, 0), ("combine", 2, 0), ("ready", 2), ("emit", 2, 1)]
        + [("pump", 3, 1), ("combine", 2, 1), ("pump", 3, 2), ("emit", 3, 0, 0, 2), ("pump", 3, 3)]
        + [("combine", 3, 0, 0, 2), ("emit", 3, 0, 2, 2), ("ready", 3, 0, 2), ("emit", 3, 1, 0, 2)]
        + [("combine", 3, 0, 2, 2), ("ready", 3, 2, 2), ("emit", 3, 1, 2, 2), ("combine", 3, 1, 0, 2)]
        + [("combine", 3, 1, 2, 2)]
        + closing[:4] + [("settle", 1, 1)] + closing[4:] + [("settle", 3, 1, 2, 2)]
    )

    @pl.when(inner)
    def _():
        tail("inner", inner_script)

    @pl.when(outer)
    def _():
        tail("outer", outer_script)

    for role, test in (("inner", inner), ("outer", outer)):

        @pl.when(test)
        def _():
            for when, build in sent:
                if when == role:
                    build().wait_send()


def local(*args):
    tokens_in, norm_gain, wq, wk, wv, wq_gain, wk_gain, sink, dq, dk, dv, dq_gain, dk_gain, w_out, d_out = args
    length, width = tokens_in.shape
    n, n_tp = lax.axis_size("sp"), lax.axis_size("tp")
    depth, cols = wq.shape
    paired = (
        n == 4 and n_tp == 4 and wk.shape[1] == LANES and cols == 2 * LANES and depth * n == width
        and length % (n_tp * 32) == 0 and length % WINDOW == 0
    )
    if not paired:
        return local_ring(*args)
    q_heads, kv_heads = cols // HD, wk.shape[1] // HD
    out_rows, out_cols = w_out.shape[0] + d_out.shape[0], w_out.shape[1]
    share = length // n_tp
    lane = np.arange(LANES)
    fixed = np.stack(
        [THETA ** (-2.0 * (lane % (wide // 2)) / wide) for wide in (HD, HD // 2)]
        + [np.where(lane % wide < wide // 2, -1.0, 1.0) for wide in (HD, HD // 2)]
    ).astype(np.float32)
    gains = [gain[None, :] for gain in (wq_gain, wk_gain, dq_gain, dk_gain)]
    chunks, out_chunks, pieces = 2, 4, width // depth
    vmem = pl.BlockSpec(memory_space=pltpu.VMEM)
    bf16 = jnp.bfloat16

    def sem(*shape):
        return pltpu.SemaphoreType.DMA(shape)

    return pl.pallas_call(
        functools.partial(pair_kernel, (q_heads, kv_heads)),
        out_shape=jax.ShapeDtypeStruct((share, width), bf16),
        in_specs=[vmem] * 6
        + [pl.BlockSpec(memory_space=pltpu.SMEM)]
        + [pl.BlockSpec(memory_space=pl.ANY)] * 9,
        out_specs=pl.BlockSpec(memory_space=pl.ANY),
        scratch_shapes=[
            pltpu.VMEM((8, LANES), jnp.float32),
            pltpu.VMEM((4, 2 * length, LANES), jnp.float32),
            pltpu.VMEM((length, width), bf16),
            pltpu.VMEM((2 * length, width), bf16),
            pltpu.VMEM((KINDS, n, depth, cols), bf16),
            pltpu.VMEM((n, out_rows, out_cols), bf16),
            pltpu.VMEM((2, 2 * length, cols), jnp.float32),
            pltpu.VMEM((n, length, cols), bf16),
            pltpu.VMEM((2, length + 2 * WINDOW, cols), bf16),
            pltpu.VMEM((2, 2, q_heads, length, LANES), bf16),
            pltpu.VMEM((2, length, out_rows), bf16),
            pltpu.VMEM((n, length, out_cols), bf16),
            pltpu.VMEM((n, 2, share, out_cols), bf16),
            pltpu.VMEM((n, share, out_cols), bf16),
            pltpu.VMEM((n, share, out_cols), bf16),
            pltpu.VMEM((n, share, out_cols), bf16),
            sem(9),
            sem(n, HALVES, out_chunks),
            sem(KINDS, 2, HALVES, chunks),
            sem(KINDS, n, HALVES, chunks),
            sem(KINDS, n, chunks),
            sem(KINDS, n, chunks),
            sem(2, HALVES, out_chunks),
            sem(n, HALVES, out_chunks),
            sem(n, out_chunks),
            sem(n, out_chunks),
            sem(n, out_chunks),
        ]
        + [sem(pieces)] * 8
        + [sem(2), sem(n), sem(1), sem(1), sem(q_heads), sem(q_heads)]
        + [sem(n, HALVES, out_chunks, 2)] * 2
        + [sem(n, HALVES, out_chunks)] * 2,
        compiler_params=pltpu.CompilerParams(
            collective_id=0, has_side_effects=True, vmem_limit_bytes=62 * 1024 * 1024
        ),
    )(norm_gain[None, :], fixed, *gains, sink[None, :], tokens_in, wq, dq, dk, dv, wk, wv, w_out, d_out)


def solution(mesh):
    return jax.shard_map(
        local,
        mesh=mesh,
        in_specs=(
            P(("grp", "sp"), None),
            P(),
            P("sp", "tp"),
            P("sp", "tp"),
            P("sp", "tp"),
            P(),
            P(),
            P("tp"),
            P("sp", "tp"),
            P("sp", "tp"),
            P("sp", "tp"),
            P(),
            P(),
            P("tp", "sp"),
            P("tp", "sp"),
        ),
        out_specs=P(("grp", "sp", "tp"), None),
        check_vma=False,
    )
```

```python
import functools

import jax
import jax.numpy as jnp
import numpy as np
from jax import lax
from jax.experimental import pallas as pl
from jax.experimental.pallas import tpu as pltpu
from jax.sharding import PartitionSpec as P

HD = 64
WINDOW = 128
GRID_W = 64


EPS = 1e-06
THETA = 10000.0


MESH = pl.DeviceIdType.MESH
HALVES = 2


class LineGather:
    def __init__(self, own, buf, z_recv, r_send, l_send, y_recv=None, y_send=None, axis=0):
        self.own, self.buf = own, buf
        self.z_recv, self.y_recv = z_recv, y_recv
        self.r_send, self.l_send, self.y_send = r_send, l_send, y_send
        self.n = lax.axis_size("sp")
        self.s = lax.axis_index("sp")
        self.shared = y_recv is not None
        self.g = lax.axis_index("grp") if self.shared else 0
        self.chunks = z_recv.shape[1]
        self.axis = axis
        extent = buf.shape[1 + axis]
        self.half = extent // HALVES if self.shared else extent
        self.size = self.half // self.chunks

    def rows(self, half, c):
        piece = pl.ds(pl.multiple_of(half * self.half + c * self.size, self.size), self.size)
        return (piece,) if self.axis == 0 else (slice(None), piece)

    def block(self, o, half, c):
        return self.buf.at[(o,) + self.rows(half, c)]

    def copy(self, src, o, c, sem, recv, target, half):
        return pltpu.make_async_remote_copy(
            src_ref=src,
            dst_ref=self.block(o, half, c),
            send_sem=sem.at[o, c],
            recv_sem=recv.at[o, c],
            device_id=target,
            device_id_type=MESH,
        )

    def right(self, src, o, c):
        return self.copy(src, o, c, self.r_send, self.z_recv, {"sp": lax.rem(self.s + 1, self.n)}, self.g)

    def left(self, src, o, c):
        return self.copy(
            src, o, c, self.l_send, self.z_recv, {"sp": lax.rem(self.s + self.n - 1, self.n)}, self.g
        )

    def twin(self, o, c, half):
        return self.copy(
            self.block(o, half, c), o, c, self.y_send, self.y_recv, {"grp": 1 - self.g}, half
        )

    def mine(self, c):
        if self.own is None:
            return self.block(self.s, self.g, c)
        return self.own.at[self.rows(self.g, c)]

    def start(self, first=0, last=None):
        for c in range(first, self.chunks if last is None else last):
            mine = self.mine(c)

            @pl.when(self.s + 1 < self.n)
            def _():
                self.right(mine, self.s, c).start()

            @pl.when(self.s > 0)
            def _():
                self.left(mine, self.s, c).start()

    def forward(self, d):
        for c in range(self.chunks):

            @pl.when(self.s - d >= 0)
            def _():
                o = self.s - d
                there = self.block(o, self.g, c)
                self.right(there, o, c).wait_recv()

                @pl.when(self.s + 1 < self.n)
                def _():
                    self.right(there, o, c).start()

                if self.shared:
                    self.twin(o, c, self.g).start()

            @pl.when(self.s + d < self.n)
            def _():
                o = self.s + d
                there = self.block(o, self.g, c)
                self.left(there, o, c).wait_recv()

                @pl.when(self.s > 0)
                def _():
                    self.left(there, o, c).start()

                if self.shared:
                    self.twin(o, c, self.g).start()

    def use(self, d, fn, near=None):
        for there, o in ((self.s - d >= 0, self.s - d), (self.s + d < self.n, self.s + d)):
            if near is not None:

                @pl.when(there)
                def _():
                    near(o)

        for there, o in ((self.s - d >= 0, self.s - d), (self.s + d < self.n, self.s + d)):

            @pl.when(there)
            def _():
                for c in range(self.chunks):
                    self.twin(o, c, 1 - self.g).wait_recv()
                fn(o)

    def run(self, fn, near=None, last=None):
        self.forward(1)
        self.rest(fn, near, last)

    def rest(self, fn, near=None, last=None):
        @pl.loop(2, self.n)
        def _(d):
            self.forward(d)
            self.use(d - 1, fn, near)

        if last is not None:
            last()
        self.use(self.n - 1, fn, near)

    def finish(self):
        @pl.loop(0, self.n)
        def _(o):
            for c in range(self.chunks):
                there = self.block(o, self.g, c)

                @pl.when((o <= self.s) & (self.s + 1 < self.n))
                def _():
                    self.right(there, o, c).wait_send()

                @pl.when((o >= self.s) & (self.s > 0))
                def _():
                    self.left(there, o, c).wait_send()

                if self.shared:

                    @pl.when(o != self.s)
                    def _():
                        self.twin(o, c, self.g).wait_send()


def greet():
    n, s, g = lax.axis_size("sp"), lax.axis_index("sp"), lax.axis_index("grp")
    n_tp, t = lax.axis_size("tp"), lax.axis_index("tp")
    barrier = pltpu.get_barrier_semaphore()
    pl.semaphore_signal(barrier, inc=1, device_id={"grp": 1 - g}, device_id_type=MESH)
    for j in range(1, n_tp):
        pl.semaphore_signal(barrier, inc=1, device_id={"tp": lax.rem(t + j, n_tp)}, device_id_type=MESH)

    @pl.when(s + 1 < n)
    def _():
        pl.semaphore_signal(barrier, inc=1, device_id={"sp": lax.rem(s + 1, n)}, device_id_type=MESH)

    @pl.when(s > 0)
    def _():
        pl.semaphore_signal(barrier, inc=1, device_id={"sp": lax.rem(s + n - 1, n)}, device_id_type=MESH)

    pl.semaphore_wait(barrier, n_tp + (s + 1 < n).astype(jnp.int32) + (s > 0).astype(jnp.int32))


LANES = 128


def by_half(low, high):
    lane = lax.broadcasted_iota(jnp.int32, low.shape, 1)
    return jnp.where(lane < HD, low, high)


def swap_pairs(values, reach):
    lane = lax.broadcasted_iota(jnp.int32, values.shape, 1)
    ahead = pltpu.roll(values, LANES - reach, 1)
    behind = pltpu.roll(values, reach, 1)
    return jnp.where(lax.rem(lane, 2 * reach) < reach, ahead, behind)


def head_tile(tile, kinds, gains_ref, tables_ref):
    square = tile * tile
    zero = jnp.zeros_like(square)
    low = jnp.sum(by_half(square, zero), axis=-1, keepdims=True)
    high = jnp.sum(by_half(zero, square), axis=-1, keepdims=True)
    mean = by_half(jnp.broadcast_to(low, tile.shape), jnp.broadcast_to(high, tile.shape)) * (1.0 / HD)
    scaled = tile * lax.rsqrt(mean + EPS)

    def one(kind):
        if kind is None:
            return tile
        gain, table, reach = kind
        normed = scaled * gains_ref[gain : gain + 1, :]
        return normed * tables_ref[2 * table] + swap_pairs(normed, reach) * tables_ref[2 * table + 1]

    if kinds[0] == kinds[1]:
        return one(kinds[0])
    return by_half(one(kinds[0]), one(kinds[1]))


def layer_kernel(
    sizes, x_ref, gain_ref, fixed_ref, g0, g1, g2, g3, sink_ref, *refs
):
    n_in = sizes[2]
    in_refs, out_refs = refs[:n_in], refs[n_in : n_in + 2]
    run_layer(sizes[:2], x_ref, gain_ref, fixed_ref, (g0, g1, g2, g3), sink_ref, in_refs, out_refs, *refs[n_in + 2 :])


def run_layer(
    sizes, x_ref, gain_ref, fixed_ref, head_gains, sink_ref, in_refs, out_refs, out_ref,
    small_ref, w_ref, wo_ref, tables_ref, load_sem, xn, proj, wbuf, wo_all, kvd, ext, qs, att, part, rs, halo_recv, halo_send, rs_recv, rs_send, *sems
):
    q_heads, kv_heads = sizes
    n, s = lax.axis_size("sp"), lax.axis_index("sp")
    n_tp, t = lax.axis_size("tp"), lax.axis_index("tp")
    depth = w_ref.shape[0]
    length = x_ref.shape[0]
    into = LineGather(w_ref, wbuf, *sems[:5])
    out = LineGather(wo_ref, wo_all, *sems[5:10], axis=1)
    keys = LineGather(None, kvd, *sems[10:])
    loads, at = [], 0
    for ref in in_refs:
        wide = ref.shape[1]
        loads.append(
            pltpu.make_async_copy(ref, w_ref.at[:, at : at + wide], load_sem.at[len(loads)])
        )
        at += wide
    at = 0
    for ref in out_refs:
        tall = ref.shape[0]
        loads.append(pltpu.make_async_copy(ref, wo_ref.at[at : at + tall], load_sem.at[len(loads)]))
        at += tall
    for load in loads:
        load.start()
    greet()
    for load in loads:
        load.wait()
    into.start()

    for k, ref in enumerate(head_gains):
        small_ref[k : k + 1, :] = jnp.concatenate([ref[...], ref[...]], axis=1)
    small_ref[4:8, :] = fixed_ref[...]
    step = 16

    @pl.loop(0, length // step)
    def _(i):
        rows = pl.ds(pl.multiple_of(i * step, step), step)
        values = x_ref[rows, :].astype(jnp.float32)
        mean = jnp.mean(values * values, axis=-1, keepdims=True)
        xn[rows, :] = (values * lax.rsqrt(mean + EPS) * gain_ref[...]).astype(jnp.bfloat16)

    def columns(o):
        return pl.ds(pl.multiple_of(o * depth, depth), depth)

    proj[...] = jnp.dot(xn[:, columns(s)], w_ref[...], preferred_element_type=jnp.float32)

    band = 64 if length % 64 == 0 else length

    @pl.loop(0, length // band)
    def _(i):
        rows = pl.ds(pl.multiple_of(i * band, band), band)
        shape = (band, LANES)
        place = lax.broadcasted_iota(jnp.int32, shape, 0) + (s * length + i * band)
        lane = lax.broadcasted_iota(jnp.int32, shape, 1)
        spot = jnp.where(lax.rem(lane, HD) < HD // 2, place // GRID_W, lax.rem(place, GRID_W))
        for k, where in enumerate((place, spot)):
            angles = where.astype(jnp.float32) * small_ref[4 + k : 5 + k, :]
            tables_ref[2 * k, rows, :] = jnp.cos(angles)
            tables_ref[2 * k + 1, rows, :] = jnp.sin(angles) * small_ref[6 + k : 7 + k, :]

    def add(o):
        proj[...] += jnp.dot(xn[:, columns(o)], wbuf[o], preferred_element_type=jnp.float32)

    into.run(add, last=lambda: out.start(0, 1))

    win_q, win_k, den_q, den_k = (0, 0, 32), (1, 0, 32), (2, 1, 16), (3, 1, 16)
    kinds = (
        [win_q] * q_heads + [den_q] * q_heads + [den_k] * kv_heads + [None] * kv_heads
        + [win_k] * kv_heads + [None] * kv_heads
    )
    q_tiles = 2 * q_heads * HD // LANES
    kv_tiles = 2 * kv_heads * HD // LANES

    def finished(i):
        return head_tile(
            proj[:, i * LANES : (i + 1) * LANES], kinds[2 * i : 2 * i + 2], small_ref, tables_ref
        )

    for i in range(kv_tiles):
        ext[WINDOW : WINDOW + length, i * LANES : (i + 1) * LANES] = finished(
            q_tiles + kv_tiles + i
        ).astype(jnp.bfloat16)
    for i in range(kv_tiles):
        kvd[s, :, i * LANES : (i + 1) * LANES] = finished(q_tiles + i).astype(jnp.bfloat16)

    def halo(side):
        source = pl.ds(length, WINDOW) if side == 0 else pl.ds(WINDOW, WINDOW)
        target = pl.ds(0, WINDOW) if side == 0 else pl.ds(WINDOW + length, WINDOW)
        peer = lax.rem(s + 1, n) if side == 0 else lax.rem(s + n - 1, n)
        return pltpu.make_async_remote_copy(
            src_ref=ext.at[source], dst_ref=ext.at[target], send_sem=halo_send.at[side],
            recv_sem=halo_recv.at[side], device_id={"sp": peer}, device_id_type=MESH,
        )

    has_right, has_left = s + 1 < n, s > 0

    @pl.when(has_right)
    def _():
        halo(0).start()

    @pl.when(has_left)
    def _():
        halo(1).start()

    keys.start()
    none = jnp.zeros((WINDOW, ext.shape[1]), jnp.bfloat16)

    @pl.when(jnp.logical_not(has_left))
    def _():
        ext[0:WINDOW, :] = none

    @pl.when(jnp.logical_not(has_right))
    def _():
        ext[WINDOW + length : WINDOW + length + WINDOW, :] = none

    group = q_heads // kv_heads

    def place(head):
        return head // 2, head % 2

    for i in range(q_tiles):
        tile = finished(i) * HD ** (-0.5)
        for b in range(2):
            head = 2 * i + b
            half = place((head % q_heads) // group)[1]
            moved = tile if half == b else pltpu.roll(tile, HD, 1)
            zero = jnp.zeros_like(moved)
            kept = by_half(moved, zero) if half == 0 else by_half(zero, moved)
            qs[head] = kept.astype(jnp.bfloat16)

    @pl.when(has_left)
    def _():
        halo(0).wait_recv()

    @pl.when(has_right)
    def _():
        halo(1).wait_recv()

    total_len = length * n

    def joined(results, heads):
        placed = []
        for b in range(2):
            half = place(kv_heads + heads[b] // group)[1]
            placed.append(results[b] if half == b else pltpu.roll(results[b], HD, 1))
        return by_half(placed[0], placed[1]).astype(jnp.bfloat16)

    def tile_of(head):
        return pl.ds(place(head)[0] * LANES, LANES)

    nt = (((1,), (1,)), ((), ()))

    def windowed(pair):
        @pl.loop(0, length // WINDOW)
        def _(b):
            base = pl.multiple_of(b * WINDOW, WINDOW)
            rows = pl.ds(base, WINDOW)
            near = pl.ds(base, 3 * WINDOW)
            shape = (WINDOW, 3 * WINDOW)
            at = lax.broadcasted_iota(jnp.int32, shape, 1) - WINDOW
            away = at - lax.broadcasted_iota(jnp.int32, shape, 0)
            pos = at + (s * length + base)
            valid = (away <= WINDOW) & (away >= -WINDOW) & (pos >= 0) & (pos < total_len)
            results = []
            for head in (2 * pair, 2 * pair + 1):
                key = ext[near, tile_of(head // group)]
                value = ext[near, tile_of(kv_heads + head // group)]
                scores = lax.dot_general(qs[head, rows, :], key, nt, preferred_element_type=jnp.float32)
                scores = jnp.where(valid, scores, -jnp.inf)
                floor = sink_ref[0, head]
                top = jnp.maximum(jnp.max(scores, axis=-1, keepdims=True), floor)
                expon = jnp.exp(scores - top)
                total = jnp.sum(expon, axis=-1, keepdims=True) + jnp.exp(floor - top)
                weights = (expon / total).astype(jnp.bfloat16)
                results.append(jnp.dot(weights, value, preferred_element_type=jnp.float32))
            att[rows, pair * LANES : (pair + 1) * LANES] = joined(results, (2 * pair, 2 * pair + 1))

    pairs = q_heads // 2
    keys.forward(1)
    windowed(0)

    @pl.loop(2, n)
    def _(d):
        keys.forward(d)

    out.start(1)
    for pair in range(1, pairs):
        windowed(pair)

    def dense(pair):
        @pl.loop(0, length // LANES)
        def _(b):
            rows = pl.ds(pl.multiple_of(b * LANES, LANES), LANES)
            results = []
            for head in (2 * pair, 2 * pair + 1):
                key = kvd[:, :, tile_of(head // group)].reshape(total_len, LANES)
                value = kvd[:, :, tile_of(kv_heads + head // group)].reshape(total_len, LANES)
                scores = lax.dot_general(
                    qs[q_heads + head, rows, :], key, nt, preferred_element_type=jnp.float32
                )
                top = jnp.max(scores, axis=-1, keepdims=True)
                expon = jnp.exp(scores - top)
                total = jnp.sum(expon, axis=-1, keepdims=True)
                summed = jnp.dot(
                    expon.astype(jnp.bfloat16), value, preferred_element_type=jnp.float32
                )
                results.append(summed / total)
            at = (pairs + pair) * LANES
            att[rows, at : at + LANES] = joined(results, (2 * pair, 2 * pair + 1))

    dense(0)
    out.forward(1)
    for pair in range(1, pairs):
        dense(pair)

    share = length // n_tp

    wide = wo_ref.shape[1]
    part_cols = wide // HALVES
    mine = lax.axis_index("grp")

    def span(h):
        return pl.ds(pl.multiple_of(h * part_cols, part_cols), part_cols)

    def exchange(o, h, j):
        peer = lax.rem(t + j, n_tp)
        return pltpu.make_async_remote_copy(
            src_ref=part.at[o, pl.ds(pl.multiple_of(peer * share, share), share), span(h)],
            dst_ref=rs.at[t, o, :, span(h)], send_sem=rs_send.at[j - 1, o, h],
            recv_sem=rs_recv.at[t, o, h], device_id={"tp": peer}, device_id_type=MESH,
        )

    def arrived(o, h, j):
        source = lax.rem(t + n_tp - j, n_tp)
        there = rs.at[source, o, :, span(h)]
        return pltpu.make_async_remote_copy(
            src_ref=there, dst_ref=there, send_sem=rs_send.at[j - 1, o, h],
            recv_sem=rs_recv.at[source, o, h], device_id={"tp": source}, device_id_type=MESH,
        )

    def emit(o, h, weight):
        part[o, :, span(h)] = jnp.dot(
            att[...], weight, preferred_element_type=jnp.float32
        ).astype(jnp.bfloat16)
        for j in range(1, n_tp):
            exchange(o, h, j).start()
        rs[t, o, :, span(h)] = part[o, pl.ds(pl.multiple_of(t * share, share), share), span(h)]

    def collect(o, h):
        for j in range(1, n_tp):
            arrived(o, h, j).wait_recv()
        total = rs[0, o, :, span(h)].astype(jnp.float32)
        for g in range(1, n_tp):
            total += rs[g, o, :, span(h)].astype(jnp.float32)
        columns_out = pl.ds(pl.multiple_of(o * wide + h * part_cols, part_cols), part_cols)
        out_ref[:, columns_out] = total.astype(jnp.bfloat16)

    for h in range(HALVES):
        emit(s, h, wo_ref[:, span(h)])
    out.rest(
        lambda o: emit(o, 1 - mine, wo_all[o, :, span(1 - mine)]),
        near=lambda o: emit(o, mine, wo_all[o, :, span(mine)]),
    )

    @pl.loop(0, n)
    def _(d):
        o = lax.rem(s + d, n)
        for h in range(HALVES):
            collect(o, h)

    @pl.loop(0, n)
    def _(o):
        for h in range(HALVES):
            for j in range(1, n_tp):
                exchange(o, h, j).wait_send()

    @pl.when(has_right)
    def _():
        halo(0).wait_send()

    @pl.when(has_left)
    def _():
        halo(1).wait_send()

    into.finish()
    out.finish()
    keys.finish()


def local_ring(
    tokens_in,
    norm_gain,
    window_query,
    window_key,
    window_value,
    window_query_gain,
    window_key_gain,
    sink_logit,
    dense_query,
    dense_key,
    dense_value,
    dense_query_gain,
    dense_key_gain,
    window_out,
    dense_out,
):
    length, width = tokens_in.shape
    n, n_tp = lax.axis_size("sp"), lax.axis_size("tp")
    q_heads, kv_heads = window_query.shape[1] // HD, window_key.shape[1] // HD
    weights, held = [], []
    for weight in (window_query, dense_query, dense_key, dense_value, window_key, window_value):
        held.append(weight)
        if sum(w.shape[1] for w in held) % LANES == 0:
            weights.append(held[0] if len(held) == 1 else jnp.concatenate(held, axis=1))
            held = []
    depth, in_cols = window_query.shape[0], sum(w.shape[1] for w in weights)
    out_rows, out_cols = window_out.shape[0] + dense_out.shape[0], window_out.shape[1]

    lane = np.arange(LANES)
    fixed = np.stack(
        [THETA ** (-2.0 * (lane % (wide // 2)) / wide) for wide in (HD, HD // 2)]
        + [np.where(lane % wide < wide // 2, -1.0, 1.0) for wide in (HD, HD // 2)]
    ).astype(np.float32)
    gains = [g[None, :] for g in (window_query_gain, window_key_gain, dense_query_gain, dense_key_gain)]

    def gather(chunks):
        return [pltpu.SemaphoreType.DMA((n, chunks)) for _ in range(5)]

    in_chunks = 8 if n <= 4 else 1
    out_chunks = out_cols // HALVES // LANES if n <= 4 else 1
    kv_cols = 2 * kv_heads * HD
    vmem = pl.BlockSpec(memory_space=pltpu.VMEM)
    share = length // n_tp
    return pl.pallas_call(
        functools.partial(layer_kernel, (q_heads, kv_heads, len(weights))),
        out_shape=jax.ShapeDtypeStruct((share, width), jnp.bfloat16),
        in_specs=[vmem] * 7
        + [pl.BlockSpec(memory_space=pltpu.SMEM)]
        + [pl.BlockSpec(memory_space=pl.ANY)] * (len(weights) + 2),
        out_specs=vmem,
        scratch_shapes=[
            pltpu.VMEM((8, LANES), jnp.float32),
            pltpu.VMEM((depth, in_cols), jnp.bfloat16),
            pltpu.VMEM((out_rows, out_cols), jnp.bfloat16),
            pltpu.VMEM((4, length, LANES), jnp.float32),
            pltpu.SemaphoreType.DMA((len(weights) + 2,)),
            pltpu.VMEM((length, width), jnp.bfloat16),
            pltpu.VMEM((length, in_cols), jnp.float32),
            pltpu.VMEM((n, depth, in_cols), jnp.bfloat16),
            pltpu.VMEM((n, out_rows, out_cols), jnp.bfloat16),
            pltpu.VMEM((n, length, kv_cols), jnp.bfloat16),
            pltpu.VMEM((length + 2 * WINDOW, kv_cols), jnp.bfloat16),
            pltpu.VMEM((2 * q_heads, length, LANES), jnp.bfloat16),
            pltpu.VMEM((length, out_rows), jnp.bfloat16),
            pltpu.VMEM((n, length, out_cols), jnp.bfloat16),
            pltpu.VMEM((n_tp, n, share, out_cols), jnp.bfloat16),
            pltpu.SemaphoreType.DMA((2,)),
            pltpu.SemaphoreType.DMA((2,)),
            pltpu.SemaphoreType.DMA((n_tp, n, HALVES)),
            pltpu.SemaphoreType.DMA((n_tp - 1, n, HALVES)),
        ]
        + gather(in_chunks)
        + gather(out_chunks)
        + [pltpu.SemaphoreType.DMA((n, 2 if n <= 4 else 1)) for _ in range(3)],
        compiler_params=pltpu.CompilerParams(
            collective_id=0, has_side_effects=True, vmem_limit_bytes=62 * 1024 * 1024
        ),
    )(tokens_in, norm_gain[None, :], fixed, *gains, sink_logit[None, :], *weights, window_out, dense_out)


KINDS = 4
SHARED = (True, False, False, False)
RECEIVES, SENDS, LOCALS = 131, 109, 20

def pair_kernel(sizes, *refs):
    gain_ref, fixed_ref, g0, g1, g2, g3, sink_ref, x_hbm = refs[:8]
    weights, outs, out_hbm = refs[8:14], refs[14:16], refs[16]
    run_pairs(sizes, gain_ref, fixed_ref, (g0, g1, g2, g3), sink_ref, x_hbm, weights, outs, out_hbm, *refs[17:])


def run_pairs(
    sizes, gain_ref, fixed_ref, head_gains, sink_ref, x_hbm, weights, outs, out_hbm,
    small_ref, tables_ref, xv, xn, wbuf, wo, proj, kvd, ext, qs, att, part, dbuf, xsend, xrecv, ostage, mpart, mbuf, msum,
    recv_sem, send_sem, load_sem,
):
    q_heads, kv_heads, chunks, out_chunks = sizes
    n, s = lax.axis_size("sp"), lax.axis_index("sp")
    n_tp, t = lax.axis_size("tp"), lax.axis_index("tp")
    g = lax.axis_index("grp")
    length, width = xv.shape
    depth, cols = wbuf.shape[2], wbuf.shape[3]
    out_rows, out_cols = wo.shape[1], wo.shape[2]
    share = length // n_tp
    low = 2 * s < n
    high = jnp.logical_not(low)
    inner = (s > 0) & (s < n - 1)
    outer = jnp.logical_not(inner)
    step = jnp.where(low, 1, -1)
    inward = s + step
    outward = lax.rem(s - step + n, n)
    core, chip = lax.rem(t, 2), t // 2
    twin = t + 1 - 2 * core
    across = lax.rem(t + 2, n_tp)
    diagonal = lax.rem(twin + 2, n_tp)

    def place_of(j):
        if j == 0:
            return s
        return jnp.where(inner, (s - step, s - step, s + step, s + 2 * step)[j], s + j * step)

    sent = {"inner": [], "outer": []}
    names = {}

    def recv_at(*name):
        at = names.setdefault(name, len(names))
        assert at < recv_sem.shape[0]
        return recv_sem.at[at]

    def remote(when, name, ends):
        at = len(sent[when])
        assert at < send_sem.shape[0]

        def build():
            src, dst, peer = ends()
            return pltpu.make_async_remote_copy(
                src_ref=src, dst_ref=dst, send_sem=send_sem.at[at], recv_sem=recv_at(*name),
                device_id=peer, device_id_type=MESH,
            )

        sent[when].append(build)
        build().start()

    def landed(ref, name, peer):
        sem = recv_at(*name)
        pltpu.make_async_remote_copy(
            src_ref=ref, dst_ref=ref, send_sem=sem, recv_sem=sem, device_id=peer, device_id_type=MESH
        ).wait_recv()

    z_in, z_out, y_peer = {"sp": inward}, {"sp": outward}, {"grp": 1 - g}

    half = depth // HALVES
    size = half // chunks

    def w_at(k, slot, rel, c):
        h = g if rel == 0 else 1 - g
        return wbuf.at[k, slot, pl.ds(pl.multiple_of(h * half + c * size, size), size)]

    def w_inward(role, k, slot, rel, c):
        to = 1 if role == "outer" else slot + 2
        remote(role, ("w", k, to, rel, c), lambda: (w_at(k, slot, rel, c), w_at(k, to, rel, c), z_in))

    def w_landed(k, slot, rel, c):
        landed(w_at(k, slot, rel, c), ("w", k, slot, rel, c), z_out if slot == 1 else z_in)

    def w_twin(k, slot, c):
        remote("inner", ("wy", k, slot, c), lambda: (w_at(k, slot, 0, c), w_at(k, slot, 0, c), y_peer))

    def w_twin_landed(k, slot, c):
        landed(w_at(k, slot, 1, c), ("wy", k, slot, c), y_peer)

    out_half = out_cols // HALVES
    out_size = out_half // out_chunks

    def o_at(slot, rel, c):
        h = g if rel == 0 else 1 - g
        return wo.at[slot, :, pl.ds(pl.multiple_of(h * out_half + c * out_size, out_size), out_size)]

    def o_inward(role, slot, rel, c):
        to = 1 if role == "outer" else slot + 2
        remote(role, ("o", to, rel, c), lambda: (o_at(slot, rel, c), o_at(to, rel, c), z_in))

    def o_outward(slot, c):
        to = 1 if slot == 0 else slot
        remote("inner", ("o", to, 0, c), lambda: (o_at(slot, 0, c), o_at(to, 0, c), z_out))

    def o_landed(slot, rel, c, peer):
        landed(o_at(slot, rel, c), ("o", slot, rel, c), peer)

    def o_twin(role, slot, c):
        remote(role, ("oy", slot, c), lambda: (o_at(slot, 0, c), o_at(slot, 0, c), y_peer))

    def o_twin_landed(slot, c):
        landed(o_at(slot, 1, c), ("oy", slot, c), y_peer)

    def x_rows(quarter):
        return pl.ds(pl.multiple_of(length + quarter * share, share), share)

    def x_cols(p):
        return pl.ds(p * depth, depth)

    def x_relay(p):
        def piece():
            return xn.at[x_rows(t), x_cols(p)]

        landed(piece(), ("x", p), z_out)
        remote("inner", ("xx", p), lambda: (piece(), piece(), {"tp": across}))
        remote("inner", ("xd", p), lambda: (piece(), piece(), {"tp": twin}))

    def x_pass(p):
        def piece():
            return xn.at[x_rows(across), x_cols(p)]

        landed(piece(), ("xx", p), {"tp": across})
        remote("inner", ("xe", p), lambda: (piece(), piece(), {"tp": twin}))

    def x_all(p):
        landed(xn.at[x_rows(twin), x_cols(p)], ("xd", p), {"tp": twin})
        landed(xn.at[x_rows(diagonal), x_cols(p)], ("xe", p), {"tp": twin})

    kv_cols = cols // 2
    loads = []

    def load(src, dst):
        copy = pltpu.make_async_copy(src, dst, load_sem.at[len(loads)])
        loads.append(copy)
        copy.start()

    wq, dq, dk, dv, wk, wv = weights
    load(dk, wbuf.at[0, 0, :, 0:kv_cols])
    load(dv, wbuf.at[0, 0, :, kv_cols:cols])
    load(x_hbm, xv)
    load(dq, wbuf.at[1, 0])
    load(wk, wbuf.at[2, 0, :, 0:kv_cols])
    load(wv, wbuf.at[2, 0, :, kv_cols:cols])
    load(wq, wbuf.at[3, 0])
    rows_of = outs[0].shape[0]
    load(outs[0], wo.at[0, 0:rows_of])
    load(outs[1], wo.at[0, rows_of:out_rows])
    greet()

    all_chunks, all_out = range(chunks), range(out_chunks)
    loads[0].wait()
    loads[1].wait()

    for role, test in (("inner", inner), ("outer", outer)):

        @pl.when(test)
        def _():
            for c in all_chunks:
                w_inward(role, 0, 0, 0, c)

    for k, ref in enumerate(head_gains):
        small_ref[k : k + 1, :] = jnp.concatenate([ref[...], ref[...]], axis=1)
    small_ref[4:8, :] = fixed_ref[...]
    loads[2].wait()

    def normalize(first, count):
        stripe = 16

        @pl.loop(0, count // stripe)
        def _(i):
            at = pl.multiple_of(i * stripe, stripe)
            values = xv[pl.ds(first + at, stripe), :].astype(jnp.float32)
            mean = jnp.mean(values * values, axis=-1, keepdims=True)
            xn[pl.ds(at, stripe), :] = (values * lax.rsqrt(mean + EPS) * gain_ref[...]).astype(jnp.bfloat16)

    band = 64

    def tables(first, count):
        @pl.loop(0, count // band)
        def _(i):
            at = pl.multiple_of(i * band, band) + first
            rows = pl.ds(at, band)
            shape = (band, LANES)
            base = jnp.where(at < length, s * length + at, (s - step) * length + at - length)
            place = lax.broadcasted_iota(jnp.int32, shape, 0) + base
            lane = lax.broadcasted_iota(jnp.int32, shape, 1)
            spot = jnp.where(lax.rem(lane, HD) < HD // 2, place // GRID_W, lax.rem(place, GRID_W))
            for k, where in enumerate((place, spot)):
                angles = where.astype(jnp.float32) * small_ref[4 + k : 5 + k, :]
                tables_ref[2 * k, rows, :] = jnp.cos(angles)
                tables_ref[2 * k + 1, rows, :] = jnp.sin(angles) * small_ref[6 + k : 7 + k, :]

    def project(k, j, sides=(0, 1)):
        at = pl.multiple_of(place_of(j) * depth, depth)

        @pl.loop(sides[0], sides[-1] + 1)
        def _(i):
            rows = pl.ds(pl.multiple_of(i * length, length), length)
            found = jnp.dot(xn[rows, pl.ds(at, depth)], wbuf[k, j], preferred_element_type=jnp.float32)
            proj[k % 2, rows, :] = found if j == 0 else proj[k % 2, rows, :] + found

    den_q, den_k, win_q, win_k = (2, 1, 16), (3, 1, 16), (0, 0, 32), (1, 0, 32)
    plans = ((den_k, None), (den_q, den_q), (win_k, None), (win_q, win_q))
    group = q_heads // kv_heads
    pairs = q_heads // 2

    def finished(k, side):
        rows = pl.ds(side * length, length)
        for tile in range(cols // LANES):
            lanes = pl.ds(tile * LANES, LANES)
            kind = plans[k][tile * 2 * LANES // cols]
            value = proj[k % 2, rows, lanes]
            if kind is not None:
                value = head_tile(
                    value, (kind, kind), small_ref, [tables_ref.at[m][rows, :] for m in range(4)]
                )
            if k % 2:
                value = value * HD ** (-0.5)
                zero = jnp.zeros_like(value)
                for b in range(2):
                    head = 2 * tile + b
                    half_of = head // group % 2
                    moved = value if half_of == b else pltpu.roll(value, HD, 1)
                    kept = by_half(moved, zero) if half_of == 0 else by_half(zero, moved)
                    qs[k // 2, side, head] = kept.astype(jnp.bfloat16)
            elif k == 0:
                kvd[side, :, lanes] = value.astype(jnp.bfloat16)
            else:
                ext[side, pl.ds(WINDOW, length), lanes] = value.astype(jnp.bfloat16)

    def mates(k, c):
        w_landed(k, 1, 0, c)
        w_inward("inner", k, 1, 0, c)
        if SHARED[k]:
            w_twin(k, 1, c)

    def crossing(k, slot, c):
        w_landed(k, slot, 0, c)
        w_twin(k, slot, c)

    def mate_ready(k):
        for c in all_chunks:
            if SHARED[k]:
                w_twin_landed(k, 1, c)
            else:
                w_landed(k, 1, 1, c)

    def twin_ready(k, slot):
        for c in all_chunks:
            w_twin_landed(k, slot, c)

    def o_mates(c):
        o_landed(1, 0, c, z_out)
        o_inward("inner", 1, 0, c)

    def o_crossing(slot, c):
        o_landed(slot, 0, c, z_in)
        if slot < 3:
            o_outward(slot, c)
        o_twin("inner", slot, c)

    def o_outer(slot, c):
        o_landed(slot, 0, c, z_in)
        o_twin("outer", slot, c)

    def edge(first):
        return pl.ds(jnp.where(first, WINDOW, length), WINDOW)

    def halo_at(leading):
        return pl.ds(jnp.where(leading, 0, WINDOW + length), WINDOW)

    def halo_inward():
        remote("inner", ("halo",), lambda: (ext.at[0, edge(high)], ext.at[0, halo_at(low)], z_in))

    def halo_landed():
        landed(ext.at[0, halo_at(high)], ("halo",), z_in)

    def halo_local():
        ext[0, halo_at(low), :] = ext[1, edge(high), :]
        ext[1, halo_at(high), :] = ext[0, edge(low), :]
        ext[1, halo_at(low), :] = jnp.zeros((WINDOW, cols), jnp.bfloat16)

    def kv_landed(j):
        landed(kvd.at[j], ("kv", j), z_in)

    def kv_inward(j):
        remote("inner", ("kv", j + 2), lambda: (kvd.at[j], kvd.at[j + 2], z_in))

    def x_inward(p):
        remote("outer", ("x", p), lambda: (xn.at[0:share, x_cols(p)], xn.at[x_rows(t), x_cols(p)], z_in))

    def att_at(side, i):
        return att.at[side, :, i * LANES : (i + 1) * LANES]

    def att_outward(i):
        remote("inner", ("att", i), lambda: (att_at(1, i), att_at(0, i), z_out))

    def att_landed(i):
        landed(att_at(0, i), ("att", i), z_in)

    def joined(results, pair):
        side = (kv_heads + pair * 2 // group) % 2
        placed = [results[b] if side == b else pltpu.roll(results[b], HD, 1) for b in range(2)]
        return by_half(placed[0], placed[1]).astype(jnp.bfloat16)

    def tile_of(head):
        return pl.ds(head // 2 * LANES, LANES)

    nt = (((1,), (1,)), ((), ()))
    total_len = length * n

    def windowed(side, pair):
        start = (s if side == 0 else s - step) * length
        shape = (2 * WINDOW, 3 * WINDOW)
        row = lax.rem(lax.broadcasted_iota(jnp.int32, shape, 0), WINDOW)
        at = lax.broadcasted_iota(jnp.int32, shape, 1) - WINDOW
        near_by = (at - row <= WINDOW) & (at - row >= -WINDOW)
        first = lax.broadcasted_iota(jnp.int32, (2 * WINDOW, 1), 0) < WINDOW
        floor = jnp.where(first, sink_ref[0, 2 * pair], sink_ref[0, 2 * pair + 1])
        blocks = range(length // WINDOW)
        near = [pl.ds(b * WINDOW, 3 * WINDOW) for b in blocks]
        rows = [pl.ds(b * WINDOW, WINDOW) for b in blocks]
        scores, expon, total = [], [], []
        for b in blocks:
            key = ext[side, near[b], tile_of(2 * pair // group)]
            query = qs[1, side, 2 * pair : 2 * pair + 2, rows[b], :].reshape(2 * WINDOW, LANES)
            pos = at + (start + b * WINDOW)
            valid = near_by & (pos >= 0) & (pos < total_len)
            found = lax.dot_general(query, key, nt, preferred_element_type=jnp.float32)
            scores.append(jnp.where(valid, found, -jnp.inf))
        tops = [jnp.maximum(jnp.max(score, axis=-1, keepdims=True), floor) for score in scores]
        for score, top in zip(scores, tops):
            expon.append(jnp.exp(score - top))
            total.append(jnp.sum(expon[-1], axis=-1, keepdims=True) + jnp.exp(floor - top))
        for b in blocks:
            value = ext[side, near[b], tile_of(kv_heads + 2 * pair // group)]
            weight = (expon[b] / total[b]).astype(jnp.bfloat16)
            found = jnp.dot(weight, value, preferred_element_type=jnp.float32)
            att[side, rows[b], pair * LANES : (pair + 1) * LANES] = joined((found[:WINDOW], found[WINDOW:]), pair)

    def dense(side, pair):
        @pl.loop(0, length // LANES)
        def _(b):
            rows = pl.ds(pl.multiple_of(b * LANES, LANES), LANES)
            key = kvd[:, :, tile_of(2 * pair // group)].reshape(total_len, LANES)
            value = kvd[:, :, tile_of(kv_heads + 2 * pair // group)].reshape(total_len, LANES)
            query = qs[0, side, 2 * pair : 2 * pair + 2, rows, :].reshape(2 * LANES, LANES)
            scores = lax.dot_general(query, key, nt, preferred_element_type=jnp.float32)
            top = jnp.max(scores, axis=-1, keepdims=True)
            expon = jnp.exp(scores - top)
            total = jnp.sum(expon, axis=-1, keepdims=True)
            summed = jnp.dot(expon.astype(jnp.bfloat16), value, preferred_element_type=jnp.float32) / total
            at = (pairs + pair) * LANES
            att[side, rows, at : at + LANES] = joined((summed[:LANES], summed[LANES:]), pair)

    @pl.when(outer)
    def _():
        normalize(t * share, share)
        for p in range(width // depth):
            x_inward(p)
        for one in loads[3:]:
            one.wait()
        for k, rel in ((1, 0), (2, 0), (1, 1), (3, 0), (2, 1), (3, 1)):
            for c in all_chunks:
                w_inward("outer", k, 0, rel, c)
        for rel in range(2):
            for c in all_out:
                o_inward("outer", 0, rel, c)
        for c in all_out:
            o_outer(1, c)
        for i in range(pairs, 2 * pairs):
            att_landed(i)

    @pl.when(inner)
    def _():
        for one in loads[3:]:
            one.wait()
        for c in all_out:
            o_outward(0, c)
        normalize(0, length)
        for c in all_chunks:
            mates(0, c)
            crossing(0, 2, c)
        for k in range(1, KINDS):
            for c in all_chunks:
                w_inward("inner", k, 0, 0, c)
        tables(0, length)
        for c in all_chunks:
            crossing(0, 3, c)
        x_relay(0)
        tables(length, length)
        crossing(1, 2, 0)
        x_relay(1)
        crossing(1, 2, 1)
        x_pass(0)
        x_relay(2)
        crossing(2, 2, 0)
        x_pass(1)
        x_relay(3)
        crossing(2, 2, 1)
        mate_ready(0)
        for j in range(2, 4):
            twin_ready(0, j)
        for j in range(4):
            project(0, j, (0,))
        finished(0, 0)
        kv_inward(0)
        x_pass(2)
        crossing(3, 2, 0)
        mates(1, 0)
        x_pass(3)
        crossing(3, 2, 1)
        mates(1, 1)
        for p in range(width // depth):
            x_all(p)
        for j in range(4):
            project(0, j, (1,))
        finished(0, 1)
        kv_inward(1)
        project(1, 0)
        twin_ready(1, 2)
        project(1, 2)
        mates(2, 0)
        crossing(1, 3, 0)
        project(2, 0)
        mates(2, 1)
        crossing(1, 3, 1)
        twin_ready(2, 2)
        project(2, 2)
        mate_ready(1)
        project(1, 1)
        twin_ready(1, 3)
        project(1, 3)
        finished(1, 1)
        finished(1, 0)
        kv_landed(2)
        kv_landed(3)
        crossing(2, 3, 0)
        mates(3, 0)
        dense(1, 0)
        att_outward(pairs)
        crossing(2, 3, 1)
        mates(3, 1)
        for c in range(2):
            o_inward("inner", 0, 0, c)
        dense(1, 1)
        att_outward(pairs + 1)
        crossing(3, 3, 0)
        dense(0, 0)
        mate_ready(2)
        project(2, 1)
        crossing(3, 3, 1)
        twin_ready(2, 3)
        project(2, 3)
        project(3, 0)
        finished(2, 1)
        finished(2, 0)
        halo_inward()
        for c in range(2, out_chunks):
            o_inward("inner", 0, 0, c)
        halo_local()
        twin_ready(3, 2)
        project(3, 2)
        mate_ready(3)
        project(3, 1)
        o_crossing(2, 0)
        twin_ready(3, 3)
        project(3, 3, (1,))
        finished(3, 1)
        windowed(1, 0)
        att_outward(0)
        windowed(1, 1)
        att_outward(1)
        o_crossing(2, 1)
        o_mates(0)
        project(3, 3, (0,))
        finished(3, 0)
        halo_landed()
        o_mates(1)
        windowed(0, 0)
        o_crossing(2, 2)
        windowed(0, 1)
        o_mates(2)
        dense(0, 1)
        o_crossing(2, 3)
        o_mates(3)
        o_crossing(3, 0)

    @pl.when(outer)
    def _():
        o_outer(2, 0)
        for i in range(pairs):
            att_landed(i)

    def span(rel, first=0, count=out_chunks):
        h = g if rel == 0 else 1 - g
        return pl.ds(pl.multiple_of(h * out_half + first * out_size, out_size), count * out_size)

    def tail(role, script):
        def emit(*piece):
            j, lanes = piece[0], span(*piece[1:])
            found = jnp.dot(att[0], wo[j, :, lanes], preferred_element_type=jnp.float32).astype(jnp.bfloat16)
            for dest in range(n_tp):
                part[j, dest % 2, dest // 2, :, lanes] = found[dest * share : (dest + 1) * share]
            remote(role, ("d",) + piece, lambda: (
                part.at[j, 1 - core, :, :, span(*piece[1:])], dbuf.at[j, :, :, span(*piece[1:])], {"tp": twin}
            ))

        def combine(*piece):
            j, lanes = piece[0], span(*piece[1:])
            landed(dbuf.at[j, :, :, lanes], ("d",) + piece, {"tp": twin})
            both = (
                part[j, core, 1 - chip, :, lanes].astype(jnp.float32) + dbuf[j, 1 - chip, :, lanes].astype(jnp.float32)
            )
            xsend[j, :, lanes] = both.astype(jnp.bfloat16)
            remote(role, ("r",) + piece, lambda: (
                xsend.at[j, :, span(*piece[1:])], xrecv.at[j, :, span(*piece[1:])], {"tp": across}
            ))

        def emit_mate(*piece):
            j, lanes = piece[0], span(*piece[1:])
            found = jnp.dot(att[1], wo[j, :, lanes], preferred_element_type=jnp.float32).astype(jnp.bfloat16)
            for dest in range(n_tp):
                mpart[dest % 2, dest // 2, :, lanes] = found[dest * share : (dest + 1) * share]
            remote(role, ("md",) + piece, lambda: (
                mpart.at[1 - core, :, :, span(*piece[1:])], mbuf.at[:, :, span(*piece[1:])], {"tp": twin}
            ))

        def combine_mate(*piece):
            lanes = span(*piece[1:])
            landed(mbuf.at[:, :, lanes], ("md",) + piece, {"tp": twin})
            both = mpart[core, :, :, lanes].astype(jnp.float32) + mbuf[:, :, lanes].astype(jnp.float32)
            msum[:, :, lanes] = both.astype(jnp.bfloat16)
            remote(role, ("m",) + piece, lambda: (
                msum.at[:, :, span(*piece[1:])], msum.at[:, :, span(*piece[1:])], z_out
            ))

        def relay(*piece):
            landed(msum.at[:, :, span(*piece[1:])], ("m",) + piece, z_in)
            remote(role, ("r",) + piece, lambda: (
                msum.at[1 - chip, :, span(*piece[1:])], xrecv.at[piece[0], :, span(*piece[1:])], {"tp": across}
            ))

        stores = []

        def settle(*piece):
            j, lanes = piece[0], span(*piece[1:])
            landed(xrecv.at[j, :, lanes], ("r",) + piece, {"tp": across})
            if role == "outer" and j == 3:
                near = msum[chip, :, lanes].astype(jnp.float32)
            else:
                near = part[j, core, chip, :, lanes].astype(jnp.float32) + dbuf[j, chip, :, lanes].astype(jnp.float32)
            total = near + xrecv[j, :, lanes].astype(jnp.float32)
            ostage[j, :, lanes] = total.astype(jnp.bfloat16)
            rel, first, count = piece[1:] if len(piece) > 2 else (piece[1], 0, out_chunks)
            h = g if rel == 0 else 1 - g
            base = place_of(j) * out_cols + h * out_half + first * out_size
            to = pl.ds(pl.multiple_of(base, out_size), count * out_size)
            copy = pltpu.make_async_copy(ostage.at[j, :, lanes], out_hbm.at[:, to], load_sem.at[len(loads) + len(stores)])
            stores.append(copy)
            copy.start()

        def ready(j, first=0, count=out_chunks):
            for c in range(first, first + count):
                if role == "inner" and j == 1:
                    o_landed(1, 1, c, z_out)
                else:
                    o_twin_landed(j, c)

        def pump(j, c):
            if role == "inner":
                o_crossing(j, c)
            else:
                o_outer(j, c)

        words = {
            "emit": emit, "combine": combine, "settle": settle, "ready": ready, "pump": pump,
            "emit_mate": emit_mate, "combine_mate": combine_mate, "relay": relay,
        }
        for word, *piece in script:
            words[word](*piece)
        for copy in stores:
            copy.wait()

    opening = [("emit", 0, 0), ("emit", 0, 1), ("combine", 0, 0), ("emit", 1, 0), ("combine", 0, 1)]
    last = [(3, 1, 0, 2), (3, 1, 2, 1), (3, 1, 3, 1)]
    far = [(3, 0, 0, 2), (3, 0, 2, 2)] + last
    inner_script = (
        opening
        + [("emit", 2, 0), ("combine", 1, 0), ("pump", 3, 1), ("ready", 2), ("emit", 2, 1), ("combine", 2, 0)]
        + [("pump", 3, 2), ("combine", 2, 1), ("emit_mate",) + far[0], ("emit",) + far[0]]
        + [("pump", 3, 3), ("combine_mate",) + far[0], ("emit_mate",) + far[1], ("emit",) + far[1]]
        + [("combine",) + far[0], ("ready", 3, 0, 2), ("combine_mate",) + far[1], ("emit_mate",) + last[0]]
        + [("emit",) + last[0], ("combine",) + far[1], ("ready", 1), ("emit", 1, 1)]
        + [("combine_mate",) + last[0], ("combine",) + last[0], ("combine", 1, 1)]
        + [("ready", 3, 2, 1), ("emit_mate",) + last[1], ("emit",) + last[1]]
        + [("settle", 0, 0), ("settle", 0, 1), ("combine_mate",) + last[1]]
        + [("ready", 3, 3, 1), ("emit_mate",) + last[2], ("emit",) + last[2]]
        + [("combine",) + last[1], ("settle", 1, 0), ("combine_mate",) + last[2], ("combine",) + last[2]]
        + [("settle", 2, 0), ("settle", 2, 1), ("settle",) + far[0], ("settle",) + far[1]]
        + [("settle",) + last[0], ("settle", 1, 1)] + [("settle",) + piece for piece in last[1:]]
    )
    outer_script = (
        opening
        + [("pump", 2, 1), ("ready", 1), ("emit", 1, 1), ("combine", 1, 0), ("pump", 2, 2), ("combine", 1, 1)]
        + [("pump", 2, 3), ("emit", 2, 0), ("ready", 2, 0, 2), ("combine", 2, 0)]
        + [("ready", 2, 2, 2), ("emit", 2, 1), ("settle", 0, 0), ("relay",) + far[0], ("combine", 2, 1)]
        + [("settle", 0, 1), ("settle", 1, 0), ("relay",) + far[1], ("settle", 1, 1), ("relay",) + last[0]]
        + [("settle", 2, 0), ("relay",) + last[1], ("relay",) + last[2], ("settle", 2, 1)]
        + [("settle",) + piece for piece in far]
    )

    @pl.when(inner)
    def _():
        tail("inner", inner_script)

    @pl.when(outer)
    def _():
        tail("outer", outer_script)

    for role, test in (("inner", inner), ("outer", outer)):

        @pl.when(test)
        def _():
            for build in sent[role]:
                build().wait_send()


def local(*args):
    tokens_in, norm_gain, wq, wk, wv, wq_gain, wk_gain, sink, dq, dk, dv, dq_gain, dk_gain, w_out, d_out = args
    length, width = tokens_in.shape
    n, n_tp = lax.axis_size("sp"), lax.axis_size("tp")
    depth, cols = wq.shape
    paired = (
        n == 4 and n_tp == 4 and wk.shape[1] == LANES and cols == 2 * LANES and depth * n == width
        and length % (n_tp * 32) == 0 and length % WINDOW == 0
    )
    if not paired:
        return local_ring(*args)
    q_heads, kv_heads = cols // HD, wk.shape[1] // HD
    out_rows, out_cols = w_out.shape[0] + d_out.shape[0], w_out.shape[1]
    share = length // n_tp
    lane = np.arange(LANES)
    fixed = np.stack(
        [THETA ** (-2.0 * (lane % (wide // 2)) / wide) for wide in (HD, HD // 2)]
        + [np.where(lane % wide < wide // 2, -1.0, 1.0) for wide in (HD, HD // 2)]
    ).astype(np.float32)
    gains = [gain[None, :] for gain in (wq_gain, wk_gain, dq_gain, dk_gain)]
    chunks, out_chunks = 2, 4
    vmem = pl.BlockSpec(memory_space=pltpu.VMEM)
    bf16 = jnp.bfloat16

    def sem(*shape):
        return pltpu.SemaphoreType.DMA(shape)

    return pl.pallas_call(
        functools.partial(pair_kernel, (q_heads, kv_heads, chunks, out_chunks)),
        out_shape=jax.ShapeDtypeStruct((share, width), bf16),
        in_specs=[vmem] * 6
        + [pl.BlockSpec(memory_space=pltpu.SMEM)]
        + [pl.BlockSpec(memory_space=pl.ANY)] * 9,
        out_specs=pl.BlockSpec(memory_space=pl.ANY),
        scratch_shapes=[
            pltpu.VMEM((8, LANES), jnp.float32),
            pltpu.VMEM((4, 2 * length, LANES), jnp.float32),
            pltpu.VMEM((length, width), bf16),
            pltpu.VMEM((2 * length, width), bf16),
            pltpu.VMEM((KINDS, n, depth, cols), bf16),
            pltpu.VMEM((n, out_rows, out_cols), bf16),
            pltpu.VMEM((2, 2 * length, cols), jnp.float32),
            pltpu.VMEM((n, length, cols), bf16),
            pltpu.VMEM((2, length + 2 * WINDOW, cols), bf16),
            pltpu.VMEM((2, 2, q_heads, length, LANES), bf16),
            pltpu.VMEM((2, length, out_rows), bf16),
            pltpu.VMEM((n, 2, n_tp // 2, share, out_cols), bf16),
            pltpu.VMEM((n, 2, share, out_cols), bf16),
            pltpu.VMEM((n, share, out_cols), bf16),
            pltpu.VMEM((n, share, out_cols), bf16),
            pltpu.VMEM((n, share, out_cols), bf16),
            pltpu.VMEM((2, n_tp // 2, share, out_cols), bf16),
            pltpu.VMEM((n_tp // 2, share, out_cols), bf16),
            pltpu.VMEM((n_tp // 2, share, out_cols), bf16),
            sem(RECEIVES),
            sem(SENDS),
            sem(LOCALS),
        ],
        compiler_params=pltpu.CompilerParams(
            collective_id=0, has_side_effects=True, vmem_limit_bytes=62 * 1024 * 1024
        ),
    )(norm_gain[None, :], fixed, *gains, sink[None, :], tokens_in, wq, dq, dk, dv, wk, wv, w_out, d_out)


def solution(mesh):
    return jax.shard_map(
        local,
        mesh=mesh,
        in_specs=(
            P(("grp", "sp"), None),
            P(),
            P("sp", "tp"),
            P("sp", "tp"),
            P("sp", "tp"),
            P(),
            P(),
            P("tp"),
            P("sp", "tp"),
            P("sp", "tp"),
            P("sp", "tp"),
            P(),
            P(),
            P("tp", "sp"),
            P("tp", "sp"),
        ),
        out_specs=P(("grp", "sp", "tp"), None),
        check_vma=False,
    )
```

```python
import functools

import jax
import jax.numpy as jnp
import numpy as np
from jax import lax
from jax.experimental import pallas as pl
from jax.experimental.pallas import tpu as pltpu
from jax.sharding import PartitionSpec as P

HD = 64
WINDOW = 128
GRID_W = 64


EPS = 1e-06
THETA = 10000.0


MESH = pl.DeviceIdType.MESH
HALVES = 2


class LineGather:
    def __init__(self, own, buf, z_recv, r_send, l_send, y_recv=None, y_send=None, axis=0):
        self.own, self.buf = own, buf
        self.z_recv, self.y_recv = z_recv, y_recv
        self.r_send, self.l_send, self.y_send = r_send, l_send, y_send
        self.n = lax.axis_size("sp")
        self.s = lax.axis_index("sp")
        self.shared = y_recv is not None
        self.g = lax.axis_index("grp") if self.shared else 0
        self.chunks = z_recv.shape[1]
        self.axis = axis
        extent = buf.shape[1 + axis]
        self.half = extent // HALVES if self.shared else extent
        self.size = self.half // self.chunks

    def rows(self, half, c):
        piece = pl.ds(pl.multiple_of(half * self.half + c * self.size, self.size), self.size)
        return (piece,) if self.axis == 0 else (slice(None), piece)

    def block(self, o, half, c):
        return self.buf.at[(o,) + self.rows(half, c)]

    def copy(self, src, o, c, sem, recv, target, half):
        return pltpu.make_async_remote_copy(
            src_ref=src,
            dst_ref=self.block(o, half, c),
            send_sem=sem.at[o, c],
            recv_sem=recv.at[o, c],
            device_id=target,
            device_id_type=MESH,
        )

    def right(self, src, o, c):
        return self.copy(src, o, c, self.r_send, self.z_recv, {"sp": lax.rem(self.s + 1, self.n)}, self.g)

    def left(self, src, o, c):
        return self.copy(
            src, o, c, self.l_send, self.z_recv, {"sp": lax.rem(self.s + self.n - 1, self.n)}, self.g
        )

    def twin(self, o, c, half):
        return self.copy(
            self.block(o, half, c), o, c, self.y_send, self.y_recv, {"grp": 1 - self.g}, half
        )

    def mine(self, c):
        if self.own is None:
            return self.block(self.s, self.g, c)
        return self.own.at[self.rows(self.g, c)]

    def start(self, first=0, last=None):
        for c in range(first, self.chunks if last is None else last):
            mine = self.mine(c)

            @pl.when(self.s + 1 < self.n)
            def _():
                self.right(mine, self.s, c).start()

            @pl.when(self.s > 0)
            def _():
                self.left(mine, self.s, c).start()

    def forward(self, d):
        for c in range(self.chunks):

            @pl.when(self.s - d >= 0)
            def _():
                o = self.s - d
                there = self.block(o, self.g, c)
                self.right(there, o, c).wait_recv()

                @pl.when(self.s + 1 < self.n)
                def _():
                    self.right(there, o, c).start()

                if self.shared:
                    self.twin(o, c, self.g).start()

            @pl.when(self.s + d < self.n)
            def _():
                o = self.s + d
                there = self.block(o, self.g, c)
                self.left(there, o, c).wait_recv()

                @pl.when(self.s > 0)
                def _():
                    self.left(there, o, c).start()

                if self.shared:
                    self.twin(o, c, self.g).start()

    def use(self, d, fn, near=None):
        for there, o in ((self.s - d >= 0, self.s - d), (self.s + d < self.n, self.s + d)):
            if near is not None:

                @pl.when(there)
                def _():
                    near(o)

        for there, o in ((self.s - d >= 0, self.s - d), (self.s + d < self.n, self.s + d)):

            @pl.when(there)
            def _():
                for c in range(self.chunks):
                    self.twin(o, c, 1 - self.g).wait_recv()
                fn(o)

    def run(self, fn, near=None, last=None):
        self.forward(1)
        self.rest(fn, near, last)

    def rest(self, fn, near=None, last=None):
        @pl.loop(2, self.n)
        def _(d):
            self.forward(d)
            self.use(d - 1, fn, near)

        if last is not None:
            last()
        self.use(self.n - 1, fn, near)

    def finish(self):
        @pl.loop(0, self.n)
        def _(o):
            for c in range(self.chunks):
                there = self.block(o, self.g, c)

                @pl.when((o <= self.s) & (self.s + 1 < self.n))
                def _():
                    self.right(there, o, c).wait_send()

                @pl.when((o >= self.s) & (self.s > 0))
                def _():
                    self.left(there, o, c).wait_send()

                if self.shared:

                    @pl.when(o != self.s)
                    def _():
                        self.twin(o, c, self.g).wait_send()


def greet():
    n, s, g = lax.axis_size("sp"), lax.axis_index("sp"), lax.axis_index("grp")
    n_tp, t = lax.axis_size("tp"), lax.axis_index("tp")
    barrier = pltpu.get_barrier_semaphore()
    pl.semaphore_signal(barrier, inc=1, device_id={"grp": 1 - g}, device_id_type=MESH)
    for j in range(1, n_tp):
        pl.semaphore_signal(barrier, inc=1, device_id={"tp": lax.rem(t + j, n_tp)}, device_id_type=MESH)

    @pl.when(s + 1 < n)
    def _():
        pl.semaphore_signal(barrier, inc=1, device_id={"sp": lax.rem(s + 1, n)}, device_id_type=MESH)

    @pl.when(s > 0)
    def _():
        pl.semaphore_signal(barrier, inc=1, device_id={"sp": lax.rem(s + n - 1, n)}, device_id_type=MESH)

    pl.semaphore_wait(barrier, n_tp + (s + 1 < n).astype(jnp.int32) + (s > 0).astype(jnp.int32))


LANES = 128


def by_half(low, high):
    lane = lax.broadcasted_iota(jnp.int32, low.shape, 1)
    return jnp.where(lane < HD, low, high)


def swap_pairs(values, reach):
    lane = lax.broadcasted_iota(jnp.int32, values.shape, 1)
    ahead = pltpu.roll(values, LANES - reach, 1)
    behind = pltpu.roll(values, reach, 1)
    return jnp.where(lax.rem(lane, 2 * reach) < reach, ahead, behind)


def head_tile(tile, kinds, gains_ref, tables_ref):
    square = tile * tile
    zero = jnp.zeros_like(square)
    low = jnp.sum(by_half(square, zero), axis=-1, keepdims=True)
    high = jnp.sum(by_half(zero, square), axis=-1, keepdims=True)
    mean = by_half(jnp.broadcast_to(low, tile.shape), jnp.broadcast_to(high, tile.shape)) * (1.0 / HD)
    scaled = tile * lax.rsqrt(mean + EPS)

    def one(kind):
        if kind is None:
            return tile
        gain, table, reach = kind
        normed = scaled * gains_ref[gain : gain + 1, :]
        return normed * tables_ref[2 * table] + swap_pairs(normed, reach) * tables_ref[2 * table + 1]

    if kinds[0] == kinds[1]:
        return one(kinds[0])
    return by_half(one(kinds[0]), one(kinds[1]))


def layer_kernel(
    sizes, x_ref, gain_ref, fixed_ref, g0, g1, g2, g3, sink_ref, *refs
):
    n_in = sizes[2]
    in_refs, out_refs = refs[:n_in], refs[n_in : n_in + 2]
    run_layer(sizes[:2], x_ref, gain_ref, fixed_ref, (g0, g1, g2, g3), sink_ref, in_refs, out_refs, *refs[n_in + 2 :])


def run_layer(
    sizes, x_ref, gain_ref, fixed_ref, head_gains, sink_ref, in_refs, out_refs, out_ref,
    small_ref, w_ref, wo_ref, tables_ref, load_sem, xn, proj, wbuf, wo_all, kvd, ext, qs, att, part, rs, halo_recv, halo_send, rs_recv, rs_send, *sems
):
    q_heads, kv_heads = sizes
    n, s = lax.axis_size("sp"), lax.axis_index("sp")
    n_tp, t = lax.axis_size("tp"), lax.axis_index("tp")
    depth = w_ref.shape[0]
    length = x_ref.shape[0]
    into = LineGather(w_ref, wbuf, *sems[:5])
    out = LineGather(wo_ref, wo_all, *sems[5:10], axis=1)
    keys = LineGather(None, kvd, *sems[10:])
    loads, at = [], 0
    for ref in in_refs:
        wide = ref.shape[1]
        loads.append(
            pltpu.make_async_copy(ref, w_ref.at[:, at : at + wide], load_sem.at[len(loads)])
        )
        at += wide
    at = 0
    for ref in out_refs:
        tall = ref.shape[0]
        loads.append(pltpu.make_async_copy(ref, wo_ref.at[at : at + tall], load_sem.at[len(loads)]))
        at += tall
    for load in loads:
        load.start()
    greet()
    for load in loads:
        load.wait()
    into.start()

    for k, ref in enumerate(head_gains):
        small_ref[k : k + 1, :] = jnp.concatenate([ref[...], ref[...]], axis=1)
    small_ref[4:8, :] = fixed_ref[...]
    step = 16

    @pl.loop(0, length // step)
    def _(i):
        rows = pl.ds(pl.multiple_of(i * step, step), step)
        values = x_ref[rows, :].astype(jnp.float32)
        mean = jnp.mean(values * values, axis=-1, keepdims=True)
        xn[rows, :] = (values * lax.rsqrt(mean + EPS) * gain_ref[...]).astype(jnp.bfloat16)

    def columns(o):
        return pl.ds(pl.multiple_of(o * depth, depth), depth)

    proj[...] = jnp.dot(xn[:, columns(s)], w_ref[...], preferred_element_type=jnp.float32)

    band = 64 if length % 64 == 0 else length

    @pl.loop(0, length // band)
    def _(i):
        rows = pl.ds(pl.multiple_of(i * band, band), band)
        shape = (band, LANES)
        place = lax.broadcasted_iota(jnp.int32, shape, 0) + (s * length + i * band)
        lane = lax.broadcasted_iota(jnp.int32, shape, 1)
        spot = jnp.where(lax.rem(lane, HD) < HD // 2, place // GRID_W, lax.rem(place, GRID_W))
        for k, where in enumerate((place, spot)):
            angles = where.astype(jnp.float32) * small_ref[4 + k : 5 + k, :]
            tables_ref[2 * k, rows, :] = jnp.cos(angles)
            tables_ref[2 * k + 1, rows, :] = jnp.sin(angles) * small_ref[6 + k : 7 + k, :]

    def add(o):
        proj[...] += jnp.dot(xn[:, columns(o)], wbuf[o], preferred_element_type=jnp.float32)

    into.run(add, last=lambda: out.start(0, 1))

    win_q, win_k, den_q, den_k = (0, 0, 32), (1, 0, 32), (2, 1, 16), (3, 1, 16)
    kinds = (
        [win_q] * q_heads + [den_q] * q_heads + [den_k] * kv_heads + [None] * kv_heads
        + [win_k] * kv_heads + [None] * kv_heads
    )
    q_tiles = 2 * q_heads * HD // LANES
    kv_tiles = 2 * kv_heads * HD // LANES

    def finished(i):
        return head_tile(
            proj[:, i * LANES : (i + 1) * LANES], kinds[2 * i : 2 * i + 2], small_ref, tables_ref
        )

    for i in range(kv_tiles):
        ext[WINDOW : WINDOW + length, i * LANES : (i + 1) * LANES] = finished(
            q_tiles + kv_tiles + i
        ).astype(jnp.bfloat16)
    for i in range(kv_tiles):
        kvd[s, :, i * LANES : (i + 1) * LANES] = finished(q_tiles + i).astype(jnp.bfloat16)

    def halo(side):
        source = pl.ds(length, WINDOW) if side == 0 else pl.ds(WINDOW, WINDOW)
        target = pl.ds(0, WINDOW) if side == 0 else pl.ds(WINDOW + length, WINDOW)
        peer = lax.rem(s + 1, n) if side == 0 else lax.rem(s + n - 1, n)
        return pltpu.make_async_remote_copy(
            src_ref=ext.at[source], dst_ref=ext.at[target], send_sem=halo_send.at[side],
            recv_sem=halo_recv.at[side], device_id={"sp": peer}, device_id_type=MESH,
        )

    has_right, has_left = s + 1 < n, s > 0

    @pl.when(has_right)
    def _():
        halo(0).start()

    @pl.when(has_left)
    def _():
        halo(1).start()

    keys.start()
    none = jnp.zeros((WINDOW, ext.shape[1]), jnp.bfloat16)

    @pl.when(jnp.logical_not(has_left))
    def _():
        ext[0:WINDOW, :] = none

    @pl.when(jnp.logical_not(has_right))
    def _():
        ext[WINDOW + length : WINDOW + length + WINDOW, :] = none

    group = q_heads // kv_heads

    def place(head):
        return head // 2, head % 2

    for i in range(q_tiles):
        tile = finished(i) * HD ** (-0.5)
        for b in range(2):
            head = 2 * i + b
            half = place((head % q_heads) // group)[1]
            moved = tile if half == b else pltpu.roll(tile, HD, 1)
            zero = jnp.zeros_like(moved)
            kept = by_half(moved, zero) if half == 0 else by_half(zero, moved)
            qs[head] = kept.astype(jnp.bfloat16)

    @pl.when(has_left)
    def _():
        halo(0).wait_recv()

    @pl.when(has_right)
    def _():
        halo(1).wait_recv()

    total_len = length * n

    def joined(results, heads):
        placed = []
        for b in range(2):
            half = place(kv_heads + heads[b] // group)[1]
            placed.append(results[b] if half == b else pltpu.roll(results[b], HD, 1))
        return by_half(placed[0], placed[1]).astype(jnp.bfloat16)

    def tile_of(head):
        return pl.ds(place(head)[0] * LANES, LANES)

    nt = (((1,), (1,)), ((), ()))

    def windowed(pair):
        @pl.loop(0, length // WINDOW)
        def _(b):
            base = pl.multiple_of(b * WINDOW, WINDOW)
            rows = pl.ds(base, WINDOW)
            near = pl.ds(base, 3 * WINDOW)
            shape = (WINDOW, 3 * WINDOW)
            at = lax.broadcasted_iota(jnp.int32, shape, 1) - WINDOW
            away = at - lax.broadcasted_iota(jnp.int32, shape, 0)
            pos = at + (s * length + base)
            valid = (away <= WINDOW) & (away >= -WINDOW) & (pos >= 0) & (pos < total_len)
            results = []
            for head in (2 * pair, 2 * pair + 1):
                key = ext[near, tile_of(head // group)]
                value = ext[near, tile_of(kv_heads + head // group)]
                scores = lax.dot_general(qs[head, rows, :], key, nt, preferred_element_type=jnp.float32)
                scores = jnp.where(valid, scores, -jnp.inf)
                floor = sink_ref[0, head]
                top = jnp.maximum(jnp.max(scores, axis=-1, keepdims=True), floor)
                expon = jnp.exp(scores - top)
                total = jnp.sum(expon, axis=-1, keepdims=True) + jnp.exp(floor - top)
                weights = (expon / total).astype(jnp.bfloat16)
                results.append(jnp.dot(weights, value, preferred_element_type=jnp.float32))
            att[rows, pair * LANES : (pair + 1) * LANES] = joined(results, (2 * pair, 2 * pair + 1))

    pairs = q_heads // 2
    keys.forward(1)
    windowed(0)

    @pl.loop(2, n)
    def _(d):
        keys.forward(d)

    out.start(1)
    for pair in range(1, pairs):
        windowed(pair)

    def dense(pair):
        @pl.loop(0, length // LANES)
        def _(b):
            rows = pl.ds(pl.multiple_of(b * LANES, LANES), LANES)
            results = []
            for head in (2 * pair, 2 * pair + 1):
                key = kvd[:, :, tile_of(head // group)].reshape(total_len, LANES)
                value = kvd[:, :, tile_of(kv_heads + head // group)].reshape(total_len, LANES)
                scores = lax.dot_general(
                    qs[q_heads + head, rows, :], key, nt, preferred_element_type=jnp.float32
                )
                top = jnp.max(scores, axis=-1, keepdims=True)
                expon = jnp.exp(scores - top)
                total = jnp.sum(expon, axis=-1, keepdims=True)
                summed = jnp.dot(
                    expon.astype(jnp.bfloat16), value, preferred_element_type=jnp.float32
                )
                results.append(summed / total)
            at = (pairs + pair) * LANES
            att[rows, at : at + LANES] = joined(results, (2 * pair, 2 * pair + 1))

    dense(0)
    out.forward(1)
    for pair in range(1, pairs):
        dense(pair)

    share = length // n_tp

    wide = wo_ref.shape[1]
    part_cols = wide // HALVES
    mine = lax.axis_index("grp")

    def span(h):
        return pl.ds(pl.multiple_of(h * part_cols, part_cols), part_cols)

    def exchange(o, h, j):
        peer = lax.rem(t + j, n_tp)
        return pltpu.make_async_remote_copy(
            src_ref=part.at[o, pl.ds(pl.multiple_of(peer * share, share), share), span(h)],
            dst_ref=rs.at[t, o, :, span(h)], send_sem=rs_send.at[j - 1, o, h],
            recv_sem=rs_recv.at[t, o, h], device_id={"tp": peer}, device_id_type=MESH,
        )

    def arrived(o, h, j):
        source = lax.rem(t + n_tp - j, n_tp)
        there = rs.at[source, o, :, span(h)]
        return pltpu.make_async_remote_copy(
            src_ref=there, dst_ref=there, send_sem=rs_send.at[j - 1, o, h],
            recv_sem=rs_recv.at[source, o, h], device_id={"tp": source}, device_id_type=MESH,
        )

    def emit(o, h, weight):
        part[o, :, span(h)] = jnp.dot(
            att[...], weight, preferred_element_type=jnp.float32
        ).astype(jnp.bfloat16)
        for j in range(1, n_tp):
            exchange(o, h, j).start()
        rs[t, o, :, span(h)] = part[o, pl.ds(pl.multiple_of(t * share, share), share), span(h)]

    def collect(o, h):
        for j in range(1, n_tp):
            arrived(o, h, j).wait_recv()
        total = rs[0, o, :, span(h)].astype(jnp.float32)
        for g in range(1, n_tp):
            total += rs[g, o, :, span(h)].astype(jnp.float32)
        columns_out = pl.ds(pl.multiple_of(o * wide + h * part_cols, part_cols), part_cols)
        out_ref[:, columns_out] = total.astype(jnp.bfloat16)

    for h in range(HALVES):
        emit(s, h, wo_ref[:, span(h)])
    out.rest(
        lambda o: emit(o, 1 - mine, wo_all[o, :, span(1 - mine)]),
        near=lambda o: emit(o, mine, wo_all[o, :, span(mine)]),
    )

    @pl.loop(0, n)
    def _(d):
        o = lax.rem(s + d, n)
        for h in range(HALVES):
            collect(o, h)

    @pl.loop(0, n)
    def _(o):
        for h in range(HALVES):
            for j in range(1, n_tp):
                exchange(o, h, j).wait_send()

    @pl.when(has_right)
    def _():
        halo(0).wait_send()

    @pl.when(has_left)
    def _():
        halo(1).wait_send()

    into.finish()
    out.finish()
    keys.finish()


def local_ring(
    tokens_in,
    norm_gain,
    window_query,
    window_key,
    window_value,
    window_query_gain,
    window_key_gain,
    sink_logit,
    dense_query,
    dense_key,
    dense_value,
    dense_query_gain,
    dense_key_gain,
    window_out,
    dense_out,
):
    length, width = tokens_in.shape
    n, n_tp = lax.axis_size("sp"), lax.axis_size("tp")
    q_heads, kv_heads = window_query.shape[1] // HD, window_key.shape[1] // HD
    weights, held = [], []
    for weight in (window_query, dense_query, dense_key, dense_value, window_key, window_value):
        held.append(weight)
        if sum(w.shape[1] for w in held) % LANES == 0:
            weights.append(held[0] if len(held) == 1 else jnp.concatenate(held, axis=1))
            held = []
    depth, in_cols = window_query.shape[0], sum(w.shape[1] for w in weights)
    out_rows, out_cols = window_out.shape[0] + dense_out.shape[0], window_out.shape[1]

    lane = np.arange(LANES)
    fixed = np.stack(
        [THETA ** (-2.0 * (lane % (wide // 2)) / wide) for wide in (HD, HD // 2)]
        + [np.where(lane % wide < wide // 2, -1.0, 1.0) for wide in (HD, HD // 2)]
    ).astype(np.float32)
    gains = [g[None, :] for g in (window_query_gain, window_key_gain, dense_query_gain, dense_key_gain)]

    def gather(chunks):
        return [pltpu.SemaphoreType.DMA((n, chunks)) for _ in range(5)]

    in_chunks = 8 if n <= 4 else 1
    out_chunks = out_cols // HALVES // LANES if n <= 4 else 1
    kv_cols = 2 * kv_heads * HD
    vmem = pl.BlockSpec(memory_space=pltpu.VMEM)
    share = length // n_tp
    return pl.pallas_call(
        functools.partial(layer_kernel, (q_heads, kv_heads, len(weights))),
        out_shape=jax.ShapeDtypeStruct((share, width), jnp.bfloat16),
        in_specs=[vmem] * 7
        + [pl.BlockSpec(memory_space=pltpu.SMEM)]
        + [pl.BlockSpec(memory_space=pl.ANY)] * (len(weights) + 2),
        out_specs=vmem,
        scratch_shapes=[
            pltpu.VMEM((8, LANES), jnp.float32),
            pltpu.VMEM((depth, in_cols), jnp.bfloat16),
            pltpu.VMEM((out_rows, out_cols), jnp.bfloat16),
            pltpu.VMEM((4, length, LANES), jnp.float32),
            pltpu.SemaphoreType.DMA((len(weights) + 2,)),
            pltpu.VMEM((length, width), jnp.bfloat16),
            pltpu.VMEM((length, in_cols), jnp.float32),
            pltpu.VMEM((n, depth, in_cols), jnp.bfloat16),
            pltpu.VMEM((n, out_rows, out_cols), jnp.bfloat16),
            pltpu.VMEM((n, length, kv_cols), jnp.bfloat16),
            pltpu.VMEM((length + 2 * WINDOW, kv_cols), jnp.bfloat16),
            pltpu.VMEM((2 * q_heads, length, LANES), jnp.bfloat16),
            pltpu.VMEM((length, out_rows), jnp.bfloat16),
            pltpu.VMEM((n, length, out_cols), jnp.bfloat16),
            pltpu.VMEM((n_tp, n, share, out_cols), jnp.bfloat16),
            pltpu.SemaphoreType.DMA((2,)),
            pltpu.SemaphoreType.DMA((2,)),
            pltpu.SemaphoreType.DMA((n_tp, n, HALVES)),
            pltpu.SemaphoreType.DMA((n_tp - 1, n, HALVES)),
        ]
        + gather(in_chunks)
        + gather(out_chunks)
        + [pltpu.SemaphoreType.DMA((n, 2 if n <= 4 else 1)) for _ in range(3)],
        compiler_params=pltpu.CompilerParams(
            collective_id=0, has_side_effects=True, vmem_limit_bytes=62 * 1024 * 1024
        ),
    )(tokens_in, norm_gain[None, :], fixed, *gains, sink_logit[None, :], *weights, window_out, dense_out)


KINDS = 4
SHARED = (True, False, False, False)
RECEIVES, SENDS, LOCALS = 131, 16, 9

def pair_kernel(sizes, *refs):
    gain_ref, fixed_ref, g0, g1, g2, g3, sink_ref, x_hbm = refs[:8]
    weights, outs, out_ref = refs[8:14], refs[14:16], refs[16]
    run_pairs(sizes, gain_ref, fixed_ref, (g0, g1, g2, g3), sink_ref, x_hbm, weights, outs, out_ref, *refs[17:])


def run_pairs(
    sizes, gain_ref, fixed_ref, head_gains, sink_ref, x_hbm, weights, outs, out_ref,
    small_ref, tables_ref, xv, xn, wbuf, wo, proj, kvd, ext, qs, att, part, dbuf, xsend, xrecv, mpart, mbuf, msum,
    recv_sem, send_sem, load_sem,
):
    q_heads, kv_heads, chunks, out_chunks = sizes
    n, s = lax.axis_size("sp"), lax.axis_index("sp")
    n_tp, t = lax.axis_size("tp"), lax.axis_index("tp")
    g = lax.axis_index("grp")
    length, width = xv.shape
    depth, cols = wbuf.shape[2], wbuf.shape[3]
    out_rows, out_cols = wo.shape[1], wo.shape[2]
    share = length // n_tp
    low = 2 * s < n
    high = jnp.logical_not(low)
    inner = (s > 0) & (s < n - 1)
    outer = jnp.logical_not(inner)
    step = jnp.where(low, 1, -1)
    inward = s + step
    outward = lax.rem(s - step + n, n)
    core, chip = lax.rem(t, 2), t // 2
    twin = t + 1 - 2 * core
    across = lax.rem(t + 2, n_tp)
    diagonal = lax.rem(twin + 2, n_tp)

    def place_of(j):
        if j == 0:
            return s
        return jnp.where(inner, (s - step, s - step, s + step, s + 2 * step)[j], s + j * step)

    sent = {"inner": {}, "outer": {}}
    names = {}

    def recv_at(*name):
        at = names.setdefault(name, len(names))
        assert at < recv_sem.shape[0]
        return recv_sem.at[at]

    def whole(when, group):
        many = when == "inner"
        return {
            "w": lambda: wbuf.at[0] if many else wbuf.at[1:KINDS, 0],
            "w0": lambda: wbuf.at[0, 0, 0:half],
            "wy": lambda: wbuf.at[0],
            "o": lambda: wo.at[0],
            "oo": lambda: wo.at[0],
            "oy": lambda: wo.at[0],
            "x": lambda: xn.at[0:share],
            "xx": lambda: xn.at[0:share],
            "xd": lambda: xn.at[0:share],
            "xe": lambda: xn.at[0:share],
            "kv": lambda: kvd.at[0:2],
            "halo": lambda: ext.at[0, 0:WINDOW],
            "att": lambda: att.at[0],
            "d": lambda: dbuf if many else dbuf.at[0:3],
            "r": lambda: xrecv,
            "md": lambda: mbuf,
            "m": lambda: msum,
        }[group]()

    def remote(when, name, ends, group=None):
        at = sent[when].setdefault(group or name[0], len(sent[when]))
        assert at < send_sem.shape[0]
        src, dst, peer = ends()
        pltpu.make_async_remote_copy(
            src_ref=src, dst_ref=dst, send_sem=send_sem.at[at], recv_sem=recv_at(*name),
            device_id=peer, device_id_type=MESH,
        ).start()

    def landed(ref, name, peer):
        sem = recv_at(*name)
        pltpu.make_async_remote_copy(
            src_ref=ref, dst_ref=ref, send_sem=sem, recv_sem=sem, device_id=peer, device_id_type=MESH
        ).wait_recv()

    z_in, z_out, y_peer = {"sp": inward}, {"sp": outward}, {"grp": 1 - g}

    half = depth // HALVES
    size = half // chunks

    def w_at(k, slot, rel, c):
        h = g if rel == 0 else 1 - g
        return wbuf.at[k, slot, pl.ds(pl.multiple_of(h * half + c * size, size), size)]

    def w_inward(role, k, slot, rel, c):
        to = 1 if role == "outer" else slot + 2
        remote(
            role, ("w", k, to, rel, c), lambda: (w_at(k, slot, rel, c), w_at(k, to, rel, c), z_in),
            "w0" if role == "outer" and k == 0 else "w",
        )

    def w_landed(k, slot, rel, c):
        landed(w_at(k, slot, rel, c), ("w", k, slot, rel, c), z_out if slot == 1 else z_in)

    def w_twin(k, slot, c):
        remote(
            "inner", ("wy", k, slot, c), lambda: (w_at(k, slot, 0, c), w_at(k, slot, 0, c), y_peer),
            "w0" if slot == 1 else "wy",
        )

    def w_twin_landed(k, slot, c):
        landed(w_at(k, slot, 1, c), ("wy", k, slot, c), y_peer)

    out_half = out_cols // HALVES
    out_size = out_half // out_chunks

    def o_at(slot, rel, c):
        h = g if rel == 0 else 1 - g
        return wo.at[slot, :, pl.ds(pl.multiple_of(h * out_half + c * out_size, out_size), out_size)]

    def o_inward(role, slot, rel, c):
        to = 1 if role == "outer" else slot + 2
        remote(role, ("o", to, rel, c), lambda: (o_at(slot, rel, c), o_at(to, rel, c), z_in))

    def o_outward(slot, c):
        to = 1 if slot == 0 else slot
        remote("inner", ("o", to, 0, c), lambda: (o_at(slot, 0, c), o_at(to, 0, c), z_out), "oo")

    def o_landed(slot, rel, c, peer):
        landed(o_at(slot, rel, c), ("o", slot, rel, c), peer)

    def o_twin(role, slot, c):
        remote(role, ("oy", slot, c), lambda: (o_at(slot, 0, c), o_at(slot, 0, c), y_peer))

    def o_twin_landed(slot, c):
        landed(o_at(slot, 1, c), ("oy", slot, c), y_peer)

    def x_rows(quarter):
        return pl.ds(pl.multiple_of(length + quarter * share, share), share)

    def x_cols(p):
        return pl.ds(p * depth, depth)

    def x_relay(p):
        def piece():
            return xn.at[x_rows(t), x_cols(p)]

        landed(piece(), ("x", p), z_out)
        remote("inner", ("xx", p), lambda: (piece(), piece(), {"tp": across}))
        remote("inner", ("xd", p), lambda: (piece(), piece(), {"tp": twin}))

    def x_pass(p):
        def piece():
            return xn.at[x_rows(across), x_cols(p)]

        landed(piece(), ("xx", p), {"tp": across})
        remote("inner", ("xe", p), lambda: (piece(), piece(), {"tp": twin}))

    def x_all(p):
        landed(xn.at[x_rows(twin), x_cols(p)], ("xd", p), {"tp": twin})
        landed(xn.at[x_rows(diagonal), x_cols(p)], ("xe", p), {"tp": twin})

    kv_cols = cols // 2
    loads = []

    def load(src, dst):
        copy = pltpu.make_async_copy(src, dst, load_sem.at[len(loads)])
        loads.append(copy)
        copy.start()

    wq, dq, dk, dv, wk, wv = weights
    load(dk, wbuf.at[0, 0, :, 0:kv_cols])
    load(dv, wbuf.at[0, 0, :, kv_cols:cols])
    load(x_hbm, xv)
    load(dq, wbuf.at[1, 0])
    load(wk, wbuf.at[2, 0, :, 0:kv_cols])
    load(wv, wbuf.at[2, 0, :, kv_cols:cols])
    load(wq, wbuf.at[3, 0])
    rows_of = outs[0].shape[0]
    load(outs[0], wo.at[0, 0:rows_of])
    load(outs[1], wo.at[0, rows_of:out_rows])
    greet()

    all_chunks, all_out = range(chunks), range(out_chunks)
    loads[0].wait()
    loads[1].wait()

    for role, test in (("inner", inner), ("outer", outer)):

        @pl.when(test)
        def _():
            for c in all_chunks:
                w_inward(role, 0, 0, 0, c)

    for k, ref in enumerate(head_gains):
        small_ref[k : k + 1, :] = jnp.concatenate([ref[...], ref[...]], axis=1)
    small_ref[4:8, :] = fixed_ref[...]
    loads[2].wait()

    def normalize(first, count):
        stripe = 16

        @pl.loop(0, count // stripe)
        def _(i):
            at = pl.multiple_of(i * stripe, stripe)
            values = xv[pl.ds(first + at, stripe), :].astype(jnp.float32)
            mean = jnp.mean(values * values, axis=-1, keepdims=True)
            xn[pl.ds(at, stripe), :] = (values * lax.rsqrt(mean + EPS) * gain_ref[...]).astype(jnp.bfloat16)

    band = 64

    def tables(first, count):
        @pl.loop(0, count // band)
        def _(i):
            at = pl.multiple_of(i * band, band) + first
            rows = pl.ds(at, band)
            shape = (band, LANES)
            base = jnp.where(at < length, s * length + at, (s - step) * length + at - length)
            place = lax.broadcasted_iota(jnp.int32, shape, 0) + base
            lane = lax.broadcasted_iota(jnp.int32, shape, 1)
            spot = jnp.where(lax.rem(lane, HD) < HD // 2, place // GRID_W, lax.rem(place, GRID_W))
            for k, where in enumerate((place, spot)):
                angles = where.astype(jnp.float32) * small_ref[4 + k : 5 + k, :]
                tables_ref[2 * k, rows, :] = jnp.cos(angles)
                tables_ref[2 * k + 1, rows, :] = jnp.sin(angles) * small_ref[6 + k : 7 + k, :]

    def project(k, j, sides=(0, 1)):
        at = pl.multiple_of(place_of(j) * depth, depth)

        @pl.loop(sides[0], sides[-1] + 1)
        def _(i):
            rows = pl.ds(pl.multiple_of(i * length, length), length)
            found = jnp.dot(xn[rows, pl.ds(at, depth)], wbuf[k, j], preferred_element_type=jnp.float32)
            proj[k % 2, rows, :] = found if j == 0 else proj[k % 2, rows, :] + found

    den_q, den_k, win_q, win_k = (2, 1, 16), (3, 1, 16), (0, 0, 32), (1, 0, 32)
    plans = ((den_k, None), (den_q, den_q), (win_k, None), (win_q, win_q))
    group = q_heads // kv_heads
    pairs = q_heads // 2

    def finished(k, side):
        rows = pl.ds(side * length, length)
        for tile in range(cols // LANES):
            lanes = pl.ds(tile * LANES, LANES)
            kind = plans[k][tile * 2 * LANES // cols]
            value = proj[k % 2, rows, lanes]
            if kind is not None:
                value = head_tile(
                    value, (kind, kind), small_ref, [tables_ref.at[m][rows, :] for m in range(4)]
                )
            if k % 2:
                value = value * HD ** (-0.5)
                zero = jnp.zeros_like(value)
                for b in range(2):
                    head = 2 * tile + b
                    half_of = head // group % 2
                    moved = value if half_of == b else pltpu.roll(value, HD, 1)
                    kept = by_half(moved, zero) if half_of == 0 else by_half(zero, moved)
                    qs[k // 2, side, head] = kept.astype(jnp.bfloat16)
            elif k == 0:
                kvd[side, :, lanes] = value.astype(jnp.bfloat16)
            else:
                ext[side, pl.ds(WINDOW, length), lanes] = value.astype(jnp.bfloat16)

    def mates(k, c):
        w_landed(k, 1, 0, c)
        w_inward("inner", k, 1, 0, c)
        if SHARED[k]:
            w_twin(k, 1, c)

    def crossing(k, slot, c):
        w_landed(k, slot, 0, c)
        w_twin(k, slot, c)

    def mate_ready(k):
        for c in all_chunks:
            if SHARED[k]:
                w_twin_landed(k, 1, c)
            else:
                w_landed(k, 1, 1, c)

    def twin_ready(k, slot):
        for c in all_chunks:
            w_twin_landed(k, slot, c)

    def o_mates(c):
        o_landed(1, 0, c, z_out)
        o_inward("inner", 1, 0, c)

    def o_crossing(slot, c):
        o_landed(slot, 0, c, z_in)
        if slot < 3:
            o_outward(slot, c)
        o_twin("inner", slot, c)

    def o_outer(slot, c):
        o_landed(slot, 0, c, z_in)
        o_twin("outer", slot, c)

    def edge(first):
        return pl.ds(jnp.where(first, WINDOW, length), WINDOW)

    def halo_at(leading):
        return pl.ds(jnp.where(leading, 0, WINDOW + length), WINDOW)

    def halo_inward():
        remote("inner", ("halo",), lambda: (ext.at[0, edge(high)], ext.at[0, halo_at(low)], z_in))

    def halo_landed():
        landed(ext.at[0, halo_at(high)], ("halo",), z_in)

    def halo_local():
        ext[0, halo_at(low), :] = ext[1, edge(high), :]
        ext[1, halo_at(high), :] = ext[0, edge(low), :]
        ext[1, halo_at(low), :] = jnp.zeros((WINDOW, cols), jnp.bfloat16)

    def kv_landed(j):
        landed(kvd.at[j], ("kv", j), z_in)

    def kv_inward(j):
        remote("inner", ("kv", j + 2), lambda: (kvd.at[j], kvd.at[j + 2], z_in))

    def x_inward(p):
        remote("outer", ("x", p), lambda: (xn.at[0:share, x_cols(p)], xn.at[x_rows(t), x_cols(p)], z_in))

    def att_at(side, i):
        return att.at[side, :, i * LANES : (i + 1) * LANES]

    def att_outward(i):
        remote("inner", ("att", i), lambda: (att_at(1, i), att_at(0, i), z_out))

    def att_landed(i):
        landed(att_at(0, i), ("att", i), z_in)

    def joined(results, pair):
        side = (kv_heads + pair * 2 // group) % 2
        placed = [results[b] if side == b else pltpu.roll(results[b], HD, 1) for b in range(2)]
        return by_half(placed[0], placed[1]).astype(jnp.bfloat16)

    def tile_of(head):
        return pl.ds(head // 2 * LANES, LANES)

    nt = (((1,), (1,)), ((), ()))
    total_len = length * n

    def windowed(side, pair):
        start = (s if side == 0 else s - step) * length
        shape = (2 * WINDOW, 3 * WINDOW)
        row = lax.rem(lax.broadcasted_iota(jnp.int32, shape, 0), WINDOW)
        at = lax.broadcasted_iota(jnp.int32, shape, 1) - WINDOW
        near_by = (at - row <= WINDOW) & (at - row >= -WINDOW)
        first = lax.broadcasted_iota(jnp.int32, (2 * WINDOW, 1), 0) < WINDOW
        floor = jnp.where(first, sink_ref[0, 2 * pair], sink_ref[0, 2 * pair + 1])
        blocks = range(length // WINDOW)
        near = [pl.ds(b * WINDOW, 3 * WINDOW) for b in blocks]
        rows = [pl.ds(b * WINDOW, WINDOW) for b in blocks]
        scores, expon, total = [], [], []
        for b in blocks:
            key = ext[side, near[b], tile_of(2 * pair // group)]
            query = qs[1, side, 2 * pair : 2 * pair + 2, rows[b], :].reshape(2 * WINDOW, LANES)
            pos = at + (start + b * WINDOW)
            valid = near_by & (pos >= 0) & (pos < total_len)
            found = lax.dot_general(query, key, nt, preferred_element_type=jnp.float32)
            scores.append(jnp.where(valid, found, -jnp.inf))
        tops = [jnp.maximum(jnp.max(score, axis=-1, keepdims=True), floor) for score in scores]
        for score, top in zip(scores, tops):
            expon.append(jnp.exp(score - top))
            total.append(jnp.sum(expon[-1], axis=-1, keepdims=True) + jnp.exp(floor - top))
        for b in blocks:
            value = ext[side, near[b], tile_of(kv_heads + 2 * pair // group)]
            weight = (expon[b] / total[b]).astype(jnp.bfloat16)
            found = jnp.dot(weight, value, preferred_element_type=jnp.float32)
            att[side, rows[b], pair * LANES : (pair + 1) * LANES] = joined((found[:WINDOW], found[WINDOW:]), pair)

    def dense(side, pair):
        @pl.loop(0, length // LANES)
        def _(b):
            rows = pl.ds(pl.multiple_of(b * LANES, LANES), LANES)
            key = kvd[:, :, tile_of(2 * pair // group)].reshape(total_len, LANES)
            value = kvd[:, :, tile_of(kv_heads + 2 * pair // group)].reshape(total_len, LANES)
            query = qs[0, side, 2 * pair : 2 * pair + 2, rows, :].reshape(2 * LANES, LANES)
            scores = lax.dot_general(query, key, nt, preferred_element_type=jnp.float32)
            top = jnp.max(scores, axis=-1, keepdims=True)
            expon = jnp.exp(scores - top)
            total = jnp.sum(expon, axis=-1, keepdims=True)
            summed = jnp.dot(expon.astype(jnp.bfloat16), value, preferred_element_type=jnp.float32) / total
            at = (pairs + pair) * LANES
            att[side, rows, at : at + LANES] = joined((summed[:LANES], summed[LANES:]), pair)

    @pl.when(outer)
    def _():
        normalize(t * share, share)
        for p in range(width // depth):
            x_inward(p)
        for one in loads[3:]:
            one.wait()
        for k, rel in ((1, 0), (2, 0), (1, 1), (3, 0), (2, 1), (3, 1)):
            for c in all_chunks:
                w_inward("outer", k, 0, rel, c)
        for rel in range(2):
            for c in all_out:
                o_inward("outer", 0, rel, c)
        for c in all_out:
            o_outer(1, c)
        for i in range(pairs, 2 * pairs):
            att_landed(i)

    @pl.when(inner)
    def _():
        for one in loads[3:]:
            one.wait()
        for c in all_out:
            o_outward(0, c)
        normalize(0, length)
        for c in all_chunks:
            mates(0, c)
            crossing(0, 2, c)
        for k in range(1, KINDS):
            for c in all_chunks:
                w_inward("inner", k, 0, 0, c)
        tables(0, length)
        for c in all_chunks:
            crossing(0, 3, c)
        x_relay(0)
        tables(length, length)
        crossing(1, 2, 0)
        x_relay(1)
        crossing(1, 2, 1)
        x_pass(0)
        x_relay(2)
        crossing(2, 2, 0)
        x_pass(1)
        x_relay(3)
        crossing(2, 2, 1)
        mate_ready(0)
        for j in range(2, 4):
            twin_ready(0, j)
        for j in range(4):
            project(0, j, (0,))
        finished(0, 0)
        kv_inward(0)
        x_pass(2)
        crossing(3, 2, 0)
        mates(1, 0)
        x_pass(3)
        crossing(3, 2, 1)
        mates(1, 1)
        for p in range(width // depth):
            x_all(p)
        for j in range(4):
            project(0, j, (1,))
        finished(0, 1)
        kv_inward(1)
        project(1, 0)
        twin_ready(1, 2)
        project(1, 2)
        mates(2, 0)
        crossing(1, 3, 0)
        project(2, 0)
        mates(2, 1)
        crossing(1, 3, 1)
        twin_ready(2, 2)
        project(2, 2)
        mate_ready(1)
        project(1, 1)
        twin_ready(1, 3)
        project(1, 3)
        finished(1, 1)
        finished(1, 0)
        kv_landed(2)
        kv_landed(3)
        crossing(2, 3, 0)
        mates(3, 0)
        dense(1, 0)
        att_outward(pairs)
        crossing(2, 3, 1)
        mates(3, 1)
        for c in range(2):
            o_inward("inner", 0, 0, c)
        dense(1, 1)
        att_outward(pairs + 1)
        crossing(3, 3, 0)
        dense(0, 0)
        mate_ready(2)
        project(2, 1)
        crossing(3, 3, 1)
        twin_ready(2, 3)
        project(2, 3)
        project(3, 0)
        finished(2, 1)
        finished(2, 0)
        halo_inward()
        for c in range(2, out_chunks):
            o_inward("inner", 0, 0, c)
        halo_local()
        twin_ready(3, 2)
        project(3, 2)
        mate_ready(3)
        project(3, 1)
        o_crossing(2, 0)
        twin_ready(3, 3)
        project(3, 3, (1,))
        finished(3, 1)
        windowed(1, 0)
        att_outward(0)
        windowed(1, 1)
        att_outward(1)
        o_crossing(2, 1)
        o_mates(0)
        project(3, 3, (0,))
        finished(3, 0)
        halo_landed()
        o_mates(1)
        windowed(0, 0)
        o_crossing(2, 2)
        windowed(0, 1)
        o_mates(2)
        dense(0, 1)
        o_crossing(2, 3)
        o_mates(3)
        o_crossing(3, 0)

    @pl.when(outer)
    def _():
        o_outer(2, 0)
        for i in range(pairs):
            att_landed(i)

    def span(rel, first=0, count=out_chunks):
        h = g if rel == 0 else 1 - g
        return pl.ds(pl.multiple_of(h * out_half + first * out_size, out_size), count * out_size)

    def tail(role, script):
        def emit(*piece):
            j, lanes = piece[0], span(*piece[1:])
            found = jnp.dot(att[0], wo[j, :, lanes], preferred_element_type=jnp.float32).astype(jnp.bfloat16)
            for dest in range(n_tp):
                part[j, dest % 2, dest // 2, :, lanes] = found[dest * share : (dest + 1) * share]
            remote(role, ("d",) + piece, lambda: (
                part.at[j, 1 - core, :, :, span(*piece[1:])], dbuf.at[j, :, :, span(*piece[1:])], {"tp": twin}
            ))

        def combine(*piece):
            j, lanes = piece[0], span(*piece[1:])
            landed(dbuf.at[j, :, :, lanes], ("d",) + piece, {"tp": twin})
            both = (
                part[j, core, 1 - chip, :, lanes].astype(jnp.float32) + dbuf[j, 1 - chip, :, lanes].astype(jnp.float32)
            )
            xsend[j, :, lanes] = both.astype(jnp.bfloat16)
            remote(role, ("r",) + piece, lambda: (
                xsend.at[j, :, span(*piece[1:])], xrecv.at[j, :, span(*piece[1:])], {"tp": across}
            ))

        def emit_mate(*piece):
            j, lanes = piece[0], span(*piece[1:])
            found = jnp.dot(att[1], wo[j, :, lanes], preferred_element_type=jnp.float32).astype(jnp.bfloat16)
            for dest in range(n_tp):
                mpart[dest % 2, dest // 2, :, lanes] = found[dest * share : (dest + 1) * share]
            remote(role, ("md",) + piece, lambda: (
                mpart.at[1 - core, :, :, span(*piece[1:])], mbuf.at[:, :, span(*piece[1:])], {"tp": twin}
            ))

        def combine_mate(*piece):
            lanes = span(*piece[1:])
            landed(mbuf.at[:, :, lanes], ("md",) + piece, {"tp": twin})
            both = mpart[core, :, :, lanes].astype(jnp.float32) + mbuf[:, :, lanes].astype(jnp.float32)
            msum[:, :, lanes] = both.astype(jnp.bfloat16)
            remote(role, ("m",) + piece, lambda: (
                msum.at[:, :, span(*piece[1:])], msum.at[:, :, span(*piece[1:])], z_out
            ))

        def relay(*piece):
            landed(msum.at[:, :, span(*piece[1:])], ("m",) + piece, z_in)
            remote(role, ("r",) + piece, lambda: (
                msum.at[1 - chip, :, span(*piece[1:])], xrecv.at[piece[0], :, span(*piece[1:])], {"tp": across}
            ))

        def settle(*piece):
            j, lanes = piece[0], span(*piece[1:])
            landed(xrecv.at[j, :, lanes], ("r",) + piece, {"tp": across})
            if role == "outer" and j == 3:
                near = msum[chip, :, lanes].astype(jnp.float32)
            else:
                near = part[j, core, chip, :, lanes].astype(jnp.float32) + dbuf[j, chip, :, lanes].astype(jnp.float32)
            total = near + xrecv[j, :, lanes].astype(jnp.float32)
            rel, first, count = piece[1:] if len(piece) > 2 else (piece[1], 0, out_chunks)
            h = g if rel == 0 else 1 - g
            base = place_of(j) * out_cols + h * out_half + first * out_size
            out_ref[:, pl.ds(pl.multiple_of(base, out_size), count * out_size)] = total.astype(jnp.bfloat16)

        def ready(j, first=0, count=out_chunks):
            for c in range(first, first + count):
                if role == "inner" and j == 1:
                    o_landed(1, 1, c, z_out)
                else:
                    o_twin_landed(j, c)

        def pump(j, c):
            if role == "inner":
                o_crossing(j, c)
            else:
                o_outer(j, c)

        words = {
            "emit": emit, "combine": combine, "settle": settle, "ready": ready, "pump": pump,
            "emit_mate": emit_mate, "combine_mate": combine_mate, "relay": relay,
        }
        for word, *piece in script:
            words[word](*piece)

    opening = [("emit", 0, 0), ("emit", 0, 1), ("combine", 0, 0), ("emit", 1, 0), ("combine", 0, 1)]
    last = [(3, 1, 0, 2), (3, 1, 2, 1), (3, 1, 3, 1)]
    far = [(3, 0, 0, 2), (3, 0, 2, 2)] + last
    inner_script = (
        opening
        + [("emit", 2, 0), ("combine", 1, 0), ("pump", 3, 1), ("ready", 2), ("emit", 2, 1), ("combine", 2, 0)]
        + [("pump", 3, 2), ("combine", 2, 1), ("emit_mate",) + far[0], ("emit",) + far[0]]
        + [("pump", 3, 3), ("combine_mate",) + far[0], ("emit_mate",) + far[1], ("emit",) + far[1]]
        + [("combine",) + far[0], ("ready", 3, 0, 2), ("combine_mate",) + far[1], ("emit_mate",) + last[0]]
        + [("emit",) + last[0], ("combine",) + far[1], ("ready", 1), ("emit", 1, 1)]
        + [("combine_mate",) + last[0], ("combine",) + last[0], ("combine", 1, 1)]
        + [("ready", 3, 2, 1), ("emit_mate",) + last[1], ("emit",) + last[1]]
        + [("settle", 0, 0), ("settle", 0, 1), ("combine_mate",) + last[1]]
        + [("ready", 3, 3, 1), ("emit_mate",) + last[2], ("emit",) + last[2]]
        + [("combine",) + last[1], ("settle", 1, 0), ("combine_mate",) + last[2], ("combine",) + last[2]]
        + [("settle", 2, 0), ("settle", 2, 1), ("settle",) + far[0], ("settle",) + far[1]]
        + [("settle",) + last[0], ("settle", 1, 1)] + [("settle",) + piece for piece in last[1:]]
    )
    outer_script = (
        opening
        + [("pump", 2, 1), ("ready", 1), ("emit", 1, 1), ("combine", 1, 0), ("pump", 2, 2), ("combine", 1, 1)]
        + [("pump", 2, 3), ("emit", 2, 0), ("ready", 2, 0, 2), ("combine", 2, 0)]
        + [("ready", 2, 2, 2), ("emit", 2, 1), ("settle", 0, 0), ("relay",) + far[0], ("combine", 2, 1)]
        + [("settle", 0, 1), ("settle", 1, 0), ("relay",) + far[1], ("settle", 1, 1), ("relay",) + last[0]]
        + [("settle", 2, 0), ("relay",) + last[1], ("relay",) + last[2], ("settle", 2, 1)]
        + [("settle",) + piece for piece in far]
    )

    @pl.when(inner)
    def _():
        tail("inner", inner_script)

    @pl.when(outer)
    def _():
        tail("outer", outer_script)

    for role, test in (("inner", inner), ("outer", outer)):

        @pl.when(test)
        def _():
            for group, at in sent[role].items():
                ref = whole(role, group)
                pltpu.make_async_remote_copy(
                    src_ref=ref, dst_ref=ref, send_sem=send_sem.at[at], recv_sem=recv_sem.at[0],
                    device_id=y_peer, device_id_type=MESH,
                ).wait_send()


def local(*args):
    tokens_in, norm_gain, wq, wk, wv, wq_gain, wk_gain, sink, dq, dk, dv, dq_gain, dk_gain, w_out, d_out = args
    length, width = tokens_in.shape
    n, n_tp = lax.axis_size("sp"), lax.axis_size("tp")
    depth, cols = wq.shape
    paired = (
        n == 4 and n_tp == 4 and wk.shape[1] == LANES and cols == 2 * LANES and depth * n == width
        and length % (n_tp * 32) == 0 and length % WINDOW == 0
    )
    if not paired:
        return local_ring(*args)
    q_heads, kv_heads = cols // HD, wk.shape[1] // HD
    out_rows, out_cols = w_out.shape[0] + d_out.shape[0], w_out.shape[1]
    share = length // n_tp
    lane = np.arange(LANES)
    fixed = np.stack(
        [THETA ** (-2.0 * (lane % (wide // 2)) / wide) for wide in (HD, HD // 2)]
        + [np.where(lane % wide < wide // 2, -1.0, 1.0) for wide in (HD, HD // 2)]
    ).astype(np.float32)
    gains = [gain[None, :] for gain in (wq_gain, wk_gain, dq_gain, dk_gain)]
    chunks, out_chunks = 2, 4
    vmem = pl.BlockSpec(memory_space=pltpu.VMEM)
    bf16 = jnp.bfloat16

    def sem(*shape):
        return pltpu.SemaphoreType.DMA(shape)

    return pl.pallas_call(
        functools.partial(pair_kernel, (q_heads, kv_heads, chunks, out_chunks)),
        out_shape=pltpu.VMEM((share, width), bf16),
        in_specs=[vmem] * 6
        + [pl.BlockSpec(memory_space=pltpu.SMEM)]
        + [pl.BlockSpec(memory_space=pl.ANY)] * 9,
        out_specs=vmem,
        scratch_shapes=[
            pltpu.VMEM((8, LANES), jnp.float32),
            pltpu.VMEM((4, 2 * length, LANES), jnp.float32),
            pltpu.VMEM((length, width), bf16),
            pltpu.VMEM((2 * length, width), bf16),
            pltpu.VMEM((KINDS, n, depth, cols), bf16),
            pltpu.VMEM((n, out_rows, out_cols), bf16),
            pltpu.VMEM((2, 2 * length, cols), jnp.float32),
            pltpu.VMEM((n, length, cols), bf16),
            pltpu.VMEM((2, length + 2 * WINDOW, cols), bf16),
            pltpu.VMEM((2, 2, q_heads, length, LANES), bf16),
            pltpu.VMEM((2, length, out_rows), bf16),
            pltpu.VMEM((n, 2, n_tp // 2, share, out_cols), bf16),
            pltpu.VMEM((n, 2, share, out_cols), bf16),
            pltpu.VMEM((n, share, out_cols), bf16),
            pltpu.VMEM((n, share, out_cols), bf16),
            pltpu.VMEM((2, n_tp // 2, share, out_cols), bf16),
            pltpu.VMEM((n_tp // 2, share, out_cols), bf16),
            pltpu.VMEM((n_tp // 2, share, out_cols), bf16),
            sem(RECEIVES),
            sem(SENDS),
            sem(LOCALS),
        ],
        compiler_params=pltpu.CompilerParams(
            collective_id=0, has_side_effects=True, vmem_limit_bytes=62 * 1024 * 1024
        ),
    )(norm_gain[None, :], fixed, *gains, sink[None, :], tokens_in, wq, dq, dk, dv, wk, wv, w_out, d_out)


def solution(mesh):
    return jax.shard_map(
        local,
        mesh=mesh,
        in_specs=(
            P(("grp", "sp"), None),
            P(),
            P("sp", "tp"),
            P("sp", "tp"),
            P("sp", "tp"),
            P(),
            P(),
            P("tp"),
            P("sp", "tp"),
            P("sp", "tp"),
            P("sp", "tp"),
            P(),
            P(),
            P("tp", "sp"),
            P("tp", "sp"),
        ),
        out_specs=P(("grp", "sp", "tp"), None),
        check_vma=False,
    )
```

```python
import functools

import jax
import jax.numpy as jnp
import numpy as np
from jax import lax
from jax.experimental import pallas as pl
from jax.experimental.pallas import tpu as pltpu
from jax.sharding import PartitionSpec as P

HD = 64
WINDOW = 128
GRID_W = 64


EPS = 1e-06
THETA = 10000.0


MESH = pl.DeviceIdType.MESH
HALVES = 2


class LineGather:
    def __init__(self, own, buf, z_recv, r_send, l_send, y_recv=None, y_send=None, axis=0):
        self.own, self.buf = own, buf
        self.z_recv, self.y_recv = z_recv, y_recv
        self.r_send, self.l_send, self.y_send = r_send, l_send, y_send
        self.n = lax.axis_size("sp")
        self.s = lax.axis_index("sp")
        self.shared = y_recv is not None
        self.g = lax.axis_index("grp") if self.shared else 0
        self.chunks = z_recv.shape[1]
        self.axis = axis
        extent = buf.shape[1 + axis]
        self.half = extent // HALVES if self.shared else extent
        self.size = self.half // self.chunks

    def rows(self, half, c):
        piece = pl.ds(pl.multiple_of(half * self.half + c * self.size, self.size), self.size)
        return (piece,) if self.axis == 0 else (slice(None), piece)

    def block(self, o, half, c):
        return self.buf.at[(o,) + self.rows(half, c)]

    def copy(self, src, o, c, sem, recv, target, half):
        return pltpu.make_async_remote_copy(
            src_ref=src,
            dst_ref=self.block(o, half, c),
            send_sem=sem.at[o, c],
            recv_sem=recv.at[o, c],
            device_id=target,
            device_id_type=MESH,
        )

    def right(self, src, o, c):
        return self.copy(src, o, c, self.r_send, self.z_recv, {"sp": lax.rem(self.s + 1, self.n)}, self.g)

    def left(self, src, o, c):
        return self.copy(
            src, o, c, self.l_send, self.z_recv, {"sp": lax.rem(self.s + self.n - 1, self.n)}, self.g
        )

    def twin(self, o, c, half):
        return self.copy(
            self.block(o, half, c), o, c, self.y_send, self.y_recv, {"grp": 1 - self.g}, half
        )

    def mine(self, c):
        if self.own is None:
            return self.block(self.s, self.g, c)
        return self.own.at[self.rows(self.g, c)]

    def start(self, first=0, last=None):
        for c in range(first, self.chunks if last is None else last):
            mine = self.mine(c)

            @pl.when(self.s + 1 < self.n)
            def _():
                self.right(mine, self.s, c).start()

            @pl.when(self.s > 0)
            def _():
                self.left(mine, self.s, c).start()

    def forward(self, d):
        for c in range(self.chunks):

            @pl.when(self.s - d >= 0)
            def _():
                o = self.s - d
                there = self.block(o, self.g, c)
                self.right(there, o, c).wait_recv()

                @pl.when(self.s + 1 < self.n)
                def _():
                    self.right(there, o, c).start()

                if self.shared:
                    self.twin(o, c, self.g).start()

            @pl.when(self.s + d < self.n)
            def _():
                o = self.s + d
                there = self.block(o, self.g, c)
                self.left(there, o, c).wait_recv()

                @pl.when(self.s > 0)
                def _():
                    self.left(there, o, c).start()

                if self.shared:
                    self.twin(o, c, self.g).start()

    def use(self, d, fn, near=None):
        for there, o in ((self.s - d >= 0, self.s - d), (self.s + d < self.n, self.s + d)):
            if near is not None:

                @pl.when(there)
                def _():
                    near(o)

        for there, o in ((self.s - d >= 0, self.s - d), (self.s + d < self.n, self.s + d)):

            @pl.when(there)
            def _():
                for c in range(self.chunks):
                    self.twin(o, c, 1 - self.g).wait_recv()
                fn(o)

    def run(self, fn, near=None, last=None):
        self.forward(1)
        self.rest(fn, near, last)

    def rest(self, fn, near=None, last=None):
        @pl.loop(2, self.n)
        def _(d):
            self.forward(d)
            self.use(d - 1, fn, near)

        if last is not None:
            last()
        self.use(self.n - 1, fn, near)

    def finish(self):
        @pl.loop(0, self.n)
        def _(o):
            for c in range(self.chunks):
                there = self.block(o, self.g, c)

                @pl.when((o <= self.s) & (self.s + 1 < self.n))
                def _():
                    self.right(there, o, c).wait_send()

                @pl.when((o >= self.s) & (self.s > 0))
                def _():
                    self.left(there, o, c).wait_send()

                if self.shared:

                    @pl.when(o != self.s)
                    def _():
                        self.twin(o, c, self.g).wait_send()


def greet():
    n, s, g = lax.axis_size("sp"), lax.axis_index("sp"), lax.axis_index("grp")
    n_tp, t = lax.axis_size("tp"), lax.axis_index("tp")
    barrier = pltpu.get_barrier_semaphore()
    pl.semaphore_signal(barrier, inc=1, device_id={"grp": 1 - g}, device_id_type=MESH)
    for j in range(1, n_tp):
        pl.semaphore_signal(barrier, inc=1, device_id={"tp": lax.rem(t + j, n_tp)}, device_id_type=MESH)

    @pl.when(s + 1 < n)
    def _():
        pl.semaphore_signal(barrier, inc=1, device_id={"sp": lax.rem(s + 1, n)}, device_id_type=MESH)

    @pl.when(s > 0)
    def _():
        pl.semaphore_signal(barrier, inc=1, device_id={"sp": lax.rem(s + n - 1, n)}, device_id_type=MESH)

    pl.semaphore_wait(barrier, n_tp + (s + 1 < n).astype(jnp.int32) + (s > 0).astype(jnp.int32))


LANES = 128


def by_half(low, high):
    lane = lax.broadcasted_iota(jnp.int32, low.shape, 1)
    return jnp.where(lane < HD, low, high)


def swap_pairs(values, reach):
    lane = lax.broadcasted_iota(jnp.int32, values.shape, 1)
    ahead = pltpu.roll(values, LANES - reach, 1)
    behind = pltpu.roll(values, reach, 1)
    return jnp.where(lax.rem(lane, 2 * reach) < reach, ahead, behind)


def head_tile(tile, kinds, gains_ref, tables_ref):
    square = tile * tile
    zero = jnp.zeros_like(square)
    low = jnp.sum(by_half(square, zero), axis=-1, keepdims=True)
    high = jnp.sum(by_half(zero, square), axis=-1, keepdims=True)
    mean = by_half(jnp.broadcast_to(low, tile.shape), jnp.broadcast_to(high, tile.shape)) * (1.0 / HD)
    scaled = tile * lax.rsqrt(mean + EPS)

    def one(kind):
        if kind is None:
            return tile
        gain, table, reach = kind
        normed = scaled * gains_ref[gain : gain + 1, :]
        return normed * tables_ref[2 * table] + swap_pairs(normed, reach) * tables_ref[2 * table + 1]

    if kinds[0] == kinds[1]:
        return one(kinds[0])
    return by_half(one(kinds[0]), one(kinds[1]))


def layer_kernel(
    sizes, x_ref, gain_ref, fixed_ref, g0, g1, g2, g3, sink_ref, *refs
):
    n_in = sizes[2]
    in_refs, out_refs = refs[:n_in], refs[n_in : n_in + 2]
    run_layer(sizes[:2], x_ref, gain_ref, fixed_ref, (g0, g1, g2, g3), sink_ref, in_refs, out_refs, *refs[n_in + 2 :])


def run_layer(
    sizes, x_ref, gain_ref, fixed_ref, head_gains, sink_ref, in_refs, out_refs, out_ref,
    small_ref, w_ref, wo_ref, tables_ref, load_sem, xn, proj, wbuf, wo_all, kvd, ext, qs, att, part, rs, halo_recv, halo_send, rs_recv, rs_send, *sems
):
    q_heads, kv_heads = sizes
    n, s = lax.axis_size("sp"), lax.axis_index("sp")
    n_tp, t = lax.axis_size("tp"), lax.axis_index("tp")
    depth = w_ref.shape[0]
    length = x_ref.shape[0]
    into = LineGather(w_ref, wbuf, *sems[:5])
    out = LineGather(wo_ref, wo_all, *sems[5:10], axis=1)
    keys = LineGather(None, kvd, *sems[10:])
    loads, at = [], 0
    for ref in in_refs:
        wide = ref.shape[1]
        loads.append(
            pltpu.make_async_copy(ref, w_ref.at[:, at : at + wide], load_sem.at[len(loads)])
        )
        at += wide
    at = 0
    for ref in out_refs:
        tall = ref.shape[0]
        loads.append(pltpu.make_async_copy(ref, wo_ref.at[at : at + tall], load_sem.at[len(loads)]))
        at += tall
    for load in loads:
        load.start()
    greet()
    for load in loads:
        load.wait()
    into.start()

    for k, ref in enumerate(head_gains):
        small_ref[k : k + 1, :] = jnp.concatenate([ref[...], ref[...]], axis=1)
    small_ref[4:8, :] = fixed_ref[...]
    step = 16

    @pl.loop(0, length // step)
    def _(i):
        rows = pl.ds(pl.multiple_of(i * step, step), step)
        values = x_ref[rows, :].astype(jnp.float32)
        mean = jnp.mean(values * values, axis=-1, keepdims=True)
        xn[rows, :] = (values * lax.rsqrt(mean + EPS) * gain_ref[...]).astype(jnp.bfloat16)

    def columns(o):
        return pl.ds(pl.multiple_of(o * depth, depth), depth)

    proj[...] = jnp.dot(xn[:, columns(s)], w_ref[...], preferred_element_type=jnp.float32)

    band = 64 if length % 64 == 0 else length

    @pl.loop(0, length // band)
    def _(i):
        rows = pl.ds(pl.multiple_of(i * band, band), band)
        shape = (band, LANES)
        place = lax.broadcasted_iota(jnp.int32, shape, 0) + (s * length + i * band)
        lane = lax.broadcasted_iota(jnp.int32, shape, 1)
        spot = jnp.where(lax.rem(lane, HD) < HD // 2, place // GRID_W, lax.rem(place, GRID_W))
        for k, where in enumerate((place, spot)):
            angles = where.astype(jnp.float32) * small_ref[4 + k : 5 + k, :]
            tables_ref[2 * k, rows, :] = jnp.cos(angles)
            tables_ref[2 * k + 1, rows, :] = jnp.sin(angles) * small_ref[6 + k : 7 + k, :]

    def add(o):
        proj[...] += jnp.dot(xn[:, columns(o)], wbuf[o], preferred_element_type=jnp.float32)

    into.run(add, last=lambda: out.start(0, 1))

    win_q, win_k, den_q, den_k = (0, 0, 32), (1, 0, 32), (2, 1, 16), (3, 1, 16)
    kinds = (
        [win_q] * q_heads + [den_q] * q_heads + [den_k] * kv_heads + [None] * kv_heads
        + [win_k] * kv_heads + [None] * kv_heads
    )
    q_tiles = 2 * q_heads * HD // LANES
    kv_tiles = 2 * kv_heads * HD // LANES

    def finished(i):
        return head_tile(
            proj[:, i * LANES : (i + 1) * LANES], kinds[2 * i : 2 * i + 2], small_ref, tables_ref
        )

    for i in range(kv_tiles):
        ext[WINDOW : WINDOW + length, i * LANES : (i + 1) * LANES] = finished(
            q_tiles + kv_tiles + i
        ).astype(jnp.bfloat16)
    for i in range(kv_tiles):
        kvd[s, :, i * LANES : (i + 1) * LANES] = finished(q_tiles + i).astype(jnp.bfloat16)

    def halo(side):
        source = pl.ds(length, WINDOW) if side == 0 else pl.ds(WINDOW, WINDOW)
        target = pl.ds(0, WINDOW) if side == 0 else pl.ds(WINDOW + length, WINDOW)
        peer = lax.rem(s + 1, n) if side == 0 else lax.rem(s + n - 1, n)
        return pltpu.make_async_remote_copy(
            src_ref=ext.at[source], dst_ref=ext.at[target], send_sem=halo_send.at[side],
            recv_sem=halo_recv.at[side], device_id={"sp": peer}, device_id_type=MESH,
        )

    has_right, has_left = s + 1 < n, s > 0

    @pl.when(has_right)
    def _():
        halo(0).start()

    @pl.when(has_left)
    def _():
        halo(1).start()

    keys.start()
    none = jnp.zeros((WINDOW, ext.shape[1]), jnp.bfloat16)

    @pl.when(jnp.logical_not(has_left))
    def _():
        ext[0:WINDOW, :] = none

    @pl.when(jnp.logical_not(has_right))
    def _():
        ext[WINDOW + length : WINDOW + length + WINDOW, :] = none

    group = q_heads // kv_heads

    def place(head):
        return head // 2, head % 2

    for i in range(q_tiles):
        tile = finished(i) * HD ** (-0.5)
        for b in range(2):
            head = 2 * i + b
            half = place((head % q_heads) // group)[1]
            moved = tile if half == b else pltpu.roll(tile, HD, 1)
            zero = jnp.zeros_like(moved)
            kept = by_half(moved, zero) if half == 0 else by_half(zero, moved)
            qs[head] = kept.astype(jnp.bfloat16)

    @pl.when(has_left)
    def _():
        halo(0).wait_recv()

    @pl.when(has_right)
    def _():
        halo(1).wait_recv()

    total_len = length * n

    def joined(results, heads):
        placed = []
        for b in range(2):
            half = place(kv_heads + heads[b] // group)[1]
            placed.append(results[b] if half == b else pltpu.roll(results[b], HD, 1))
        return by_half(placed[0], placed[1]).astype(jnp.bfloat16)

    def tile_of(head):
        return pl.ds(place(head)[0] * LANES, LANES)

    nt = (((1,), (1,)), ((), ()))

    def windowed(pair):
        @pl.loop(0, length // WINDOW)
        def _(b):
            base = pl.multiple_of(b * WINDOW, WINDOW)
            rows = pl.ds(base, WINDOW)
            near = pl.ds(base, 3 * WINDOW)
            shape = (WINDOW, 3 * WINDOW)
            at = lax.broadcasted_iota(jnp.int32, shape, 1) - WINDOW
            away = at - lax.broadcasted_iota(jnp.int32, shape, 0)
            pos = at + (s * length + base)
            valid = (away <= WINDOW) & (away >= -WINDOW) & (pos >= 0) & (pos < total_len)
            results = []
            for head in (2 * pair, 2 * pair + 1):
                key = ext[near, tile_of(head // group)]
                value = ext[near, tile_of(kv_heads + head // group)]
                scores = lax.dot_general(qs[head, rows, :], key, nt, preferred_element_type=jnp.float32)
                scores = jnp.where(valid, scores, -jnp.inf)
                floor = sink_ref[0, head]
                top = jnp.maximum(jnp.max(scores, axis=-1, keepdims=True), floor)
                expon = jnp.exp(scores - top)
                total = jnp.sum(expon, axis=-1, keepdims=True) + jnp.exp(floor - top)
                weights = (expon / total).astype(jnp.bfloat16)
                results.append(jnp.dot(weights, value, preferred_element_type=jnp.float32))
            att[rows, pair * LANES : (pair + 1) * LANES] = joined(results, (2 * pair, 2 * pair + 1))

    pairs = q_heads // 2
    keys.forward(1)
    windowed(0)

    @pl.loop(2, n)
    def _(d):
        keys.forward(d)

    out.start(1)
    for pair in range(1, pairs):
        windowed(pair)

    def dense(pair):
        @pl.loop(0, length // LANES)
        def _(b):
            rows = pl.ds(pl.multiple_of(b * LANES, LANES), LANES)
            results = []
            for head in (2 * pair, 2 * pair + 1):
                key = kvd[:, :, tile_of(head // group)].reshape(total_len, LANES)
                value = kvd[:, :, tile_of(kv_heads + head // group)].reshape(total_len, LANES)
                scores = lax.dot_general(
                    qs[q_heads + head, rows, :], key, nt, preferred_element_type=jnp.float32
                )
                top = jnp.max(scores, axis=-1, keepdims=True)
                expon = jnp.exp(scores - top)
                total = jnp.sum(expon, axis=-1, keepdims=True)
                summed = jnp.dot(
                    expon.astype(jnp.bfloat16), value, preferred_element_type=jnp.float32
                )
                results.append(summed / total)
            at = (pairs + pair) * LANES
            att[rows, at : at + LANES] = joined(results, (2 * pair, 2 * pair + 1))

    dense(0)
    out.forward(1)
    for pair in range(1, pairs):
        dense(pair)

    share = length // n_tp

    wide = wo_ref.shape[1]
    part_cols = wide // HALVES
    mine = lax.axis_index("grp")

    def span(h):
        return pl.ds(pl.multiple_of(h * part_cols, part_cols), part_cols)

    def exchange(o, h, j):
        peer = lax.rem(t + j, n_tp)
        return pltpu.make_async_remote_copy(
            src_ref=part.at[o, pl.ds(pl.multiple_of(peer * share, share), share), span(h)],
            dst_ref=rs.at[t, o, :, span(h)], send_sem=rs_send.at[j - 1, o, h],
            recv_sem=rs_recv.at[t, o, h], device_id={"tp": peer}, device_id_type=MESH,
        )

    def arrived(o, h, j):
        source = lax.rem(t + n_tp - j, n_tp)
        there = rs.at[source, o, :, span(h)]
        return pltpu.make_async_remote_copy(
            src_ref=there, dst_ref=there, send_sem=rs_send.at[j - 1, o, h],
            recv_sem=rs_recv.at[source, o, h], device_id={"tp": source}, device_id_type=MESH,
        )

    def emit(o, h, weight):
        part[o, :, span(h)] = jnp.dot(
            att[...], weight, preferred_element_type=jnp.float32
        ).astype(jnp.bfloat16)
        for j in range(1, n_tp):
            exchange(o, h, j).start()
        rs[t, o, :, span(h)] = part[o, pl.ds(pl.multiple_of(t * share, share), share), span(h)]

    def collect(o, h):
        for j in range(1, n_tp):
            arrived(o, h, j).wait_recv()
        total = rs[0, o, :, span(h)].astype(jnp.float32)
        for g in range(1, n_tp):
            total += rs[g, o, :, span(h)].astype(jnp.float32)
        columns_out = pl.ds(pl.multiple_of(o * wide + h * part_cols, part_cols), part_cols)
        out_ref[:, columns_out] = total.astype(jnp.bfloat16)

    for h in range(HALVES):
        emit(s, h, wo_ref[:, span(h)])
    out.rest(
        lambda o: emit(o, 1 - mine, wo_all[o, :, span(1 - mine)]),
        near=lambda o: emit(o, mine, wo_all[o, :, span(mine)]),
    )

    @pl.loop(0, n)
    def _(d):
        o = lax.rem(s + d, n)
        for h in range(HALVES):
            collect(o, h)

    @pl.loop(0, n)
    def _(o):
        for h in range(HALVES):
            for j in range(1, n_tp):
                exchange(o, h, j).wait_send()

    @pl.when(has_right)
    def _():
        halo(0).wait_send()

    @pl.when(has_left)
    def _():
        halo(1).wait_send()

    into.finish()
    out.finish()
    keys.finish()


def local_ring(
    tokens_in,
    norm_gain,
    window_query,
    window_key,
    window_value,
    window_query_gain,
    window_key_gain,
    sink_logit,
    dense_query,
    dense_key,
    dense_value,
    dense_query_gain,
    dense_key_gain,
    window_out,
    dense_out,
):
    length, width = tokens_in.shape
    n, n_tp = lax.axis_size("sp"), lax.axis_size("tp")
    q_heads, kv_heads = window_query.shape[1] // HD, window_key.shape[1] // HD
    weights, held = [], []
    for weight in (window_query, dense_query, dense_key, dense_value, window_key, window_value):
        held.append(weight)
        if sum(w.shape[1] for w in held) % LANES == 0:
            weights.append(held[0] if len(held) == 1 else jnp.concatenate(held, axis=1))
            held = []
    depth, in_cols = window_query.shape[0], sum(w.shape[1] for w in weights)
    out_rows, out_cols = window_out.shape[0] + dense_out.shape[0], window_out.shape[1]

    lane = np.arange(LANES)
    fixed = np.stack(
        [THETA ** (-2.0 * (lane % (wide // 2)) / wide) for wide in (HD, HD // 2)]
        + [np.where(lane % wide < wide // 2, -1.0, 1.0) for wide in (HD, HD // 2)]
    ).astype(np.float32)
    gains = [g[None, :] for g in (window_query_gain, window_key_gain, dense_query_gain, dense_key_gain)]

    def gather(chunks):
        return [pltpu.SemaphoreType.DMA((n, chunks)) for _ in range(5)]

    in_chunks = 8 if n <= 4 else 1
    out_chunks = out_cols // HALVES // LANES if n <= 4 else 1
    kv_cols = 2 * kv_heads * HD
    vmem = pl.BlockSpec(memory_space=pltpu.VMEM)
    share = length // n_tp
    return pl.pallas_call(
        functools.partial(layer_kernel, (q_heads, kv_heads, len(weights))),
        out_shape=jax.ShapeDtypeStruct((share, width), jnp.bfloat16),
        in_specs=[vmem] * 7
        + [pl.BlockSpec(memory_space=pltpu.SMEM)]
        + [pl.BlockSpec(memory_space=pl.ANY)] * (len(weights) + 2),
        out_specs=vmem,
        scratch_shapes=[
            pltpu.VMEM((8, LANES), jnp.float32),
            pltpu.VMEM((depth, in_cols), jnp.bfloat16),
            pltpu.VMEM((out_rows, out_cols), jnp.bfloat16),
            pltpu.VMEM((4, length, LANES), jnp.float32),
            pltpu.SemaphoreType.DMA((len(weights) + 2,)),
            pltpu.VMEM((length, width), jnp.bfloat16),
            pltpu.VMEM((length, in_cols), jnp.float32),
            pltpu.VMEM((n, depth, in_cols), jnp.bfloat16),
            pltpu.VMEM((n, out_rows, out_cols), jnp.bfloat16),
            pltpu.VMEM((n, length, kv_cols), jnp.bfloat16),
            pltpu.VMEM((length + 2 * WINDOW, kv_cols), jnp.bfloat16),
            pltpu.VMEM((2 * q_heads, length, LANES), jnp.bfloat16),
            pltpu.VMEM((length, out_rows), jnp.bfloat16),
            pltpu.VMEM((n, length, out_cols), jnp.bfloat16),
            pltpu.VMEM((n_tp, n, share, out_cols), jnp.bfloat16),
            pltpu.SemaphoreType.DMA((2,)),
            pltpu.SemaphoreType.DMA((2,)),
            pltpu.SemaphoreType.DMA((n_tp, n, HALVES)),
            pltpu.SemaphoreType.DMA((n_tp - 1, n, HALVES)),
        ]
        + gather(in_chunks)
        + gather(out_chunks)
        + [pltpu.SemaphoreType.DMA((n, 2 if n <= 4 else 1)) for _ in range(3)],
        compiler_params=pltpu.CompilerParams(
            collective_id=0, has_side_effects=True, vmem_limit_bytes=62 * 1024 * 1024
        ),
    )(tokens_in, norm_gain[None, :], fixed, *gains, sink_logit[None, :], *weights, window_out, dense_out)


KINDS = 4
SHARED = (True, False, False, False)
RECEIVES, SENDS, LOCALS = 131, 16, 9

def pair_kernel(sizes, *refs):
    gain_ref, fixed_ref, g0, g1, g2, g3, sink_ref, x_hbm = refs[:8]
    weights, outs, out_ref = refs[8:14], refs[14:16], refs[16]
    run_pairs(sizes, gain_ref, fixed_ref, (g0, g1, g2, g3), sink_ref, x_hbm, weights, outs, out_ref, *refs[17:])


def run_pairs(
    sizes, gain_ref, fixed_ref, head_gains, sink_ref, x_hbm, weights, outs, out_ref,
    small_ref, tables_ref, xv, xn, wbuf, wo, proj, kvd, ext, qs, att, part, dbuf, xsend, xrecv, mpart, mbuf, msum,
    recv_sem, send_sem, load_sem,
):
    q_heads, kv_heads, chunks, out_chunks = sizes
    n, s = lax.axis_size("sp"), lax.axis_index("sp")
    n_tp, t = lax.axis_size("tp"), lax.axis_index("tp")
    g = lax.axis_index("grp")
    length, width = xv.shape
    depth, cols = wbuf.shape[2], wbuf.shape[3]
    out_rows, out_cols = wo.shape[1], wo.shape[2]
    share = length // n_tp
    low = 2 * s < n
    high = jnp.logical_not(low)
    inner = (s > 0) & (s < n - 1)
    outer = jnp.logical_not(inner)
    step = jnp.where(low, 1, -1)
    inward = s + step
    outward = lax.rem(s - step + n, n)
    core, chip = lax.rem(t, 2), t // 2
    twin = t + 1 - 2 * core
    across = lax.rem(t + 2, n_tp)
    diagonal = lax.rem(twin + 2, n_tp)

    def place_of(j):
        if j == 0:
            return s
        return jnp.where(inner, (s - step, s - step, s + step, s + 2 * step)[j], s + j * step)

    sent = {"inner": {}, "outer": {}}
    names = {}

    def recv_at(*name):
        at = names.setdefault(name, len(names))
        assert at < recv_sem.shape[0]
        return recv_sem.at[at]

    def whole(when, group):
        many = when == "inner"
        return {
            "w": lambda: wbuf.at[0] if many else wbuf.at[1:KINDS, 0],
            "w0": lambda: wbuf.at[0, 0, 0:half],
            "wy": lambda: wbuf.at[0],
            "o": lambda: wo.at[0],
            "oo": lambda: wo.at[0],
            "oy": lambda: wo.at[0],
            "x": lambda: xn.at[0:share],
            "xx": lambda: xn.at[0:share],
            "xd": lambda: xn.at[0:share],
            "xe": lambda: xn.at[0:share],
            "kv": lambda: kvd.at[0:2],
            "halo": lambda: ext.at[0, 0:WINDOW],
            "att": lambda: att.at[0],
            "d": lambda: dbuf if many else dbuf.at[0:3],
            "r": lambda: xrecv if many else xrecv.at[0:3],
            "md": lambda: mbuf,
            "m": lambda: msum,
        }[group]()

    def remote(when, name, ends, group=None):
        at = sent[when].setdefault(group or name[0], len(sent[when]))
        assert at < send_sem.shape[0]
        src, dst, peer = ends()
        pltpu.make_async_remote_copy(
            src_ref=src, dst_ref=dst, send_sem=send_sem.at[at], recv_sem=recv_at(*name),
            device_id=peer, device_id_type=MESH,
        ).start()

    def landed(ref, name, peer):
        sem = recv_at(*name)
        pltpu.make_async_remote_copy(
            src_ref=ref, dst_ref=ref, send_sem=sem, recv_sem=sem, device_id=peer, device_id_type=MESH
        ).wait_recv()

    z_in, z_out, y_peer = {"sp": inward}, {"sp": outward}, {"grp": 1 - g}

    half = depth // HALVES
    size = half // chunks

    def w_at(k, slot, rel, c):
        h = g if rel == 0 else 1 - g
        return wbuf.at[k, slot, pl.ds(pl.multiple_of(h * half + c * size, size), size)]

    def w_inward(role, k, slot, rel, c):
        to = 1 if role == "outer" else slot + 2
        remote(
            role, ("w", k, to, rel, c), lambda: (w_at(k, slot, rel, c), w_at(k, to, rel, c), z_in),
            "w0" if role == "outer" and k == 0 else "w",
        )

    def w_landed(k, slot, rel, c):
        landed(w_at(k, slot, rel, c), ("w", k, slot, rel, c), z_out if slot == 1 else z_in)

    def w_twin(k, slot, c):
        remote(
            "inner", ("wy", k, slot, c), lambda: (w_at(k, slot, 0, c), w_at(k, slot, 0, c), y_peer),
            "w0" if slot == 1 else "wy",
        )

    def w_twin_landed(k, slot, c):
        landed(w_at(k, slot, 1, c), ("wy", k, slot, c), y_peer)

    out_half = out_cols // HALVES
    out_size = out_half // out_chunks

    def o_at(slot, rel, c):
        h = g if rel == 0 else 1 - g
        return wo.at[slot, :, pl.ds(pl.multiple_of(h * out_half + c * out_size, out_size), out_size)]

    def o_inward(role, slot, rel, c):
        to = 1 if role == "outer" else slot + 2
        remote(role, ("o", to, rel, c), lambda: (o_at(slot, rel, c), o_at(to, rel, c), z_in))

    def o_outward(slot, c):
        to = 1 if slot == 0 else slot
        remote("inner", ("o", to, 0, c), lambda: (o_at(slot, 0, c), o_at(to, 0, c), z_out), "oo")

    def o_landed(slot, rel, c, peer):
        landed(o_at(slot, rel, c), ("o", slot, rel, c), peer)

    def o_twin(role, slot, c):
        remote(role, ("oy", slot, c), lambda: (o_at(slot, 0, c), o_at(slot, 0, c), y_peer))

    def o_twin_landed(slot, c):
        landed(o_at(slot, 1, c), ("oy", slot, c), y_peer)

    def x_rows(quarter):
        return pl.ds(pl.multiple_of(length + quarter * share, share), share)

    def x_cols(p):
        return pl.ds(p * depth, depth)

    def x_relay(p):
        def piece():
            return xn.at[x_rows(t), x_cols(p)]

        landed(piece(), ("x", p), z_out)
        remote("inner", ("xx", p), lambda: (piece(), piece(), {"tp": across}))
        remote("inner", ("xd", p), lambda: (piece(), piece(), {"tp": twin}))

    def x_pass(p):
        def piece():
            return xn.at[x_rows(across), x_cols(p)]

        landed(piece(), ("xx", p), {"tp": across})
        remote("inner", ("xe", p), lambda: (piece(), piece(), {"tp": twin}))

    def x_all(p):
        landed(xn.at[x_rows(twin), x_cols(p)], ("xd", p), {"tp": twin})
        landed(xn.at[x_rows(diagonal), x_cols(p)], ("xe", p), {"tp": twin})

    kv_cols = cols // 2
    loads = []

    def load(src, dst):
        copy = pltpu.make_async_copy(src, dst, load_sem.at[len(loads)])
        loads.append(copy)
        copy.start()

    wq, dq, dk, dv, wk, wv = weights
    load(dk, wbuf.at[0, 0, :, 0:kv_cols])
    load(dv, wbuf.at[0, 0, :, kv_cols:cols])
    load(x_hbm, xv)
    load(dq, wbuf.at[1, 0])
    load(wk, wbuf.at[2, 0, :, 0:kv_cols])
    load(wv, wbuf.at[2, 0, :, kv_cols:cols])
    load(wq, wbuf.at[3, 0])
    rows_of = outs[0].shape[0]
    load(outs[0], wo.at[0, 0:rows_of])
    load(outs[1], wo.at[0, rows_of:out_rows])
    greet()

    all_chunks, all_out = range(chunks), range(out_chunks)
    loads[0].wait()
    loads[1].wait()

    for role, test in (("inner", inner), ("outer", outer)):

        @pl.when(test)
        def _():
            for c in all_chunks:
                w_inward(role, 0, 0, 0, c)

    for k, ref in enumerate(head_gains):
        small_ref[k : k + 1, :] = jnp.concatenate([ref[...], ref[...]], axis=1)
    small_ref[4:8, :] = fixed_ref[...]
    loads[2].wait()

    def normalize(first, count):
        stripe = 16

        @pl.loop(0, count // stripe)
        def _(i):
            at = pl.multiple_of(i * stripe, stripe)
            values = xv[pl.ds(first + at, stripe), :].astype(jnp.float32)
            mean = jnp.mean(values * values, axis=-1, keepdims=True)
            xn[pl.ds(at, stripe), :] = (values * lax.rsqrt(mean + EPS) * gain_ref[...]).astype(jnp.bfloat16)

    band = 64

    def tables(first, count):
        @pl.loop(0, count // band)
        def _(i):
            at = pl.multiple_of(i * band, band) + first
            rows = pl.ds(at, band)
            shape = (band, LANES)
            base = jnp.where(at < length, s * length + at, (s - step) * length + at - length)
            place = lax.broadcasted_iota(jnp.int32, shape, 0) + base
            lane = lax.broadcasted_iota(jnp.int32, shape, 1)
            spot = jnp.where(lax.rem(lane, HD) < HD // 2, place // GRID_W, lax.rem(place, GRID_W))
            for k, where in enumerate((place, spot)):
                angles = where.astype(jnp.float32) * small_ref[4 + k : 5 + k, :]
                tables_ref[2 * k, rows, :] = jnp.cos(angles)
                tables_ref[2 * k + 1, rows, :] = jnp.sin(angles) * small_ref[6 + k : 7 + k, :]

    def project(k, j, sides=(0, 1)):
        at = pl.multiple_of(place_of(j) * depth, depth)

        @pl.loop(sides[0], sides[-1] + 1)
        def _(i):
            rows = pl.ds(pl.multiple_of(i * length, length), length)
            found = jnp.dot(xn[rows, pl.ds(at, depth)], wbuf[k, j], preferred_element_type=jnp.float32)
            proj[k % 2, rows, :] = found if j == 0 else proj[k % 2, rows, :] + found

    den_q, den_k, win_q, win_k = (2, 1, 16), (3, 1, 16), (0, 0, 32), (1, 0, 32)
    plans = ((den_k, None), (den_q, den_q), (win_k, None), (win_q, win_q))
    group = q_heads // kv_heads
    pairs = q_heads // 2

    def finished(k, side):
        rows = pl.ds(side * length, length)
        for tile in range(cols // LANES):
            lanes = pl.ds(tile * LANES, LANES)
            kind = plans[k][tile * 2 * LANES // cols]
            value = proj[k % 2, rows, lanes]
            if kind is not None:
                value = head_tile(
                    value, (kind, kind), small_ref, [tables_ref.at[m][rows, :] for m in range(4)]
                )
            if k % 2:
                value = value * HD ** (-0.5)
                zero = jnp.zeros_like(value)
                for b in range(2):
                    head = 2 * tile + b
                    half_of = head // group % 2
                    moved = value if half_of == b else pltpu.roll(value, HD, 1)
                    kept = by_half(moved, zero) if half_of == 0 else by_half(zero, moved)
                    qs[k // 2, side, head] = kept.astype(jnp.bfloat16)
            elif k == 0:
                kvd[side, :, lanes] = value.astype(jnp.bfloat16)
            else:
                ext[side, pl.ds(WINDOW, length), lanes] = value.astype(jnp.bfloat16)

    def mates(k, c):
        w_landed(k, 1, 0, c)
        w_inward("inner", k, 1, 0, c)
        if SHARED[k]:
            w_twin(k, 1, c)

    def crossing(k, slot, c):
        w_landed(k, slot, 0, c)
        w_twin(k, slot, c)

    def mate_ready(k):
        for c in all_chunks:
            if SHARED[k]:
                w_twin_landed(k, 1, c)
            else:
                w_landed(k, 1, 1, c)

    def twin_ready(k, slot):
        for c in all_chunks:
            w_twin_landed(k, slot, c)

    def o_mates(c):
        o_landed(1, 0, c, z_out)
        o_inward("inner", 1, 0, c)

    def o_crossing(slot, c):
        o_landed(slot, 0, c, z_in)
        if slot < 3:
            o_outward(slot, c)
        o_twin("inner", slot, c)

    def o_outer(slot, c):
        o_landed(slot, 0, c, z_in)
        o_twin("outer", slot, c)

    def edge(first):
        return pl.ds(jnp.where(first, WINDOW, length), WINDOW)

    def halo_at(leading):
        return pl.ds(jnp.where(leading, 0, WINDOW + length), WINDOW)

    def halo_inward():
        remote("inner", ("halo",), lambda: (ext.at[0, edge(high)], ext.at[0, halo_at(low)], z_in))

    def halo_landed():
        landed(ext.at[0, halo_at(high)], ("halo",), z_in)

    def halo_local():
        ext[0, halo_at(low), :] = ext[1, edge(high), :]
        ext[1, halo_at(high), :] = ext[0, edge(low), :]
        ext[1, halo_at(low), :] = jnp.zeros((WINDOW, cols), jnp.bfloat16)

    def kv_landed(j):
        landed(kvd.at[j], ("kv", j), z_in)

    def kv_inward(j):
        remote("inner", ("kv", j + 2), lambda: (kvd.at[j], kvd.at[j + 2], z_in))

    def x_inward(p):
        remote("outer", ("x", p), lambda: (xn.at[0:share, x_cols(p)], xn.at[x_rows(t), x_cols(p)], z_in))

    def att_at(side, i):
        return att.at[side, :, i * LANES : (i + 1) * LANES]

    def att_outward(i):
        remote("inner", ("att", i), lambda: (att_at(1, i), att_at(0, i), z_out))

    def att_landed(i):
        landed(att_at(0, i), ("att", i), z_in)

    def joined(results, pair):
        side = (kv_heads + pair * 2 // group) % 2
        placed = [results[b] if side == b else pltpu.roll(results[b], HD, 1) for b in range(2)]
        return by_half(placed[0], placed[1]).astype(jnp.bfloat16)

    def tile_of(head):
        return pl.ds(head // 2 * LANES, LANES)

    nt = (((1,), (1,)), ((), ()))
    total_len = length * n

    def windowed(side, pair):
        start = (s if side == 0 else s - step) * length
        shape = (2 * WINDOW, 3 * WINDOW)
        row = lax.rem(lax.broadcasted_iota(jnp.int32, shape, 0), WINDOW)
        at = lax.broadcasted_iota(jnp.int32, shape, 1) - WINDOW
        near_by = (at - row <= WINDOW) & (at - row >= -WINDOW)
        first = lax.broadcasted_iota(jnp.int32, (2 * WINDOW, 1), 0) < WINDOW
        floor = jnp.where(first, sink_ref[0, 2 * pair], sink_ref[0, 2 * pair + 1])
        blocks = range(length // WINDOW)
        near = [pl.ds(b * WINDOW, 3 * WINDOW) for b in blocks]
        rows = [pl.ds(b * WINDOW, WINDOW) for b in blocks]
        scores, expon, total = [], [], []
        for b in blocks:
            key = ext[side, near[b], tile_of(2 * pair // group)]
            query = qs[1, side, 2 * pair : 2 * pair + 2, rows[b], :].reshape(2 * WINDOW, LANES)
            pos = at + (start + b * WINDOW)
            valid = near_by & (pos >= 0) & (pos < total_len)
            found = lax.dot_general(query, key, nt, preferred_element_type=jnp.float32)
            scores.append(jnp.where(valid, found, -jnp.inf))
        tops = [jnp.maximum(jnp.max(score, axis=-1, keepdims=True), floor) for score in scores]
        for score, top in zip(scores, tops):
            expon.append(jnp.exp(score - top))
            total.append(jnp.sum(expon[-1], axis=-1, keepdims=True) + jnp.exp(floor - top))
        for b in blocks:
            value = ext[side, near[b], tile_of(kv_heads + 2 * pair // group)]
            weight = (expon[b] / total[b]).astype(jnp.bfloat16)
            found = jnp.dot(weight, value, preferred_element_type=jnp.float32)
            att[side, rows[b], pair * LANES : (pair + 1) * LANES] = joined((found[:WINDOW], found[WINDOW:]), pair)

    def dense(side, pair, first=0, last=length // LANES):
        @pl.loop(first, last)
        def _(b):
            rows = pl.ds(pl.multiple_of(b * LANES, LANES), LANES)
            key = kvd[:, :, tile_of(2 * pair // group)].reshape(total_len, LANES)
            value = kvd[:, :, tile_of(kv_heads + 2 * pair // group)].reshape(total_len, LANES)
            query = qs[0, side, 2 * pair : 2 * pair + 2, rows, :].reshape(2 * LANES, LANES)
            scores = lax.dot_general(query, key, nt, preferred_element_type=jnp.float32)
            top = jnp.max(scores, axis=-1, keepdims=True)
            expon = jnp.exp(scores - top)
            total = jnp.sum(expon, axis=-1, keepdims=True)
            summed = jnp.dot(expon.astype(jnp.bfloat16), value, preferred_element_type=jnp.float32) / total
            at = (pairs + pair) * LANES
            att[side, rows, at : at + LANES] = joined((summed[:LANES], summed[LANES:]), pair)

    @pl.when(outer)
    def _():
        normalize(t * share, share)
        for p in range(width // depth):
            x_inward(p)
        for one in loads[3:]:
            one.wait()
        for k, rel in ((1, 0), (2, 0), (1, 1), (3, 0), (2, 1), (3, 1)):
            for c in all_chunks:
                w_inward("outer", k, 0, rel, c)
        for rel in range(2):
            for c in all_out:
                o_inward("outer", 0, rel, c)
        for c in all_out:
            o_outer(1, c)
        for i in range(pairs, 2 * pairs):
            att_landed(i)

    @pl.when(inner)
    def _():
        for one in loads[3:]:
            one.wait()
        for c in all_out:
            o_outward(0, c)
        normalize(0, length)
        for c in all_chunks:
            mates(0, c)
            crossing(0, 2, c)
        for k in range(1, KINDS):
            for c in all_chunks:
                w_inward("inner", k, 0, 0, c)
        tables(0, length)
        for c in all_chunks:
            crossing(0, 3, c)
        x_relay(0)
        tables(length, length)
        crossing(1, 2, 0)
        x_relay(1)
        crossing(1, 2, 1)
        x_pass(0)
        x_relay(2)
        crossing(2, 2, 0)
        x_pass(1)
        x_relay(3)
        crossing(2, 2, 1)
        mate_ready(0)
        for j in range(2, 4):
            twin_ready(0, j)
        for j in range(4):
            project(0, j, (0,))
        finished(0, 0)
        kv_inward(0)
        x_pass(2)
        crossing(3, 2, 0)
        mates(1, 0)
        x_pass(3)
        crossing(3, 2, 1)
        mates(1, 1)
        for p in range(width // depth):
            x_all(p)
        for j in range(4):
            project(0, j, (1,))
        finished(0, 1)
        kv_inward(1)
        project(1, 0)
        twin_ready(1, 2)
        project(1, 2)
        mates(2, 0)
        crossing(1, 3, 0)
        project(2, 0)
        mates(2, 1)
        crossing(1, 3, 1)
        twin_ready(2, 2)
        project(2, 2)
        mate_ready(1)
        project(1, 1)
        twin_ready(1, 3)
        project(1, 3)
        finished(1, 1)
        finished(1, 0)
        kv_landed(2)
        kv_landed(3)
        crossing(2, 3, 0)
        mates(3, 0)
        dense(1, 0)
        att_outward(pairs)
        crossing(2, 3, 1)
        mates(3, 1)
        for c in range(2):
            o_inward("inner", 0, 0, c)
        dense(1, 1)
        att_outward(pairs + 1)
        crossing(3, 3, 0)
        dense(0, 0)
        mate_ready(2)
        project(2, 1)
        crossing(3, 3, 1)
        twin_ready(2, 3)
        project(2, 3)
        project(3, 0)
        finished(2, 1)
        finished(2, 0)
        halo_inward()
        for c in range(2, out_chunks):
            o_inward("inner", 0, 0, c)
        halo_local()
        twin_ready(3, 2)
        project(3, 2)
        mate_ready(3)
        project(3, 1)
        o_crossing(2, 0)
        twin_ready(3, 3)
        project(3, 3, (1,))
        finished(3, 1)
        windowed(1, 0)
        att_outward(0)
        windowed(1, 1)
        att_outward(1)
        o_crossing(2, 1)
        o_mates(0)
        project(3, 3, (0,))
        finished(3, 0)
        halo_landed()
        o_mates(1)
        windowed(0, 0)
        o_crossing(2, 2)
        windowed(0, 1)
        o_mates(2)
        dense(0, 1, 0, 1)
        o_crossing(2, 3)
        dense(0, 1, 1, 2)
        o_mates(3)
        dense(0, 1, 2)

    @pl.when(outer)
    def _():
        o_outer(2, 0)
        for i in range(pairs):
            att_landed(i)

    def span(rel, first=0, count=out_chunks):
        h = g if rel == 0 else 1 - g
        return pl.ds(pl.multiple_of(h * out_half + first * out_size, out_size), count * out_size)

    def tail(role, script):
        def emit(*piece):
            j, lanes = piece[0], span(*piece[1:])
            found = jnp.dot(att[0], wo[j, :, lanes], preferred_element_type=jnp.float32).astype(jnp.bfloat16)
            for dest in range(n_tp):
                part[j, dest % 2, dest // 2, :, lanes] = found[dest * share : (dest + 1) * share]
            remote(role, ("d",) + piece, lambda: (
                part.at[j, 1 - core, :, :, span(*piece[1:])], dbuf.at[j, :, :, span(*piece[1:])], {"tp": twin}
            ))

        def combine(*piece):
            j, lanes = piece[0], span(*piece[1:])
            landed(dbuf.at[j, :, :, lanes], ("d",) + piece, {"tp": twin})
            both = (
                part[j, core, 1 - chip, :, lanes].astype(jnp.float32) + dbuf[j, 1 - chip, :, lanes].astype(jnp.float32)
            )
            xsend[j, :, lanes] = both.astype(jnp.bfloat16)
            remote(role, ("r",) + piece, lambda: (
                xsend.at[j, :, span(*piece[1:])], xrecv.at[j, :, span(*piece[1:])], {"tp": across}
            ))

        def emit_mate(*piece):
            j, lanes = piece[0], span(*piece[1:])
            found = jnp.dot(att[1], wo[j, :, lanes], preferred_element_type=jnp.float32).astype(jnp.bfloat16)
            for dest in range(n_tp):
                mpart[dest % 2, dest // 2, :, lanes] = found[dest * share : (dest + 1) * share]
            remote(role, ("md",) + piece, lambda: (
                mpart.at[1 - core, :, :, span(*piece[1:])], mbuf.at[:, :, span(*piece[1:])], {"tp": twin}
            ))

        def combine_mate(*piece):
            lanes = span(*piece[1:])
            landed(mbuf.at[:, :, lanes], ("md",) + piece, {"tp": twin})
            both = mpart[core, :, :, lanes].astype(jnp.float32) + mbuf[:, :, lanes].astype(jnp.float32)
            msum[:, :, lanes] = both.astype(jnp.bfloat16)
            remote(role, ("r",) + piece, lambda: (
                msum.at[1 - chip, :, span(*piece[1:])], xrecv.at[piece[0], :, span(*piece[1:])],
                {"sp": outward, "tp": across},
            ), "m")
            remote(role, ("m",) + piece, lambda: (
                msum.at[chip, :, span(*piece[1:])], msum.at[chip, :, span(*piece[1:])], z_out
            ))

        def settle(*piece):
            j, lanes = piece[0], span(*piece[1:])
            landed(xrecv.at[j, :, lanes], ("r",) + piece, {"tp": across})
            if role == "outer" and j == 3:
                landed(msum.at[chip, :, lanes], ("m",) + piece, z_in)
                near = msum[chip, :, lanes].astype(jnp.float32)
            else:
                near = part[j, core, chip, :, lanes].astype(jnp.float32) + dbuf[j, chip, :, lanes].astype(jnp.float32)
            total = near + xrecv[j, :, lanes].astype(jnp.float32)
            rel, first, count = piece[1:] if len(piece) > 2 else (piece[1], 0, out_chunks)
            h = g if rel == 0 else 1 - g
            base = place_of(j) * out_cols + h * out_half + first * out_size
            out_ref[:, pl.ds(pl.multiple_of(base, out_size), count * out_size)] = total.astype(jnp.bfloat16)

        def ready(j, first=0, count=out_chunks):
            for c in range(first, first + count):
                if role == "inner" and j == 1:
                    o_landed(1, 1, c, z_out)
                else:
                    o_twin_landed(j, c)

        def pump(j, c):
            if role == "inner":
                o_crossing(j, c)
            else:
                o_outer(j, c)

        words = {
            "emit": emit, "combine": combine, "settle": settle, "ready": ready, "pump": pump,
            "emit_mate": emit_mate, "combine_mate": combine_mate,
        }
        for word, *piece in script:
            words[word](*piece)

    opening = [("emit", 0, 0), ("emit", 0, 1), ("emit", 1, 0)]
    last = [(3, 1, 0, 2), (3, 1, 2, 1), (3, 1, 3, 1)]
    far = [(3, 0, 0, 2), (3, 0, 2, 2)] + last
    inner_script = (
        opening
        + [("pump", 3, 0), ("combine", 0, 0), ("emit", 2, 0), ("combine", 0, 1), ("ready", 2), ("emit", 2, 1)]
        + [("combine", 1, 0), ("pump", 3, 1), ("combine", 2, 0), ("combine", 2, 1), ("pump", 3, 2)]
        + [("emit_mate",) + far[0], ("emit",) + far[0]]
        + [("pump", 3, 3), ("combine_mate",) + far[0], ("emit_mate",) + far[1], ("emit",) + far[1]]
        + [("combine",) + far[0], ("ready", 3, 0, 2), ("combine_mate",) + far[1], ("emit_mate",) + last[0]]
        + [("emit",) + last[0], ("combine",) + far[1], ("ready", 1), ("emit", 1, 1)]
        + [("combine_mate",) + last[0], ("combine",) + last[0], ("combine", 1, 1)]
        + [("ready", 3, 2, 1), ("emit_mate",) + last[1], ("emit",) + last[1]]
        + [("settle", 0, 0), ("settle", 0, 1), ("combine_mate",) + last[1]]
        + [("ready", 3, 3, 1), ("emit_mate",) + last[2], ("emit",) + last[2]]
        + [("combine",) + last[1], ("settle", 1, 0), ("combine_mate",) + last[2], ("combine",) + last[2]]
        + [("settle", 2, 0), ("settle", 2, 1), ("settle",) + far[0], ("settle",) + far[1]]
        + [("settle",) + last[0], ("settle", 1, 1)] + [("settle",) + piece for piece in last[1:]]
    )
    outer_script = (
        [("emit", 0, 0), ("emit", 0, 1), ("combine", 0, 0), ("emit", 1, 0), ("combine", 0, 1), ("ready", 1)]
        + [("emit", 1, 1), ("combine", 1, 0), ("pump", 2, 1), ("combine", 1, 1), ("pump", 2, 2), ("pump", 2, 3)]
        + [("emit", 2, 0), ("ready", 2, 0, 2), ("combine", 2, 0)]
        + [("ready", 2, 2, 2), ("emit", 2, 1), ("settle", 0, 0), ("settle", 0, 1), ("combine", 2, 1)]
        + [("settle", 1, 0), ("settle", 1, 1), ("settle", 2, 0), ("settle",) + far[0], ("settle", 2, 1)]
        + [("settle",) + piece for piece in far[1:]]
    )

    @pl.when(inner)
    def _():
        tail("inner", inner_script)

    @pl.when(outer)
    def _():
        tail("outer", outer_script)

    for role, test in (("inner", inner), ("outer", outer)):

        @pl.when(test)
        def _():
            for group, at in sent[role].items():
                ref = whole(role, group)
                pltpu.make_async_remote_copy(
                    src_ref=ref, dst_ref=ref, send_sem=send_sem.at[at], recv_sem=recv_sem.at[0],
                    device_id=y_peer, device_id_type=MESH,
                ).wait_send()


def local(*args):
    tokens_in, norm_gain, wq, wk, wv, wq_gain, wk_gain, sink, dq, dk, dv, dq_gain, dk_gain, w_out, d_out = args
    length, width = tokens_in.shape
    n, n_tp = lax.axis_size("sp"), lax.axis_size("tp")
    depth, cols = wq.shape
    paired = (
        n == 4 and n_tp == 4 and wk.shape[1] == LANES and cols == 2 * LANES and depth * n == width
        and length % (n_tp * 32) == 0 and length % WINDOW == 0
    )
    if not paired:
        return local_ring(*args)
    q_heads, kv_heads = cols // HD, wk.shape[1] // HD
    out_rows, out_cols = w_out.shape[0] + d_out.shape[0], w_out.shape[1]
    share = length // n_tp
    lane = np.arange(LANES)
    fixed = np.stack(
        [THETA ** (-2.0 * (lane % (wide // 2)) / wide) for wide in (HD, HD // 2)]
        + [np.where(lane % wide < wide // 2, -1.0, 1.0) for wide in (HD, HD // 2)]
    ).astype(np.float32)
    gains = [gain[None, :] for gain in (wq_gain, wk_gain, dq_gain, dk_gain)]
    chunks, out_chunks = 2, 4
    vmem = pl.BlockSpec(memory_space=pltpu.VMEM)
    bf16 = jnp.bfloat16

    def sem(*shape):
        return pltpu.SemaphoreType.DMA(shape)

    return pl.pallas_call(
        functools.partial(pair_kernel, (q_heads, kv_heads, chunks, out_chunks)),
        out_shape=pltpu.VMEM((share, width), bf16),
        in_specs=[vmem] * 6
        + [pl.BlockSpec(memory_space=pltpu.SMEM)]
        + [pl.BlockSpec(memory_space=pl.ANY)] * 9,
        out_specs=vmem,
        scratch_shapes=[
            pltpu.VMEM((8, LANES), jnp.float32),
            pltpu.VMEM((4, 2 * length, LANES), jnp.float32),
            pltpu.VMEM((length, width), bf16),
            pltpu.VMEM((2 * length, width), bf16),
            pltpu.VMEM((KINDS, n, depth, cols), bf16),
            pltpu.VMEM((n, out_rows, out_cols), bf16),
            pltpu.VMEM((2, 2 * length, cols), jnp.float32),
            pltpu.VMEM((n, length, cols), bf16),
            pltpu.VMEM((2, length + 2 * WINDOW, cols), bf16),
            pltpu.VMEM((2, 2, q_heads, length, LANES), bf16),
            pltpu.VMEM((2, length, out_rows), bf16),
            pltpu.VMEM((n, 2, n_tp // 2, share, out_cols), bf16),
            pltpu.VMEM((n, 2, share, out_cols), bf16),
            pltpu.VMEM((n, share, out_cols), bf16),
            pltpu.VMEM((n, share, out_cols), bf16),
            pltpu.VMEM((2, n_tp // 2, share, out_cols), bf16),
            pltpu.VMEM((n_tp // 2, share, out_cols), bf16),
            pltpu.VMEM((n_tp // 2, share, out_cols), bf16),
            sem(RECEIVES),
            sem(SENDS),
            sem(LOCALS),
        ],
        compiler_params=pltpu.CompilerParams(
            collective_id=0, has_side_effects=True, vmem_limit_bytes=62 * 1024 * 1024
        ),
    )(norm_gain[None, :], fixed, *gains, sink[None, :], tokens_in, wq, dq, dk, dv, wk, wv, w_out, d_out)


def solution(mesh):
    return jax.shard_map(
        local,
        mesh=mesh,
        in_specs=(
            P(("grp", "sp"), None),
            P(),
            P("sp", "tp"),
            P("sp", "tp"),
            P("sp", "tp"),
            P(),
            P(),
            P("tp"),
            P("sp", "tp"),
            P("sp", "tp"),
            P("sp", "tp"),
            P(),
            P(),
            P("tp", "sp"),
            P("tp", "sp"),
        ),
        out_specs=P(("grp", "sp", "tp"), None),
        check_vma=False,
    )
```

```python
import functools

import jax
import jax.numpy as jnp
import numpy as np
from jax import lax
from jax.experimental import pallas as pl
from jax.experimental.pallas import tpu as pltpu
from jax.sharding import PartitionSpec as P

HD = 64
WINDOW = 128
GRID_W = 64


EPS = 1e-06
THETA = 10000.0


MESH = pl.DeviceIdType.MESH
HALVES = 2


class LineGather:
    def __init__(self, own, buf, z_recv, r_send, l_send, y_recv=None, y_send=None, axis=0):
        self.own, self.buf = own, buf
        self.z_recv, self.y_recv = z_recv, y_recv
        self.r_send, self.l_send, self.y_send = r_send, l_send, y_send
        self.n = lax.axis_size("sp")
        self.s = lax.axis_index("sp")
        self.shared = y_recv is not None
        self.g = lax.axis_index("grp") if self.shared else 0
        self.chunks = z_recv.shape[1]
        self.axis = axis
        extent = buf.shape[1 + axis]
        self.half = extent // HALVES if self.shared else extent
        self.size = self.half // self.chunks

    def rows(self, half, c):
        piece = pl.ds(pl.multiple_of(half * self.half + c * self.size, self.size), self.size)
        return (piece,) if self.axis == 0 else (slice(None), piece)

    def block(self, o, half, c):
        return self.buf.at[(o,) + self.rows(half, c)]

    def copy(self, src, o, c, sem, recv, target, half):
        return pltpu.make_async_remote_copy(
            src_ref=src,
            dst_ref=self.block(o, half, c),
            send_sem=sem.at[o, c],
            recv_sem=recv.at[o, c],
            device_id=target,
            device_id_type=MESH,
        )

    def right(self, src, o, c):
        return self.copy(src, o, c, self.r_send, self.z_recv, {"sp": lax.rem(self.s + 1, self.n)}, self.g)

    def left(self, src, o, c):
        return self.copy(
            src, o, c, self.l_send, self.z_recv, {"sp": lax.rem(self.s + self.n - 1, self.n)}, self.g
        )

    def twin(self, o, c, half):
        return self.copy(
            self.block(o, half, c), o, c, self.y_send, self.y_recv, {"grp": 1 - self.g}, half
        )

    def mine(self, c):
        if self.own is None:
            return self.block(self.s, self.g, c)
        return self.own.at[self.rows(self.g, c)]

    def start(self, first=0, last=None):
        for c in range(first, self.chunks if last is None else last):
            mine = self.mine(c)

            @pl.when(self.s + 1 < self.n)
            def _():
                self.right(mine, self.s, c).start()

            @pl.when(self.s > 0)
            def _():
                self.left(mine, self.s, c).start()

    def forward(self, d):
        for c in range(self.chunks):

            @pl.when(self.s - d >= 0)
            def _():
                o = self.s - d
                there = self.block(o, self.g, c)
                self.right(there, o, c).wait_recv()

                @pl.when(self.s + 1 < self.n)
                def _():
                    self.right(there, o, c).start()

                if self.shared:
                    self.twin(o, c, self.g).start()

            @pl.when(self.s + d < self.n)
            def _():
                o = self.s + d
                there = self.block(o, self.g, c)
                self.left(there, o, c).wait_recv()

                @pl.when(self.s > 0)
                def _():
                    self.left(there, o, c).start()

                if self.shared:
                    self.twin(o, c, self.g).start()

    def use(self, d, fn, near=None):
        for there, o in ((self.s - d >= 0, self.s - d), (self.s + d < self.n, self.s + d)):
            if near is not None:

                @pl.when(there)
                def _():
                    near(o)

        for there, o in ((self.s - d >= 0, self.s - d), (self.s + d < self.n, self.s + d)):

            @pl.when(there)
            def _():
                for c in range(self.chunks):
                    self.twin(o, c, 1 - self.g).wait_recv()
                fn(o)

    def run(self, fn, near=None, last=None):
        self.forward(1)
        self.rest(fn, near, last)

    def rest(self, fn, near=None, last=None):
        @pl.loop(2, self.n)
        def _(d):
            self.forward(d)
            self.use(d - 1, fn, near)

        if last is not None:
            last()
        self.use(self.n - 1, fn, near)

    def finish(self):
        @pl.loop(0, self.n)
        def _(o):
            for c in range(self.chunks):
                there = self.block(o, self.g, c)

                @pl.when((o <= self.s) & (self.s + 1 < self.n))
                def _():
                    self.right(there, o, c).wait_send()

                @pl.when((o >= self.s) & (self.s > 0))
                def _():
                    self.left(there, o, c).wait_send()

                if self.shared:

                    @pl.when(o != self.s)
                    def _():
                        self.twin(o, c, self.g).wait_send()


def greet():
    n, s, g = lax.axis_size("sp"), lax.axis_index("sp"), lax.axis_index("grp")
    n_tp, t = lax.axis_size("tp"), lax.axis_index("tp")
    barrier = pltpu.get_barrier_semaphore()
    pl.semaphore_signal(barrier, inc=1, device_id={"grp": 1 - g}, device_id_type=MESH)
    for j in range(1, n_tp):
        pl.semaphore_signal(barrier, inc=1, device_id={"tp": lax.rem(t + j, n_tp)}, device_id_type=MESH)

    @pl.when(s + 1 < n)
    def _():
        pl.semaphore_signal(barrier, inc=1, device_id={"sp": lax.rem(s + 1, n)}, device_id_type=MESH)

    @pl.when(s > 0)
    def _():
        pl.semaphore_signal(barrier, inc=1, device_id={"sp": lax.rem(s + n - 1, n)}, device_id_type=MESH)

    pl.semaphore_wait(barrier, n_tp + (s + 1 < n).astype(jnp.int32) + (s > 0).astype(jnp.int32))


LANES = 128


def by_half(low, high):
    lane = lax.broadcasted_iota(jnp.int32, low.shape, 1)
    return jnp.where(lane < HD, low, high)


def swap_pairs(values, reach):
    lane = lax.broadcasted_iota(jnp.int32, values.shape, 1)
    ahead = pltpu.roll(values, LANES - reach, 1)
    behind = pltpu.roll(values, reach, 1)
    return jnp.where(lax.rem(lane, 2 * reach) < reach, ahead, behind)


def head_tile(tile, kinds, gains_ref, tables_ref):
    square = tile * tile
    zero = jnp.zeros_like(square)
    low = jnp.sum(by_half(square, zero), axis=-1, keepdims=True)
    high = jnp.sum(by_half(zero, square), axis=-1, keepdims=True)
    mean = by_half(jnp.broadcast_to(low, tile.shape), jnp.broadcast_to(high, tile.shape)) * (1.0 / HD)
    scaled = tile * lax.rsqrt(mean + EPS)

    def one(kind):
        if kind is None:
            return tile
        gain, table, reach = kind
        normed = scaled * gains_ref[gain : gain + 1, :]
        return normed * tables_ref[2 * table] + swap_pairs(normed, reach) * tables_ref[2 * table + 1]

    if kinds[0] == kinds[1]:
        return one(kinds[0])
    return by_half(one(kinds[0]), one(kinds[1]))


def layer_kernel(
    sizes, x_ref, gain_ref, fixed_ref, g0, g1, g2, g3, sink_ref, *refs
):
    n_in = sizes[2]
    in_refs, out_refs = refs[:n_in], refs[n_in : n_in + 2]
    run_layer(sizes[:2], x_ref, gain_ref, fixed_ref, (g0, g1, g2, g3), sink_ref, in_refs, out_refs, *refs[n_in + 2 :])


def run_layer(
    sizes, x_ref, gain_ref, fixed_ref, head_gains, sink_ref, in_refs, out_refs, out_ref,
    small_ref, w_ref, wo_ref, tables_ref, load_sem, xn, proj, wbuf, wo_all, kvd, ext, qs, att, part, rs, halo_recv, halo_send, rs_recv, rs_send, *sems
):
    q_heads, kv_heads = sizes
    n, s = lax.axis_size("sp"), lax.axis_index("sp")
    n_tp, t = lax.axis_size("tp"), lax.axis_index("tp")
    depth = w_ref.shape[0]
    length = x_ref.shape[0]
    into = LineGather(w_ref, wbuf, *sems[:5])
    out = LineGather(wo_ref, wo_all, *sems[5:10], axis=1)
    keys = LineGather(None, kvd, *sems[10:])
    loads, at = [], 0
    for ref in in_refs:
        wide = ref.shape[1]
        loads.append(
            pltpu.make_async_copy(ref, w_ref.at[:, at : at + wide], load_sem.at[len(loads)])
        )
        at += wide
    at = 0
    for ref in out_refs:
        tall = ref.shape[0]
        loads.append(pltpu.make_async_copy(ref, wo_ref.at[at : at + tall], load_sem.at[len(loads)]))
        at += tall
    for load in loads:
        load.start()
    greet()
    for load in loads:
        load.wait()
    into.start()

    for k, ref in enumerate(head_gains):
        small_ref[k : k + 1, :] = jnp.concatenate([ref[...], ref[...]], axis=1)
    small_ref[4:8, :] = fixed_ref[...]
    step = 16

    @pl.loop(0, length // step)
    def _(i):
        rows = pl.ds(pl.multiple_of(i * step, step), step)
        values = x_ref[rows, :].astype(jnp.float32)
        mean = jnp.mean(values * values, axis=-1, keepdims=True)
        xn[rows, :] = (values * lax.rsqrt(mean + EPS) * gain_ref[...]).astype(jnp.bfloat16)

    def columns(o):
        return pl.ds(pl.multiple_of(o * depth, depth), depth)

    proj[...] = jnp.dot(xn[:, columns(s)], w_ref[...], preferred_element_type=jnp.float32)

    band = 64 if length % 64 == 0 else length

    @pl.loop(0, length // band)
    def _(i):
        rows = pl.ds(pl.multiple_of(i * band, band), band)
        shape = (band, LANES)
        place = lax.broadcasted_iota(jnp.int32, shape, 0) + (s * length + i * band)
        lane = lax.broadcasted_iota(jnp.int32, shape, 1)
        spot = jnp.where(lax.rem(lane, HD) < HD // 2, place // GRID_W, lax.rem(place, GRID_W))
        for k, where in enumerate((place, spot)):
            angles = where.astype(jnp.float32) * small_ref[4 + k : 5 + k, :]
            tables_ref[2 * k, rows, :] = jnp.cos(angles)
            tables_ref[2 * k + 1, rows, :] = jnp.sin(angles) * small_ref[6 + k : 7 + k, :]

    def add(o):
        proj[...] += jnp.dot(xn[:, columns(o)], wbuf[o], preferred_element_type=jnp.float32)

    into.run(add, last=lambda: out.start(0, 1))

    win_q, win_k, den_q, den_k = (0, 0, 32), (1, 0, 32), (2, 1, 16), (3, 1, 16)
    kinds = (
        [win_q] * q_heads + [den_q] * q_heads + [den_k] * kv_heads + [None] * kv_heads
        + [win_k] * kv_heads + [None] * kv_heads
    )
    q_tiles = 2 * q_heads * HD // LANES
    kv_tiles = 2 * kv_heads * HD // LANES

    def finished(i):
        return head_tile(
            proj[:, i * LANES : (i + 1) * LANES], kinds[2 * i : 2 * i + 2], small_ref, tables_ref
        )

    for i in range(kv_tiles):
        ext[WINDOW : WINDOW + length, i * LANES : (i + 1) * LANES] = finished(
            q_tiles + kv_tiles + i
        ).astype(jnp.bfloat16)
    for i in range(kv_tiles):
        kvd[s, :, i * LANES : (i + 1) * LANES] = finished(q_tiles + i).astype(jnp.bfloat16)

    def halo(side):
        source = pl.ds(length, WINDOW) if side == 0 else pl.ds(WINDOW, WINDOW)
        target = pl.ds(0, WINDOW) if side == 0 else pl.ds(WINDOW + length, WINDOW)
        peer = lax.rem(s + 1, n) if side == 0 else lax.rem(s + n - 1, n)
        return pltpu.make_async_remote_copy(
            src_ref=ext.at[source], dst_ref=ext.at[target], send_sem=halo_send.at[side],
            recv_sem=halo_recv.at[side], device_id={"sp": peer}, device_id_type=MESH,
        )

    has_right, has_left = s + 1 < n, s > 0

    @pl.when(has_right)
    def _():
        halo(0).start()

    @pl.when(has_left)
    def _():
        halo(1).start()

    keys.start()
    none = jnp.zeros((WINDOW, ext.shape[1]), jnp.bfloat16)

    @pl.when(jnp.logical_not(has_left))
    def _():
        ext[0:WINDOW, :] = none

    @pl.when(jnp.logical_not(has_right))
    def _():
        ext[WINDOW + length : WINDOW + length + WINDOW, :] = none

    group = q_heads // kv_heads

    def place(head):
        return head // 2, head % 2

    for i in range(q_tiles):
        tile = finished(i) * HD ** (-0.5)
        for b in range(2):
            head = 2 * i + b
            half = place((head % q_heads) // group)[1]
            moved = tile if half == b else pltpu.roll(tile, HD, 1)
            zero = jnp.zeros_like(moved)
            kept = by_half(moved, zero) if half == 0 else by_half(zero, moved)
            qs[head] = kept.astype(jnp.bfloat16)

    @pl.when(has_left)
    def _():
        halo(0).wait_recv()

    @pl.when(has_right)
    def _():
        halo(1).wait_recv()

    total_len = length * n

    def joined(results, heads):
        placed = []
        for b in range(2):
            half = place(kv_heads + heads[b] // group)[1]
            placed.append(results[b] if half == b else pltpu.roll(results[b], HD, 1))
        return by_half(placed[0], placed[1]).astype(jnp.bfloat16)

    def tile_of(head):
        return pl.ds(place(head)[0] * LANES, LANES)

    nt = (((1,), (1,)), ((), ()))

    def windowed(pair):
        @pl.loop(0, length // WINDOW)
        def _(b):
            base = pl.multiple_of(b * WINDOW, WINDOW)
            rows = pl.ds(base, WINDOW)
            near = pl.ds(base, 3 * WINDOW)
            shape = (WINDOW, 3 * WINDOW)
            at = lax.broadcasted_iota(jnp.int32, shape, 1) - WINDOW
            away = at - lax.broadcasted_iota(jnp.int32, shape, 0)
            pos = at + (s * length + base)
            valid = (away <= WINDOW) & (away >= -WINDOW) & (pos >= 0) & (pos < total_len)
            results = []
            for head in (2 * pair, 2 * pair + 1):
                key = ext[near, tile_of(head // group)]
                value = ext[near, tile_of(kv_heads + head // group)]
                scores = lax.dot_general(qs[head, rows, :], key, nt, preferred_element_type=jnp.float32)
                scores = jnp.where(valid, scores, -jnp.inf)
                floor = sink_ref[0, head]
                top = jnp.maximum(jnp.max(scores, axis=-1, keepdims=True), floor)
                expon = jnp.exp(scores - top)
                total = jnp.sum(expon, axis=-1, keepdims=True) + jnp.exp(floor - top)
                weights = (expon / total).astype(jnp.bfloat16)
                results.append(jnp.dot(weights, value, preferred_element_type=jnp.float32))
            att[rows, pair * LANES : (pair + 1) * LANES] = joined(results, (2 * pair, 2 * pair + 1))

    pairs = q_heads // 2
    keys.forward(1)
    windowed(0)

    @pl.loop(2, n)
    def _(d):
        keys.forward(d)

    out.start(1)
    for pair in range(1, pairs):
        windowed(pair)

    def dense(pair):
        @pl.loop(0, length // LANES)
        def _(b):
            rows = pl.ds(pl.multiple_of(b * LANES, LANES), LANES)
            results = []
            for head in (2 * pair, 2 * pair + 1):
                key = kvd[:, :, tile_of(head // group)].reshape(total_len, LANES)
                value = kvd[:, :, tile_of(kv_heads + head // group)].reshape(total_len, LANES)
                scores = lax.dot_general(
                    qs[q_heads + head, rows, :], key, nt, preferred_element_type=jnp.float32
                )
                top = jnp.max(scores, axis=-1, keepdims=True)
                expon = jnp.exp(scores - top)
                total = jnp.sum(expon, axis=-1, keepdims=True)
                summed = jnp.dot(
                    expon.astype(jnp.bfloat16), value, preferred_element_type=jnp.float32
                )
                results.append(summed / total)
            at = (pairs + pair) * LANES
            att[rows, at : at + LANES] = joined(results, (2 * pair, 2 * pair + 1))

    dense(0)
    out.forward(1)
    for pair in range(1, pairs):
        dense(pair)

    share = length // n_tp

    wide = wo_ref.shape[1]
    part_cols = wide // HALVES
    mine = lax.axis_index("grp")

    def span(h):
        return pl.ds(pl.multiple_of(h * part_cols, part_cols), part_cols)

    def exchange(o, h, j):
        peer = lax.rem(t + j, n_tp)
        return pltpu.make_async_remote_copy(
            src_ref=part.at[o, pl.ds(pl.multiple_of(peer * share, share), share), span(h)],
            dst_ref=rs.at[t, o, :, span(h)], send_sem=rs_send.at[j - 1, o, h],
            recv_sem=rs_recv.at[t, o, h], device_id={"tp": peer}, device_id_type=MESH,
        )

    def arrived(o, h, j):
        source = lax.rem(t + n_tp - j, n_tp)
        there = rs.at[source, o, :, span(h)]
        return pltpu.make_async_remote_copy(
            src_ref=there, dst_ref=there, send_sem=rs_send.at[j - 1, o, h],
            recv_sem=rs_recv.at[source, o, h], device_id={"tp": source}, device_id_type=MESH,
        )

    def emit(o, h, weight):
        part[o, :, span(h)] = jnp.dot(
            att[...], weight, preferred_element_type=jnp.float32
        ).astype(jnp.bfloat16)
        for j in range(1, n_tp):
            exchange(o, h, j).start()
        rs[t, o, :, span(h)] = part[o, pl.ds(pl.multiple_of(t * share, share), share), span(h)]

    def collect(o, h):
        for j in range(1, n_tp):
            arrived(o, h, j).wait_recv()
        total = rs[0, o, :, span(h)].astype(jnp.float32)
        for g in range(1, n_tp):
            total += rs[g, o, :, span(h)].astype(jnp.float32)
        columns_out = pl.ds(pl.multiple_of(o * wide + h * part_cols, part_cols), part_cols)
        out_ref[:, columns_out] = total.astype(jnp.bfloat16)

    for h in range(HALVES):
        emit(s, h, wo_ref[:, span(h)])
    out.rest(
        lambda o: emit(o, 1 - mine, wo_all[o, :, span(1 - mine)]),
        near=lambda o: emit(o, mine, wo_all[o, :, span(mine)]),
    )

    @pl.loop(0, n)
    def _(d):
        o = lax.rem(s + d, n)
        for h in range(HALVES):
            collect(o, h)

    @pl.loop(0, n)
    def _(o):
        for h in range(HALVES):
            for j in range(1, n_tp):
                exchange(o, h, j).wait_send()

    @pl.when(has_right)
    def _():
        halo(0).wait_send()

    @pl.when(has_left)
    def _():
        halo(1).wait_send()

    into.finish()
    out.finish()
    keys.finish()


def local_ring(
    tokens_in,
    norm_gain,
    window_query,
    window_key,
    window_value,
    window_query_gain,
    window_key_gain,
    sink_logit,
    dense_query,
    dense_key,
    dense_value,
    dense_query_gain,
    dense_key_gain,
    window_out,
    dense_out,
):
    length, width = tokens_in.shape
    n, n_tp = lax.axis_size("sp"), lax.axis_size("tp")
    q_heads, kv_heads = window_query.shape[1] // HD, window_key.shape[1] // HD
    weights, held = [], []
    for weight in (window_query, dense_query, dense_key, dense_value, window_key, window_value):
        held.append(weight)
        if sum(w.shape[1] for w in held) % LANES == 0:
            weights.append(held[0] if len(held) == 1 else jnp.concatenate(held, axis=1))
            held = []
    depth, in_cols = window_query.shape[0], sum(w.shape[1] for w in weights)
    out_rows, out_cols = window_out.shape[0] + dense_out.shape[0], window_out.shape[1]

    lane = np.arange(LANES)
    fixed = np.stack(
        [THETA ** (-2.0 * (lane % (wide // 2)) / wide) for wide in (HD, HD // 2)]
        + [np.where(lane % wide < wide // 2, -1.0, 1.0) for wide in (HD, HD // 2)]
    ).astype(np.float32)
    gains = [g[None, :] for g in (window_query_gain, window_key_gain, dense_query_gain, dense_key_gain)]

    def gather(chunks):
        return [pltpu.SemaphoreType.DMA((n, chunks)) for _ in range(5)]

    in_chunks = 8 if n <= 4 else 1
    out_chunks = out_cols // HALVES // LANES if n <= 4 else 1
    kv_cols = 2 * kv_heads * HD
    vmem = pl.BlockSpec(memory_space=pltpu.VMEM)
    share = length // n_tp
    return pl.pallas_call(
        functools.partial(layer_kernel, (q_heads, kv_heads, len(weights))),
        out_shape=jax.ShapeDtypeStruct((share, width), jnp.bfloat16),
        in_specs=[vmem] * 7
        + [pl.BlockSpec(memory_space=pltpu.SMEM)]
        + [pl.BlockSpec(memory_space=pl.ANY)] * (len(weights) + 2),
        out_specs=vmem,
        scratch_shapes=[
            pltpu.VMEM((8, LANES), jnp.float32),
            pltpu.VMEM((depth, in_cols), jnp.bfloat16),
            pltpu.VMEM((out_rows, out_cols), jnp.bfloat16),
            pltpu.VMEM((4, length, LANES), jnp.float32),
            pltpu.SemaphoreType.DMA((len(weights) + 2,)),
            pltpu.VMEM((length, width), jnp.bfloat16),
            pltpu.VMEM((length, in_cols), jnp.float32),
            pltpu.VMEM((n, depth, in_cols), jnp.bfloat16),
            pltpu.VMEM((n, out_rows, out_cols), jnp.bfloat16),
            pltpu.VMEM((n, length, kv_cols), jnp.bfloat16),
            pltpu.VMEM((length + 2 * WINDOW, kv_cols), jnp.bfloat16),
            pltpu.VMEM((2 * q_heads, length, LANES), jnp.bfloat16),
            pltpu.VMEM((length, out_rows), jnp.bfloat16),
            pltpu.VMEM((n, length, out_cols), jnp.bfloat16),
            pltpu.VMEM((n_tp, n, share, out_cols), jnp.bfloat16),
            pltpu.SemaphoreType.DMA((2,)),
            pltpu.SemaphoreType.DMA((2,)),
            pltpu.SemaphoreType.DMA((n_tp, n, HALVES)),
            pltpu.SemaphoreType.DMA((n_tp - 1, n, HALVES)),
        ]
        + gather(in_chunks)
        + gather(out_chunks)
        + [pltpu.SemaphoreType.DMA((n, 2 if n <= 4 else 1)) for _ in range(3)],
        compiler_params=pltpu.CompilerParams(
            collective_id=0, has_side_effects=True, vmem_limit_bytes=62 * 1024 * 1024
        ),
    )(tokens_in, norm_gain[None, :], fixed, *gains, sink_logit[None, :], *weights, window_out, dense_out)


KINDS = 4
SHARED = (True, False, False, False)
RECEIVES, SENDS, LOCALS = 131, 16, 9

def pair_kernel(sizes, *refs):
    gain_ref, fixed_ref, g0, g1, g2, g3, sink_ref, x_hbm = refs[:8]
    weights, outs, out_ref = refs[8:14], refs[14:16], refs[16]
    run_pairs(sizes, gain_ref, fixed_ref, (g0, g1, g2, g3), sink_ref, x_hbm, weights, outs, out_ref, *refs[17:])


def run_pairs(
    sizes, gain_ref, fixed_ref, head_gains, sink_ref, x_hbm, weights, outs, out_ref,
    small_ref, tables_ref, xv, xn, wbuf, wo, proj, kvd, ext, qs, att, part, dbuf, xsend, xrecv, mpart, mbuf, msum,
    recv_sem, send_sem, load_sem,
):
    q_heads, kv_heads, chunks, out_chunks = sizes
    n, s = lax.axis_size("sp"), lax.axis_index("sp")
    n_tp, t = lax.axis_size("tp"), lax.axis_index("tp")
    g = lax.axis_index("grp")
    length, width = xv.shape
    depth, cols = wbuf.shape[2], wbuf.shape[3]
    out_rows, out_cols = wo.shape[1], wo.shape[2]
    share = length // n_tp
    low = 2 * s < n
    high = jnp.logical_not(low)
    inner = (s > 0) & (s < n - 1)
    outer = jnp.logical_not(inner)
    step = jnp.where(low, 1, -1)
    inward = s + step
    outward = lax.rem(s - step + n, n)
    core, chip = lax.rem(t, 2), t // 2
    twin = t + 1 - 2 * core
    across = lax.rem(t + 2, n_tp)
    diagonal = lax.rem(twin + 2, n_tp)

    def place_of(j):
        if j == 0:
            return s
        return jnp.where(inner, (s - step, s - step, s + step, s + 2 * step)[j], s + j * step)

    sent = {"inner": {}, "outer": {}}
    names = {}

    def recv_at(*name):
        at = names.setdefault(name, len(names))
        assert at < recv_sem.shape[0]
        return recv_sem.at[at]

    def whole(when, group):
        many = when == "inner"
        return {
            "w": lambda: wbuf.at[0] if many else wbuf.at[1:KINDS, 0],
            "w0": lambda: wbuf.at[0, 0, 0:half],
            "wy": lambda: wbuf.at[0],
            "o": lambda: wo.at[0],
            "oo": lambda: wo.at[0],
            "oy": lambda: wo.at[0],
            "x": lambda: xn.at[0:share],
            "xx": lambda: xn.at[0:share],
            "xd": lambda: xn.at[0:share],
            "xe": lambda: xn.at[0:share],
            "kv": lambda: kvd.at[0:2],
            "halo": lambda: ext.at[0, 0:WINDOW],
            "att": lambda: att.at[0],
            "d": lambda: dbuf if many else dbuf.at[0:3],
            "r": lambda: xrecv if many else xrecv.at[0:3],
            "md": lambda: mbuf,
            "m": lambda: msum,
        }[group]()

    def remote(when, name, ends, group=None):
        at = sent[when].setdefault(group or name[0], len(sent[when]))
        assert at < send_sem.shape[0]
        src, dst, peer = ends()
        pltpu.make_async_remote_copy(
            src_ref=src, dst_ref=dst, send_sem=send_sem.at[at], recv_sem=recv_at(*name),
            device_id=peer, device_id_type=MESH,
        ).start()

    def landed(ref, name, peer):
        sem = recv_at(*name)
        pltpu.make_async_remote_copy(
            src_ref=ref, dst_ref=ref, send_sem=sem, recv_sem=sem, device_id=peer, device_id_type=MESH
        ).wait_recv()

    z_in, z_out, y_peer = {"sp": inward}, {"sp": outward}, {"grp": 1 - g}

    half = depth // HALVES
    size = half // chunks

    def w_at(k, slot, rel, c):
        h = g if rel == 0 else 1 - g
        return wbuf.at[k, slot, pl.ds(pl.multiple_of(h * half + c * size, size), size)]

    def w_inward(role, k, slot, rel, c):
        to = 1 if role == "outer" else slot + 2
        remote(
            role, ("w", k, to, rel, c), lambda: (w_at(k, slot, rel, c), w_at(k, to, rel, c), z_in),
            "w0" if role == "outer" and k == 0 else "w",
        )

    def w_landed(k, slot, rel, c):
        landed(w_at(k, slot, rel, c), ("w", k, slot, rel, c), z_out if slot == 1 else z_in)

    def w_twin(k, slot, c):
        remote(
            "inner", ("wy", k, slot, c), lambda: (w_at(k, slot, 0, c), w_at(k, slot, 0, c), y_peer),
            "w0" if slot == 1 else "wy",
        )

    def w_twin_landed(k, slot, c):
        landed(w_at(k, slot, 1, c), ("wy", k, slot, c), y_peer)

    out_half = out_cols // HALVES
    out_size = out_half // out_chunks

    def o_at(slot, rel, c):
        h = g if rel == 0 else 1 - g
        return wo.at[slot, :, pl.ds(pl.multiple_of(h * out_half + c * out_size, out_size), out_size)]

    def o_inward(role, slot, rel, c):
        to = 1 if role == "outer" else slot + 2
        remote(role, ("o", to, rel, c), lambda: (o_at(slot, rel, c), o_at(to, rel, c), z_in))

    def o_outward(slot, c):
        to = 1 if slot == 0 else slot
        remote("inner", ("o", to, 0, c), lambda: (o_at(slot, 0, c), o_at(to, 0, c), z_out), "oo")

    def o_landed(slot, rel, c, peer):
        landed(o_at(slot, rel, c), ("o", slot, rel, c), peer)

    def o_twin(role, slot, c):
        remote(role, ("oy", slot, c), lambda: (o_at(slot, 0, c), o_at(slot, 0, c), y_peer))

    def o_twin_landed(slot, c):
        landed(o_at(slot, 1, c), ("oy", slot, c), y_peer)

    def x_rows(quarter):
        return pl.ds(pl.multiple_of(length + quarter * share, share), share)

    def x_cols(p):
        return pl.ds(p * depth, depth)

    def x_relay(p):
        def piece():
            return xn.at[x_rows(t), x_cols(p)]

        landed(piece(), ("x", p), z_out)
        remote("inner", ("xx", p), lambda: (piece(), piece(), {"tp": across}))
        remote("inner", ("xd", p), lambda: (piece(), piece(), {"tp": twin}))

    def x_pass(p):
        def piece():
            return xn.at[x_rows(across), x_cols(p)]

        landed(piece(), ("xx", p), {"tp": across})
        remote("inner", ("xe", p), lambda: (piece(), piece(), {"tp": twin}))

    def x_all(p):
        landed(xn.at[x_rows(twin), x_cols(p)], ("xd", p), {"tp": twin})
        landed(xn.at[x_rows(diagonal), x_cols(p)], ("xe", p), {"tp": twin})

    kv_cols = cols // 2
    loads = []

    def load(src, dst):
        copy = pltpu.make_async_copy(src, dst, load_sem.at[len(loads)])
        loads.append(copy)
        copy.start()

    wq, dq, dk, dv, wk, wv = weights
    load(dk, wbuf.at[0, 0, :, 0:kv_cols])
    load(dv, wbuf.at[0, 0, :, kv_cols:cols])
    load(x_hbm, xv)
    load(dq, wbuf.at[1, 0])
    load(wk, wbuf.at[2, 0, :, 0:kv_cols])
    load(wv, wbuf.at[2, 0, :, kv_cols:cols])
    load(wq, wbuf.at[3, 0])
    rows_of = outs[0].shape[0]
    load(outs[0], wo.at[0, 0:rows_of])
    load(outs[1], wo.at[0, rows_of:out_rows])
    greet()

    all_chunks, all_out = range(chunks), range(out_chunks)
    loads[0].wait()
    loads[1].wait()

    for role, test in (("inner", inner), ("outer", outer)):

        @pl.when(test)
        def _():
            for c in all_chunks:
                w_inward(role, 0, 0, 0, c)

    for k, ref in enumerate(head_gains):
        small_ref[k : k + 1, :] = jnp.concatenate([ref[...], ref[...]], axis=1)
    small_ref[4:8, :] = fixed_ref[...]
    loads[2].wait()

    def normalize(first, count):
        stripe = 16

        @pl.loop(0, count // stripe)
        def _(i):
            at = pl.multiple_of(i * stripe, stripe)
            values = xv[pl.ds(first + at, stripe), :].astype(jnp.float32)
            mean = jnp.mean(values * values, axis=-1, keepdims=True)
            xn[pl.ds(at, stripe), :] = (values * lax.rsqrt(mean + EPS) * gain_ref[...]).astype(jnp.bfloat16)

    band = 64

    def tables(first, count):
        @pl.loop(0, count // band)
        def _(i):
            at = pl.multiple_of(i * band, band) + first
            rows = pl.ds(at, band)
            shape = (band, LANES)
            base = jnp.where(at < length, s * length + at, (s - step) * length + at - length)
            place = lax.broadcasted_iota(jnp.int32, shape, 0) + base
            lane = lax.broadcasted_iota(jnp.int32, shape, 1)
            spot = jnp.where(lax.rem(lane, HD) < HD // 2, place // GRID_W, lax.rem(place, GRID_W))
            for k, where in enumerate((place, spot)):
                angles = where.astype(jnp.float32) * small_ref[4 + k : 5 + k, :]
                tables_ref[2 * k, rows, :] = jnp.cos(angles)
                tables_ref[2 * k + 1, rows, :] = jnp.sin(angles) * small_ref[6 + k : 7 + k, :]

    def project(k, j, sides=(0, 1)):
        at = pl.multiple_of(place_of(j) * depth, depth)

        @pl.loop(sides[0], sides[-1] + 1)
        def _(i):
            rows = pl.ds(pl.multiple_of(i * length, length), length)
            found = jnp.dot(xn[rows, pl.ds(at, depth)], wbuf[k, j], preferred_element_type=jnp.float32)
            proj[k % 2, rows, :] = found if j == 0 else proj[k % 2, rows, :] + found

    den_q, den_k, win_q, win_k = (2, 1, 16), (3, 1, 16), (0, 0, 32), (1, 0, 32)
    plans = ((den_k, None), (den_q, den_q), (win_k, None), (win_q, win_q))
    group = q_heads // kv_heads
    pairs = q_heads // 2

    def finished(k, side, *tiles):
        rows = pl.ds(side * length, length)
        for tile in tiles or range(cols // LANES):
            lanes = pl.ds(tile * LANES, LANES)
            kind = plans[k][tile * 2 * LANES // cols]
            value = proj[k % 2, rows, lanes]
            if kind is not None:
                value = head_tile(
                    value, (kind, kind), small_ref, [tables_ref.at[m][rows, :] for m in range(4)]
                )
            if k % 2:
                value = value * HD ** (-0.5)
                zero = jnp.zeros_like(value)
                for b in range(2):
                    head = 2 * tile + b
                    half_of = head // group % 2
                    moved = value if half_of == b else pltpu.roll(value, HD, 1)
                    kept = by_half(moved, zero) if half_of == 0 else by_half(zero, moved)
                    qs[k // 2, side, head] = kept.astype(jnp.bfloat16)
            elif k == 0:
                kvd[side, :, lanes] = value.astype(jnp.bfloat16)
            else:
                ext[side, pl.ds(WINDOW, length), lanes] = value.astype(jnp.bfloat16)

    def mates(k, c):
        w_landed(k, 1, 0, c)
        w_inward("inner", k, 1, 0, c)
        if SHARED[k]:
            w_twin(k, 1, c)

    def crossing(k, slot, c):
        w_landed(k, slot, 0, c)
        w_twin(k, slot, c)

    def mate_ready(k):
        for c in all_chunks:
            if SHARED[k]:
                w_twin_landed(k, 1, c)
            else:
                w_landed(k, 1, 1, c)

    def twin_ready(k, slot):
        for c in all_chunks:
            w_twin_landed(k, slot, c)

    def o_mates(c):
        o_landed(1, 0, c, z_out)
        o_inward("inner", 1, 0, c)

    def o_crossing(slot, c):
        o_landed(slot, 0, c, z_in)
        if slot < 3:
            o_outward(slot, c)
        o_twin("inner", slot, c)

    def o_outer(slot, c):
        o_landed(slot, 0, c, z_in)
        o_twin("outer", slot, c)

    def edge(first):
        return pl.ds(jnp.where(first, WINDOW, length), WINDOW)

    def halo_at(leading):
        return pl.ds(jnp.where(leading, 0, WINDOW + length), WINDOW)

    def halo_inward():
        remote("inner", ("halo",), lambda: (ext.at[0, edge(high)], ext.at[0, halo_at(low)], z_in))

    def halo_landed():
        landed(ext.at[0, halo_at(high)], ("halo",), z_in)

    def halo_local():
        ext[0, halo_at(low), :] = ext[1, edge(high), :]
        ext[1, halo_at(high), :] = ext[0, edge(low), :]
        ext[1, halo_at(low), :] = jnp.zeros((WINDOW, cols), jnp.bfloat16)

    def kv_landed(j):
        landed(kvd.at[j], ("kv", j), z_in)

    def kv_inward(j):
        remote("inner", ("kv", j + 2), lambda: (kvd.at[j], kvd.at[j + 2], z_in))

    def x_inward(p):
        remote("outer", ("x", p), lambda: (xn.at[0:share, x_cols(p)], xn.at[x_rows(t), x_cols(p)], z_in))

    def att_at(side, i):
        return att.at[side, :, i * LANES : (i + 1) * LANES]

    def att_outward(i):
        remote("inner", ("att", i), lambda: (att_at(1, i), att_at(0, i), z_out))

    def att_landed(i):
        landed(att_at(0, i), ("att", i), z_in)

    def joined(results, pair):
        side = (kv_heads + pair * 2 // group) % 2
        placed = [results[b] if side == b else pltpu.roll(results[b], HD, 1) for b in range(2)]
        return by_half(placed[0], placed[1]).astype(jnp.bfloat16)

    def tile_of(head):
        return pl.ds(head // 2 * LANES, LANES)

    nt = (((1,), (1,)), ((), ()))
    total_len = length * n

    def windowed(side, pair):
        start = (s if side == 0 else s - step) * length
        shape = (2 * WINDOW, 3 * WINDOW)
        row = lax.rem(lax.broadcasted_iota(jnp.int32, shape, 0), WINDOW)
        at = lax.broadcasted_iota(jnp.int32, shape, 1) - WINDOW
        near_by = (at - row <= WINDOW) & (at - row >= -WINDOW)
        first = lax.broadcasted_iota(jnp.int32, (2 * WINDOW, 1), 0) < WINDOW
        floor = jnp.where(first, sink_ref[0, 2 * pair], sink_ref[0, 2 * pair + 1])
        blocks = range(length // WINDOW)
        near = [pl.ds(b * WINDOW, 3 * WINDOW) for b in blocks]
        rows = [pl.ds(b * WINDOW, WINDOW) for b in blocks]
        scores, expon, total = [], [], []
        for b in blocks:
            key = ext[side, near[b], tile_of(2 * pair // group)]
            query = qs[1, side, 2 * pair : 2 * pair + 2, rows[b], :].reshape(2 * WINDOW, LANES)
            pos = at + (start + b * WINDOW)
            valid = near_by & (pos >= 0) & (pos < total_len)
            found = lax.dot_general(query, key, nt, preferred_element_type=jnp.float32)
            scores.append(jnp.where(valid, found, -jnp.inf))
        tops = [jnp.maximum(jnp.max(score, axis=-1, keepdims=True), floor) for score in scores]
        for score, top in zip(scores, tops):
            expon.append(jnp.exp(score - top))
            total.append(jnp.sum(expon[-1], axis=-1, keepdims=True) + jnp.exp(floor - top))
        for b in blocks:
            value = ext[side, near[b], tile_of(kv_heads + 2 * pair // group)]
            weight = (expon[b] / total[b]).astype(jnp.bfloat16)
            found = jnp.dot(weight, value, preferred_element_type=jnp.float32)
            att[side, rows[b], pair * LANES : (pair + 1) * LANES] = joined((found[:WINDOW], found[WINDOW:]), pair)

    def dense(side, pair, first=0, last=length // LANES):
        @pl.loop(first, last)
        def _(b):
            rows = pl.ds(pl.multiple_of(b * LANES, LANES), LANES)
            key = kvd[:, :, tile_of(2 * pair // group)].reshape(total_len, LANES)
            value = kvd[:, :, tile_of(kv_heads + 2 * pair // group)].reshape(total_len, LANES)
            query = qs[0, side, 2 * pair : 2 * pair + 2, rows, :].reshape(2 * LANES, LANES)
            scores = lax.dot_general(query, key, nt, preferred_element_type=jnp.float32)
            top = jnp.max(scores, axis=-1, keepdims=True)
            expon = jnp.exp(scores - top)
            total = jnp.sum(expon, axis=-1, keepdims=True)
            summed = jnp.dot(expon.astype(jnp.bfloat16), value, preferred_element_type=jnp.float32) / total
            at = (pairs + pair) * LANES
            att[side, rows, at : at + LANES] = joined((summed[:LANES], summed[LANES:]), pair)

    @pl.when(outer)
    def _():
        normalize(t * share, share)
        for p in range(width // depth):
            x_inward(p)
        for one in loads[3:]:
            one.wait()
        for k, rel in ((1, 0), (2, 0), (1, 1), (3, 0), (2, 1), (3, 1)):
            for c in all_chunks:
                w_inward("outer", k, 0, rel, c)
        for rel in range(2):
            for c in all_out:
                o_inward("outer", 0, rel, c)
        for c in all_out:
            o_outer(1, c)
        for i in range(pairs, 2 * pairs):
            att_landed(i)

    @pl.when(inner)
    def _():
        for one in loads[3:]:
            one.wait()
        for c in all_out:
            o_outward(0, c)
        normalize(0, length)
        for c in all_chunks:
            mates(0, c)
            crossing(0, 2, c)
        for k in range(1, KINDS):
            for c in all_chunks:
                w_inward("inner", k, 0, 0, c)
        tables(0, length)
        for c in all_chunks:
            crossing(0, 3, c)
        x_relay(0)
        tables(length, length)
        crossing(1, 2, 0)
        x_relay(1)
        crossing(1, 2, 1)
        x_pass(0)
        x_relay(2)
        crossing(2, 2, 0)
        x_pass(1)
        x_relay(3)
        crossing(2, 2, 1)
        mate_ready(0)
        for j in range(2, 4):
            twin_ready(0, j)
        for j in range(4):
            project(0, j, (0,))
        finished(0, 0)
        kv_inward(0)
        x_pass(2)
        crossing(3, 2, 0)
        mates(1, 0)
        x_pass(3)
        crossing(3, 2, 1)
        mates(1, 1)
        for p in range(width // depth):
            x_all(p)
        for j in range(4):
            project(0, j, (1,))
        finished(0, 1)
        kv_inward(1)
        project(1, 0)
        twin_ready(1, 2)
        project(1, 2)
        mates(2, 0)
        crossing(1, 3, 0)
        project(2, 0)
        mates(2, 1)
        crossing(1, 3, 1)
        twin_ready(2, 2)
        project(2, 2)
        mate_ready(1)
        project(1, 1)
        twin_ready(1, 3)
        project(1, 3)
        finished(1, 1)
        finished(1, 0)
        kv_landed(2)
        kv_landed(3)
        crossing(2, 3, 0)
        mates(3, 0)
        dense(1, 0)
        att_outward(pairs)
        crossing(2, 3, 1)
        mates(3, 1)
        for c in range(2):
            o_inward("inner", 0, 0, c)
        dense(1, 1)
        att_outward(pairs + 1)
        crossing(3, 3, 0)
        dense(0, 0)
        mate_ready(2)
        project(2, 1)
        crossing(3, 3, 1)
        twin_ready(2, 3)
        project(2, 3)
        project(3, 0)
        finished(2, 1)
        finished(2, 0)
        halo_inward()
        for c in range(2, out_chunks):
            o_inward("inner", 0, 0, c)
        halo_local()
        twin_ready(3, 2)
        project(3, 2)
        mate_ready(3)
        project(3, 1)
        o_crossing(2, 0)
        twin_ready(3, 3)
        project(3, 3, (1,))
        finished(3, 1, 0)
        windowed(1, 0)
        att_outward(0)
        finished(3, 1, 1)
        windowed(1, 1)
        att_outward(1)
        o_crossing(2, 1)
        o_mates(0)
        project(3, 3, (0,))
        finished(3, 0)
        halo_landed()
        o_mates(1)
        windowed(0, 0)
        o_crossing(2, 2)
        windowed(0, 1)
        o_mates(2)
        dense(0, 1, 0, 1)
        o_crossing(2, 3)
        dense(0, 1, 1, 2)
        o_mates(3)
        dense(0, 1, 2)

    @pl.when(outer)
    def _():
        o_outer(2, 0)
        for i in range(pairs):
            att_landed(i)

    def span(rel, first=0, count=out_chunks):
        h = g if rel == 0 else 1 - g
        return pl.ds(pl.multiple_of(h * out_half + first * out_size, out_size), count * out_size)

    def tail(role, script):
        def emit(*piece):
            j, lanes = piece[0], span(*piece[1:])
            found = jnp.dot(att[0], wo[j, :, lanes], preferred_element_type=jnp.float32).astype(jnp.bfloat16)
            for dest in range(n_tp):
                part[j, dest % 2, dest // 2, :, lanes] = found[dest * share : (dest + 1) * share]
            remote(role, ("d",) + piece, lambda: (
                part.at[j, 1 - core, :, :, span(*piece[1:])], dbuf.at[j, :, :, span(*piece[1:])], {"tp": twin}
            ))

        def combine(*piece):
            j, lanes = piece[0], span(*piece[1:])
            landed(dbuf.at[j, :, :, lanes], ("d",) + piece, {"tp": twin})
            both = (
                part[j, core, 1 - chip, :, lanes].astype(jnp.float32) + dbuf[j, 1 - chip, :, lanes].astype(jnp.float32)
            )
            xsend[j, :, lanes] = both.astype(jnp.bfloat16)
            remote(role, ("r",) + piece, lambda: (
                xsend.at[j, :, span(*piece[1:])], xrecv.at[j, :, span(*piece[1:])], {"tp": across}
            ))

        def emit_mate(*piece):
            j, lanes = piece[0], span(*piece[1:])
            found = jnp.dot(att[1], wo[j, :, lanes], preferred_element_type=jnp.float32).astype(jnp.bfloat16)
            for dest in range(n_tp):
                mpart[dest % 2, dest // 2, :, lanes] = found[dest * share : (dest + 1) * share]
            remote(role, ("md",) + piece, lambda: (
                mpart.at[1 - core, :, :, span(*piece[1:])], mbuf.at[:, :, span(*piece[1:])], {"tp": twin}
            ))

        def combine_mate(*piece):
            lanes = span(*piece[1:])
            landed(mbuf.at[:, :, lanes], ("md",) + piece, {"tp": twin})
            both = mpart[core, :, :, lanes].astype(jnp.float32) + mbuf[:, :, lanes].astype(jnp.float32)
            msum[:, :, lanes] = both.astype(jnp.bfloat16)
            remote(role, ("r",) + piece, lambda: (
                msum.at[1 - chip, :, span(*piece[1:])], xrecv.at[piece[0], :, span(*piece[1:])],
                {"sp": outward, "tp": across},
            ), "m")
            remote(role, ("m",) + piece, lambda: (
                msum.at[chip, :, span(*piece[1:])], msum.at[chip, :, span(*piece[1:])], z_out
            ))

        def settle(*piece):
            j, lanes = piece[0], span(*piece[1:])
            landed(xrecv.at[j, :, lanes], ("r",) + piece, {"tp": across})
            if role == "outer" and j == 3:
                landed(msum.at[chip, :, lanes], ("m",) + piece, z_in)
                near = msum[chip, :, lanes].astype(jnp.float32)
            else:
                near = part[j, core, chip, :, lanes].astype(jnp.float32) + dbuf[j, chip, :, lanes].astype(jnp.float32)
            total = near + xrecv[j, :, lanes].astype(jnp.float32)
            rel, first, count = piece[1:] if len(piece) > 2 else (piece[1], 0, out_chunks)
            h = g if rel == 0 else 1 - g
            base = place_of(j) * out_cols + h * out_half + first * out_size
            out_ref[:, pl.ds(pl.multiple_of(base, out_size), count * out_size)] = total.astype(jnp.bfloat16)

        def ready(j, first=0, count=out_chunks):
            for c in range(first, first + count):
                if role == "inner" and j == 1:
                    o_landed(1, 1, c, z_out)
                else:
                    o_twin_landed(j, c)

        def pump(j, c):
            if role == "inner":
                o_crossing(j, c)
            else:
                o_outer(j, c)

        words = {
            "emit": emit, "combine": combine, "settle": settle, "ready": ready, "pump": pump,
            "emit_mate": emit_mate, "combine_mate": combine_mate,
        }
        for word, *piece in script:
            words[word](*piece)

    opening = [("emit", 0, 0), ("emit", 0, 1), ("emit", 1, 0)]
    last = [(3, 1, 0, 2), (3, 1, 2, 1), (3, 1, 3, 1)]
    far = [(3, 0, 0, 2), (3, 0, 2, 2)] + last
    inner_script = (
        opening
        + [("pump", 3, 0), ("combine", 0, 0), ("emit", 2, 0), ("combine", 0, 1), ("ready", 2), ("emit", 2, 1)]
        + [("combine", 1, 0), ("pump", 3, 1), ("combine", 2, 0), ("combine", 2, 1), ("pump", 3, 2)]
        + [("emit_mate",) + far[0], ("emit",) + far[0]]
        + [("pump", 3, 3), ("combine_mate",) + far[0], ("emit_mate",) + far[1], ("emit",) + far[1]]
        + [("combine",) + far[0], ("ready", 3, 0, 2), ("combine_mate",) + far[1], ("emit_mate",) + last[0]]
        + [("emit",) + last[0], ("combine",) + far[1], ("ready", 1), ("emit", 1, 1)]
        + [("combine_mate",) + last[0], ("combine",) + last[0], ("combine", 1, 1)]
        + [("ready", 3, 2, 1), ("emit_mate",) + last[1], ("emit",) + last[1]]
        + [("settle", 0, 0), ("settle", 0, 1), ("combine_mate",) + last[1]]
        + [("ready", 3, 3, 1), ("emit_mate",) + last[2], ("emit",) + last[2]]
        + [("combine",) + last[1], ("settle", 1, 0), ("combine_mate",) + last[2], ("combine",) + last[2]]
        + [("settle", 2, 0), ("settle", 2, 1), ("settle",) + far[0], ("settle",) + far[1]]
        + [("settle",) + last[0], ("settle", 1, 1)] + [("settle",) + piece for piece in last[1:]]
    )
    outer_script = (
        [("emit", 0, 0), ("emit", 0, 1), ("combine", 0, 0), ("emit", 1, 0), ("combine", 0, 1), ("ready", 1)]
        + [("emit", 1, 1), ("combine", 1, 0), ("pump", 2, 1), ("combine", 1, 1), ("pump", 2, 2), ("pump", 2, 3)]
        + [("emit", 2, 0), ("ready", 2, 0, 2), ("combine", 2, 0)]
        + [("ready", 2, 2, 2), ("emit", 2, 1), ("settle", 0, 0), ("settle", 0, 1), ("combine", 2, 1)]
        + [("settle", 1, 0), ("settle", 1, 1), ("settle", 2, 0), ("settle",) + far[0], ("settle", 2, 1)]
        + [("settle",) + piece for piece in far[1:]]
    )

    @pl.when(inner)
    def _():
        tail("inner", inner_script)

    @pl.when(outer)
    def _():
        tail("outer", outer_script)

    for role, test in (("inner", inner), ("outer", outer)):

        @pl.when(test)
        def _():
            for group, at in sent[role].items():
                ref = whole(role, group)
                pltpu.make_async_remote_copy(
                    src_ref=ref, dst_ref=ref, send_sem=send_sem.at[at], recv_sem=recv_sem.at[0],
                    device_id=y_peer, device_id_type=MESH,
                ).wait_send()


def local(*args):
    tokens_in, norm_gain, wq, wk, wv, wq_gain, wk_gain, sink, dq, dk, dv, dq_gain, dk_gain, w_out, d_out = args
    length, width = tokens_in.shape
    n, n_tp = lax.axis_size("sp"), lax.axis_size("tp")
    depth, cols = wq.shape
    paired = (
        n == 4 and n_tp == 4 and wk.shape[1] == LANES and cols == 2 * LANES and depth * n == width
        and length % (n_tp * 32) == 0 and length % WINDOW == 0
    )
    if not paired:
        return local_ring(*args)
    q_heads, kv_heads = cols // HD, wk.shape[1] // HD
    out_rows, out_cols = w_out.shape[0] + d_out.shape[0], w_out.shape[1]
    share = length // n_tp
    lane = np.arange(LANES)
    fixed = np.stack(
        [THETA ** (-2.0 * (lane % (wide // 2)) / wide) for wide in (HD, HD // 2)]
        + [np.where(lane % wide < wide // 2, -1.0, 1.0) for wide in (HD, HD // 2)]
    ).astype(np.float32)
    gains = [gain[None, :] for gain in (wq_gain, wk_gain, dq_gain, dk_gain)]
    chunks, out_chunks = 2, 4
    vmem = pl.BlockSpec(memory_space=pltpu.VMEM)
    bf16 = jnp.bfloat16

    def sem(*shape):
        return pltpu.SemaphoreType.DMA(shape)

    return pl.pallas_call(
        functools.partial(pair_kernel, (q_heads, kv_heads, chunks, out_chunks)),
        out_shape=pltpu.VMEM((share, width), bf16),
        in_specs=[vmem] * 6
        + [pl.BlockSpec(memory_space=pltpu.SMEM)]
        + [pl.BlockSpec(memory_space=pl.ANY)] * 9,
        out_specs=vmem,
        scratch_shapes=[
            pltpu.VMEM((8, LANES), jnp.float32),
            pltpu.VMEM((4, 2 * length, LANES), jnp.float32),
            pltpu.VMEM((length, width), bf16),
            pltpu.VMEM((2 * length, width), bf16),
            pltpu.VMEM((KINDS, n, depth, cols), bf16),
            pltpu.VMEM((n, out_rows, out_cols), bf16),
            pltpu.VMEM((2, 2 * length, cols), jnp.float32),
            pltpu.VMEM((n, length, cols), bf16),
            pltpu.VMEM((2, length + 2 * WINDOW, cols), bf16),
            pltpu.VMEM((2, 2, q_heads, length, LANES), bf16),
            pltpu.VMEM((2, length, out_rows), bf16),
            pltpu.VMEM((n, 2, n_tp // 2, share, out_cols), bf16),
            pltpu.VMEM((n, 2, share, out_cols), bf16),
            pltpu.VMEM((n, share, out_cols), bf16),
            pltpu.VMEM((n, share, out_cols), bf16),
            pltpu.VMEM((2, n_tp // 2, share, out_cols), bf16),
            pltpu.VMEM((n_tp // 2, share, out_cols), bf16),
            pltpu.VMEM((n_tp // 2, share, out_cols), bf16),
            sem(RECEIVES),
            sem(SENDS),
            sem(LOCALS),
        ],
        compiler_params=pltpu.CompilerParams(
            collective_id=0, has_side_effects=True, vmem_limit_bytes=62 * 1024 * 1024
        ),
    )(norm_gain[None, :], fixed, *gains, sink[None, :], tokens_in, wq, dq, dk, dv, wk, wv, w_out, d_out)


def solution(mesh):
    return jax.shard_map(
        local,
        mesh=mesh,
        in_specs=(
            P(("grp", "sp"), None),
            P(),
            P("sp", "tp"),
            P("sp", "tp"),
            P("sp", "tp"),
            P(),
            P(),
            P("tp"),
            P("sp", "tp"),
            P("sp", "tp"),
            P("sp", "tp"),
            P(),
            P(),
            P("tp", "sp"),
            P("tp", "sp"),
        ),
        out_specs=P(("grp", "sp", "tp"), None),
        check_vma=False,
    )
```
